256 devices in a mesh: sp: 64 (over z, x, core), tp: 4 (over y).
Axes of the slice: x: 4, y: 4, z: 8, core: 2. Of those that a mesh axis runs over, the one named last changes fastest.
Arguments:
- layer_cot: bfloat16 [16384, 2048], P('sp'), may hold values from -16 to 16
- moe_input: bfloat16 [16384, 2048], P('sp'), may hold values from -6 to 6
- routes: int32 [16384, 2], P('sp'), may hold values from 0 to 63, all different within a row; in each aligned block of 256 rows (0 to 255, 256 to 511, ...) at most 12 rows name the same one
- route_weights: float32 [16384, 2], P('sp'), may hold values from 0.1 to 1.2
- gate_proj: bfloat16 [64, 2048, 1024], P('sp', None, 'tp'), may hold values from -0.125 to 0.125
- up_proj: bfloat16 [64, 2048, 1024], P('sp', None, 'tp'), may hold values from -0.125 to 0.125
- down_proj: bfloat16 [64, 1024, 2048], P('sp', 'tp'), may hold values from -0.1875 to 0.1875
- out_proj: bfloat16 [2048, 2048], P('tp'), may hold values from -0.0625 to 0.0625
- mixer_out: bfloat16 [16384, 2048], P('sp', 'tp'), may hold values from -6 to 6
- queries: bfloat16 [16384, 1024], P('sp', 'tp'), may hold values from -0.75 to 0.75
- key_rows: bfloat16 [16384, 1024], P('sp', 'tp'), may hold values from -0.75 to 0.75
- values: bfloat16 [16384, 2048], P('sp', 'tp'), may hold values from -6 to 6
- log_decay: float32 [16384, 1024], P('sp', 'tp'), may hold values from -2 to 0, as said below
- saved_state: float32 [64, 32, 32, 64], P('sp', 'tp'), may hold values from -6 to 6
Outputs:
- grad_gate: bfloat16 [64, 2048, 1024], P('sp', None, 'tp')
- grad_up: bfloat16 [64, 2048, 1024], P('sp', None, 'tp')
- grad_down: bfloat16 [64, 1024, 2048], P('sp', 'tp')
- grad_outproj: float32 [2048, 2048], P('sp', 'tp')
- grad_queries: bfloat16 [16384, 1024], P('sp', 'tp')
- grad_keys: bfloat16 [16384, 1024], P('sp', 'tp')
- grad_values: bfloat16 [16384, 2048], P('sp', 'tp')
- grad_decay: float32 [16384, 1024], P('sp', 'tp')
The draws below stay inside these ranges and needn't reach their ends.
Inputs may be any that keep to these rules, and one draw needn't show every extreme that they name: `routes`: each row names 2 different experts; no expert is named by more than 12 of the tokens of one index of sp, and in every draw some expert is named exactly 12 times by one such span. `log_decay`: log decays are negative.
All inputs are finite; a program needn't handle non-finite values.
Results may differ from the reference program's by a relative error of at most 0.014.
Values may be sent and summed in bfloat16 or wider, within the bound.
No kernel may reach another device: no remote copies, remote signals or barrier semaphores. Data moves between devices by JAX's collectives and lax.ppermute only.
A program may use at most 128 MiB of HBM per device.

```python
import math
import jax
import jax.numpy as jnp
import numpy as np
from jax import lax

D = 2048
HEAD_COUNT = 32
KEY_CHANNELS = 32
DV = 64
FF = 1024
TOK_DEV = 256
BLOCK = 64
TOPK = 2
TOKEN_COUNT = 16384
SPANS = 64
EXPERTS = 64
CAP = 12
SLOTS = 768
HK = 1024
HV = 2048
N_TP = 4


def draw_log_decay(key, part):
    random_subkeys = jax.random.split(key, 10)
    fast_share = 0.5
    head_quick_rates = jax.random.uniform(random_subkeys[0], (HEAD_COUNT,), jnp.float32) < fast_share
    channel_fast = jnp.repeat(head_quick_rates, KEY_CHANNELS)
    slow_rates = 0.3 * 2.302585 / TOKEN_COUNT * jax.random.uniform(random_subkeys[1], (HEAD_COUNT * KEY_CHANNELS,), jnp.float32, 0.3, 1.0)
    fast_rates = jnp.exp(jax.random.uniform(random_subkeys[2], (HEAD_COUNT * KEY_CHANNELS,), jnp.float32, -4.6, -3.4))
    decay_rates = jnp.where(channel_fast, fast_rates, slow_rates)
    span_factor = jnp.exp(jax.random.uniform(random_subkeys[3], (SPANS,), jnp.float32, -0.69, 0.69))
    position_factor = jnp.repeat(span_factor, TOK_DEV)
    jitter = jnp.exp(0.5 * jnp.clip(jax.random.normal(random_subkeys[4], (TOKEN_COUNT, HEAD_COUNT * KEY_CHANNELS), jnp.float32), -2.0, 2.0) - 0.125)
    logarithm_rates = -decay_rates[None, :] * position_factor[:, None] * jitter
    spike_position = jax.random.randint(random_subkeys[5], (HEAD_COUNT, 2), 0, TOKEN_COUNT)
    spike_length = jax.random.uniform(random_subkeys[6], (HEAD_COUNT, 2), jnp.float32, -0.69, -0.22)
    token_positions = jnp.arange(TOKEN_COUNT, dtype=jnp.int32)
    spike_events = jnp.sum(jnp.where(token_positions[:, None, None] == spike_position[None, :, :], spike_length[None, :, :], 0.0), axis=2)
    spike_events = jnp.where(head_quick_rates[None, :], 0.0, spike_events)
    base_values = logarithm_rates + jnp.repeat(spike_events, KEY_CHANNELS, axis=1)
    channel_order = jax.random.permutation(random_subkeys[7], HEAD_COUNT * KEY_CHANNELS)
    strong_channel = channel_order < HEAD_COUNT * KEY_CHANNELS // 16
    run_start = jax.random.randint(random_subkeys[8], (HEAD_COUNT * KEY_CHANNELS,), 0, TOKEN_COUNT - 127)
    in_run = strong_channel[None, :] & (token_positions[:, None] >= run_start[None, :]) & (token_positions[:, None] < run_start[None, :] + 128)
    strong_values = jax.random.uniform(random_subkeys[9], (TOKEN_COUNT, HEAD_COUNT * KEY_CHANNELS), jnp.float32, -2.0, -1.6)
    return jnp.where(in_run, strong_values, base_values).astype(jnp.float32)


def raised(result, stream_key, source, target, blocks, factor):
    def block_of(axis_at):
        return (jnp.arange(result.shape[axis_at]) // (result.shape[axis_at] // blocks)).reshape((-1,) + (1,) * (result.ndim - 1 - axis_at))

    near = jax.random.permutation(stream_key, blocks)[block_of(target)]
    other_side = (block_of(target) + blocks // 2) % blocks
    return jnp.where((block_of(source) == near) | (block_of(source) == other_side), factor * result, result)


def block_scale(own_key, shape, cuts, least, high):
    def one(position, parts):
        draws = jax.random.uniform(jax.random.fold_in(jax.random.fold_in(own_key, 6), position), (parts,), jnp.float32, least / len(cuts), high / len(cuts))
        return jnp.repeat(jnp.exp(draws), shape[position] // parts).reshape((-1,) + (1,) * (len(shape) - position - 1))

    factor_of = one(*cuts[0])
    for cut in cuts[1:]:
        factor_of = factor_of * one(*cut)
    return factor_of


def routed_block(stream_key, own, number, rows, number_of, top, reach, lean):
    sequence = jax.random.permutation(stream_key, number_of)
    heavy_load, common = load_shares(number_of, rows * top, reach, lean, True), load_shares(number_of, rows * top, reach, lean, False)
    places = jnp.arange(number_of)

    def named(sizes, offset_by):
        used = int((sizes > 0).sum())
        fixed = max(1, used // 4)
        moved = fixed + (places - fixed + offset_by * (used - fixed)) % max(1, number_of - fixed)
        return jnp.zeros((number_of,), jnp.int32).at[sequence[jnp.where(places < fixed, places, moved)]].set(jnp.asarray(sizes, jnp.int32))

    sizes = jnp.where(number % 4 == 0, named(heavy_load, number // 4), named(common, number - number // 4 - 1))
    mixed = jax.random.permutation(jax.random.fold_in(own, 3), number_of)
    donor, receiver = mixed[0:number_of // 2 * 2:2], mixed[1:number_of // 2 * 2:2]
    margin = jnp.minimum(sizes[donor] - 1, reach - sizes[receiver]) // 2
    margin = jnp.where((donor == sequence[0]) | (receiver == sequence[0]) | (sizes[receiver] == 0), 0, jnp.maximum(margin, 0))
    moved = jax.random.randint(jax.random.fold_in(own, 4), (number_of // 2,), 0, 1 << 20) % (margin + 1)
    sizes = sizes.at[donor].add(-moved).at[receiver].add(moved)
    items = jnp.searchsorted(jnp.cumsum(sizes), jnp.arange(rows * top), side="right").astype(jnp.int32)
    table = items.reshape(top, rows).T
    table = table[jax.random.permutation(jax.random.fold_in(own, 1), rows)]
    offset_by = jax.random.randint(jax.random.fold_in(own, 2), (rows, 1), 0, top)
    return jnp.take_along_axis(table, (jnp.arange(top)[None, :] + offset_by) % top, axis=1)


def load_shares(number_of, total, limit, slope, full):
    loads = [(1 << 20) // math.isqrt(grade ** slope) + 1 for grade in range(1, number_of + 1)]
    largest = limit if full else min(limit, max(-(-total // number_of), total * loads[0] // sum(loads)))
    least = 1 if total - largest >= number_of - 1 else 0
    given, rest = [largest] + [least] * (number_of - 1), total - largest - least * (number_of - 1)
    while rest > 0:
        candidates = [i for i in range(1, number_of) if given[i] < largest] or [i for i in range(1, number_of) if given[i] < limit]
        whole, left = sum([loads[i] for i in candidates]), rest
        for i in candidates:
            extra = min(limit - given[i], max(1, left * loads[i] // whole), rest)
            given[i] = given[i] + extra
            rest = rest - extra
    return np.array(given)


def noise(stream_key, extent, spread, most, cuts=(), kind=jnp.bfloat16):
    gain = block_scale(stream_key, extent, cuts, -0.22, 0.18) if cuts else 1.0
    entries = jax.random.normal(stream_key, extent, jnp.float32) * spread * gain
    return jnp.minimum(jnp.maximum(entries, -most), most).astype(kind)


def bell_draw_with(stream_key, shape, width, limit, shards, heavy, held_as=jnp.bfloat16):
    entries = width * jax.random.normal(stream_key, shape, jnp.float32)
    if shards:
        entries = entries * block_scale(stream_key, shape, shards, -0.22, 0.18)
    return jnp.clip(raised(entries, jax.random.fold_in(stream_key, 3), *heavy), -limit, limit).astype(held_as)


def setup_inputs(seed: int = 0) -> dict:
    keys = jax.random.split(jax.random.key(seed), 15)
    layer_cot = bell_draw_with(keys[0], (TOKEN_COUNT, D), 1.0, 16.0, ((0, 64),), (0, 1, 64, 4.0))
    moe_input = noise(keys[1], (TOKEN_COUNT, D), 1.0, 6.0, ((0, 64),))
    routes_keys = jax.random.split(jax.random.fold_in(keys[2], 1), TOKEN_COUNT // TOK_DEV)
    routes_turns = jax.random.permutation(jax.random.fold_in(keys[2], 3), TOKEN_COUNT // TOK_DEV)
    routes = jax.vmap(lambda own, number: routed_block(jax.random.fold_in(keys[2], 2), own, number, TOK_DEV, EXPERTS, TOPK, CAP, 2))(routes_keys, routes_turns).reshape((TOKEN_COUNT, TOPK))
    route_weights = jnp.clip(0.1 + 1.1 * jax.random.uniform(keys[3], (TOKEN_COUNT, TOPK), jnp.float32) ** block_scale(keys[3], (TOKEN_COUNT, TOPK), ((0, 64),), -0.2, 0.2), 0.1, 1.2)
    gate_proj = noise(keys[4], (EXPERTS, D, FF), D ** -0.5, 0.125, ((0, 64), (2, 4)))
    up_proj = noise(keys[5], (EXPERTS, D, FF), D ** -0.5, 0.125, ((0, 64), (2, 4)))
    down_proj = noise(keys[6], (EXPERTS, FF, D), FF ** -0.5, 0.1875, ((0, 64), (1, 4)))
    out_proj = noise(keys[7], (HV, D), (4 * D) ** -0.5, 0.0625, ((0, 4),))
    mixer_out = noise(keys[8], (TOKEN_COUNT, HV), 1.0, 6.0, ((0, 64), (1, 4)))
    queries = noise(keys[9], (TOKEN_COUNT, HK), 0.125, 0.75, ((0, 64), (1, 4)))
    key_rows = noise(keys[10], (TOKEN_COUNT, HK), 0.125, 0.75, ((0, 64), (1, 4)))
    values = noise(keys[11], (TOKEN_COUNT, HV), 1.0, 6.0, ((0, 64), (1, 4)))
    log_decay = draw_log_decay(jax.random.fold_in(keys[14], 71), 0)
    saved_state = noise(keys[13], (SPANS, HEAD_COUNT, KEY_CHANNELS, DV), 1.0, 6.0, ((0, 64), (1, 4)), jnp.float32)
    return {"layer_cot": layer_cot, "moe_input": moe_input, "routes": routes, "route_weights": route_weights, "gate_proj": gate_proj, "up_proj": up_proj, "down_proj": down_proj, "out_proj": out_proj, "mixer_out": mixer_out, "queries": queries, "key_rows": key_rows, "values": values, "log_decay": log_decay, "saved_state": saved_state}


highest = lax.Precision.HIGHEST


def to_blocks(tensor, col_width):
    block_count = tensor.shape[0] // BLOCK
    head_count = tensor.shape[1] // col_width
    return tensor.astype(jnp.float32).reshape(block_count, BLOCK, head_count, col_width).transpose(0, 2, 1, 3)


def from_blocks(tensor):
    block_count, head_count, length, col_width = tensor.shape
    return tensor.transpose(0, 2, 1, 3).reshape(block_count * length, head_count * col_width)


def block_grads(queries, key_rows, values, cumulative, out_grad, state_in, from_later):
    final_log = cumulative[:, -1, :]
    token_positions = jnp.arange(cumulative.shape[1], dtype=jnp.int32)
    causal_mask = (token_positions[:, None] >= token_positions[None, :])[None, :, :, None]
    log_gaps = cumulative[:, :, None, :] - cumulative[:, None, :, :]
    decays = jnp.where(causal_mask, jnp.exp(jnp.where(causal_mask, log_gaps, 0.0)), 0.0)
    scores = jnp.einsum('htd,hsd,htsd->hts', queries, key_rows, decays, precision=highest)
    couplings = jnp.einsum('htv,hsv->hts', out_grad, values, precision=highest)
    to_end = jnp.exp(final_log[:, None, :] - cumulative)
    grad_queries = jnp.exp(cumulative) * jnp.einsum('hdv,htv->htd', state_in, out_grad, precision=highest) + jnp.einsum('hts,hsd,htsd->htd', couplings, key_rows, decays, precision=highest)
    grad_keys = to_end * jnp.einsum('hdv,hsv->hsd', from_later, values, precision=highest) + jnp.einsum('hts,htd,htsd->hsd', couplings, queries, decays, precision=highest)
    grad_values = jnp.einsum('hdv,hsd->hsv', from_later, key_rows * to_end, precision=highest) + jnp.einsum('hts,htv->hsv', scores, out_grad, precision=highest)
    grad_cumul = queries * grad_queries - key_rows * grad_keys
    to_start = jnp.exp(final_log)[:, :, None] * from_later + jnp.einsum('htd,htv->hdv', queries * jnp.exp(cumulative), out_grad, precision=highest)
    return to_start, (grad_queries, grad_keys, grad_values, grad_cumul)


def expert_grads(operands):
    rows_in, rows_cot, gate_w, up_w, down_w = operands
    pre_gate = jnp.dot(rows_in, gate_w, preferred_element_type=jnp.float32)
    pre_up = jnp.dot(rows_in, up_w, preferred_element_type=jnp.float32)
    sigmoid_gate = jax.nn.sigmoid(pre_gate)
    hidden = (pre_gate * sigmoid_gate * pre_up).astype(jnp.bfloat16)
    grad_hidden = lax.dot_general(rows_cot, down_w, (((1,), (1,)), ((), ())), preferred_element_type=jnp.float32)
    grad_down = lax.dot_general(hidden, rows_cot, (((0,), (0,)), ((), ())), preferred_element_type=jnp.float32).astype(jnp.bfloat16)
    grad_pre_gate = (grad_hidden * pre_up * sigmoid_gate * (1.0 + pre_gate * (1.0 - sigmoid_gate))).astype(jnp.bfloat16)
    grad_pre_up = (grad_hidden * pre_gate * sigmoid_gate).astype(jnp.bfloat16)
    grad_gate = lax.dot_general(rows_in, grad_pre_gate, (((0,), (0,)), ((), ())), preferred_element_type=jnp.float32).astype(jnp.bfloat16)
    grad_up = lax.dot_general(rows_in, grad_pre_up, (((0,), (0,)), ((), ())), preferred_element_type=jnp.float32).astype(jnp.bfloat16)
    group_size = FF // N_TP
    gate_parts = jnp.einsum('rjf,djf->jrd', grad_pre_gate.astype(jnp.float32).reshape(-1, N_TP, group_size), gate_w.astype(jnp.float32).reshape(D, N_TP, group_size))
    up_parts = jnp.einsum('rjf,djf->jrd', grad_pre_up.astype(jnp.float32).reshape(-1, N_TP, group_size), up_w.astype(jnp.float32).reshape(D, N_TP, group_size))
    rounded = lax.optimization_barrier((gate_parts + up_parts).astype(jnp.bfloat16))
    row_grads = jnp.sum(rounded.astype(jnp.float32), axis=0).astype(jnp.bfloat16)
    return grad_gate, grad_up, grad_down, row_grads


def mixer_grads(queries, key_rows, values, log_decay, out_grad, saved_state):
    span_blocks = TOK_DEV // BLOCK
    query_b = to_blocks(queries, KEY_CHANNELS)
    key_b = to_blocks(key_rows, KEY_CHANNELS)
    value_b = to_blocks(values, DV)
    grad_b = to_blocks(out_grad, DV)
    cumulative = jnp.cumsum(to_blocks(log_decay, KEY_CHANNELS), axis=2)
    indices = jnp.arange(query_b.shape[0], dtype=jnp.int32)

    def forward(carried, inputs):
        key_blk, value_blk, cumul_blk, block_index = inputs
        state_in = jnp.where(block_index % span_blocks == 0, saved_state[block_index // span_blocks], carried)
        final_log = cumul_blk[:, -1, :]
        state_after = jnp.exp(final_log)[:, :, None] * state_in + jnp.einsum('hsd,hsv->hdv', key_blk * jnp.exp(final_log[:, None, :] - cumul_blk), value_blk, precision=highest)
        return state_after, (state_in, state_after)

    zeros_state = jnp.zeros(saved_state.shape[1:], jnp.float32)
    _, (starts, afters) = lax.scan(forward, zeros_state, (key_b, value_b, cumulative, indices))

    def backward(carried, inputs):
        to_start, block_out = block_grads(*inputs, carried)
        return to_start, (carried,) + block_out

    _, outputs = lax.scan(backward, zeros_state, (query_b, key_b, value_b, cumulative, grad_b, starts), reverse=True)
    laters, query_grads, key_grads, value_grads, cumul_grads = outputs
    span_ends = afters[span_blocks - 1::span_blocks]
    later_ends = laters[span_blocks - 1::span_blocks]
    cross_term = jnp.sum(span_ends * later_ends, axis=3).reshape(SPANS, 1, HK)
    flat_cum = from_blocks(cumul_grads).reshape(SPANS, TOK_DEV, HK)
    reversed_sum = jnp.flip(jnp.cumsum(jnp.flip(flat_cum, 1), axis=1), 1)
    grad_decay = (reversed_sum + cross_term).reshape(TOKEN_COUNT, HK)
    return (from_blocks(query_grads).astype(jnp.bfloat16), from_blocks(key_grads).astype(jnp.bfloat16),
            from_blocks(value_grads).astype(jnp.bfloat16), grad_decay)


def reference(layer_cot, moe_input, routes, route_weights, gate_proj, up_proj, down_proj, out_proj, mixer_out, queries, key_rows, values, log_decay, saved_state):
    flat_routes = routes.reshape(-1).astype(jnp.int32)
    assign_count = flat_routes.shape[0]
    onehot = (flat_routes[:, None] == jnp.arange(EXPERTS, dtype=jnp.int32)[None, :]).astype(jnp.int32)
    per_span = onehot.reshape(SPANS, TOPK * TOK_DEV, EXPERTS)
    before = jnp.cumsum(per_span, axis=1) - per_span
    slot_ranks = jnp.sum(before * per_span, axis=2).reshape(-1)
    span_ids = jnp.arange(assign_count, dtype=jnp.int32) // (TOPK * TOK_DEV)
    places = (flat_routes * SLOTS + span_ids * CAP + slot_ranks).astype(jnp.int32)
    sources = jnp.full((EXPERTS * SLOTS,), assign_count, jnp.int32).at[places].set(jnp.arange(assign_count, dtype=jnp.int32))
    filled = sources < assign_count
    clipped = jnp.minimum(sources, assign_count - 1)
    token_ids = clipped // TOPK
    slot_weights = jnp.where(filled, route_weights.reshape(-1)[clipped], 0.0)
    expert_rows = jnp.where(filled[:, None], moe_input[token_ids], jnp.zeros((), moe_input.dtype)).reshape(EXPERTS, SLOTS, D)
    expert_cots = (slot_weights[:, None] * layer_cot[token_ids].astype(jnp.float32)).astype(jnp.bfloat16).reshape(EXPERTS, SLOTS, D)
    grad_gate, grad_up, grad_down, row_grads = lax.map(expert_grads, (expert_rows, expert_cots, gate_proj, up_proj, down_proj))
    picked = row_grads.reshape(EXPERTS * SLOTS, D)[places].astype(jnp.float32)
    moe_grad = jnp.sum(picked.reshape(TOKEN_COUNT, TOPK, D), axis=1)
    mix_grad = (layer_cot.astype(jnp.float32) + moe_grad).astype(jnp.bfloat16)
    out_grad = lax.dot_general(mix_grad, out_proj, (((1,), (1,)), ((), ())), preferred_element_type=jnp.float32).astype(jnp.bfloat16)
    grad_outproj = lax.dot_general(mix_grad, mixer_out, (((0,), (0,)), ((), ())), preferred_element_type=jnp.float32)
    grad_queries, grad_keys, grad_values, grad_decay = mixer_grads(queries, key_rows, values, log_decay, out_grad, saved_state)
    return (grad_gate, grad_up, grad_down, grad_outproj, grad_queries, grad_keys, grad_values, grad_decay)
```

```python
import jax
import jax.numpy as jnp
from jax import lax
from jax.experimental import pallas as pl
from jax.experimental.pallas import tpu as pltpu
from jax.sharding import Mesh
from jax.sharding import PartitionSpec as P

KEY_CHANNELS = 32
DV = 64
BLOCK = 64
CAP = 12
SP = ("sp_0", "sp_1", "sp_2")
F32 = jnp.float32
BF16 = jnp.bfloat16


def dot(a, b, contract, dt=jnp.bfloat16):
    return lax.dot_general(
        a.astype(dt), b.astype(dt), (contract, ((), ())), preferred_element_type=jnp.float32
    )


NN = ((1,), (0,))
NT = ((1,), (1,))
TN = ((0,), (0,))


def summed_by(x, mask, pieces):
    total, rest = (None, x)
    for _ in range(pieces):
        part = rest.astype(jnp.bfloat16)
        rest = rest - part.astype(jnp.float32)
        term = dot(part, mask, NN)
        total = term if total is None else total + term
    return total


def triangle(length, keep):
    down = lax.broadcasted_iota(jnp.int32, (length, length), 0)
    across = lax.broadcasted_iota(jnp.int32, (length, length), 1)
    return jnp.where(keep(down, across), 1.0, 0.0).astype(jnp.bfloat16)


def route_kernel(rank_ref, routes_ref, weights_ref, in_ref, cot_ref, rows_in_ref, rows_cot_ref, places_ref):
    tokens = routes_ref.shape[1]
    slots = rows_in_ref.shape[0]
    experts = slots // CAP
    first, second = (routes_ref[0:1, :], routes_ref[1:2, :])
    expert_ids = lax.broadcasted_iota(jnp.int32, (experts, tokens), 0)
    named_first, named_second = (expert_ids == first, expert_ids == second)
    named = jnp.where(named_first | named_second, 1.0, 0.0)
    before = dot(named, triangle(tokens, lambda u, t: u < t), NN)

    def place(hit, route):
        rank = jnp.sum(jnp.where(hit, before, 0.0), axis=0, keepdims=True)
        return route * CAP + rank.astype(jnp.int32)

    place_a, place_b = (place(named_first, first), place(named_second, second))
    places_ref[0:1, :] = place_a
    places_ref[1:2, :] = place_b
    slot_ids = lax.broadcasted_iota(jnp.int32, (slots, tokens), 0)
    hit_a, hit_b = (slot_ids == place_a, slot_ids == place_b)
    chosen = jnp.where(hit_a | hit_b, 1.0, 0.0).astype(jnp.bfloat16)
    slot_weights = jnp.sum(
        jnp.where(hit_a, weights_ref[0:1, :], 0.0) + jnp.where(hit_b, weights_ref[1:2, :], 0.0),
        axis=1,
        keepdims=True,
    )
    rows_in_ref[...] = dot(chosen, in_ref[...], NN).astype(jnp.bfloat16)
    rows_cot_ref[...] = (slot_weights * dot(chosen, cot_ref[...], NN)).astype(jnp.bfloat16)


def combine_kernel(rank_ref, places_ref, returned_ref, cot_ref, out_ref):
    tokens, slots = (cot_ref.shape[0], returned_ref.shape[0])
    slot_ids = lax.broadcasted_iota(jnp.int32, (tokens, slots), 1)
    hits = (slot_ids == places_ref[:, 0:1]) | (slot_ids == places_ref[:, 1:2])
    moe_grad = dot(jnp.where(hits, 1.0, 0.0), returned_ref[...], NN)
    out_ref[...] = (cot_ref[...].astype(jnp.float32) + moe_grad).astype(jnp.bfloat16)


def turned(x):
    return x.astype(jnp.float32).T


def span_kernel(q_ref, log_ref, grad_ref, term_ref, total_ref):
    tokens = q_ref.shape[0]
    cum = summed_by(turned(log_ref[...]), triangle(tokens, lambda u, t: u <= t), 3)
    total_ref[...] = cum[:, tokens - 1 :]
    q_start = (turned(q_ref[...]) * jnp.exp(cum)).astype(jnp.bfloat16)
    grad = grad_ref[...]
    for h in range(q_ref.shape[1] // KEY_CHANNELS):
        ks, vs = (slice(h * KEY_CHANNELS, (h + 1) * KEY_CHANNELS), slice(h * DV, (h + 1) * DV))
        term_ref[ks, :] = dot(q_start[ks], grad[vs], NT)


def mixer_kernel(
    q_ref, k_ref, v_ref, log_ref, grad_ref, state_ref, later_ref, gq_ref, gk_ref, gv_ref, gd_ref,
    dq_s, dk_s, dv_s, cross_s,
):
    tokens, channels = q_ref.shape
    half = tokens // 2
    cum = summed_by(turned(log_ref[...]), triangle(tokens, lambda u, t: u <= t), 3)
    q, k = (turned(q_ref[...]), turned(k_ref[...]))
    v = turned(v_ref[...]).astype(jnp.bfloat16)
    grad = grad_ref[...]
    lane = lax.broadcasted_iota(jnp.int32, (channels, tokens), 1)
    block = lane // BLOCK
    at = lambda t: cum[:, t : t + 1]
    near = jnp.where(
        block < 2,
        jnp.where(block == 0, at(31), at(95)),
        jnp.where(block == 2, at(159), at(223)),
    )
    wide = jnp.exp(-jnp.abs(cum - at(127)))
    mid = jnp.exp(-jnp.abs(cum - jnp.where(block < 2, at(63), at(191))))
    gap = cum - near
    up, down = (jnp.exp(gap), jnp.exp(-gap))
    start = jnp.exp(cum)
    end = jnp.exp(at(tokens - 1) - cum)
    whole = jnp.exp(at(tokens - 1))
    q_wide = jnp.where(block >= 2, q * wide, 0.0).astype(jnp.bfloat16)
    k_wide = jnp.where(block < 2, k * wide, 0.0).astype(jnp.bfloat16)
    q_mid, k_mid = ((q * mid), (k * mid))
    q_mids = [jnp.where(block == b, q_mid, 0.0).astype(jnp.bfloat16) for b in (1, 3)]
    k_mids = [jnp.where(block == b, k_mid, 0.0).astype(jnp.bfloat16) for b in (0, 2)]
    q_near, k_near = (q * up, k * down)
    q_nears = [jnp.where(block == b, q_near, 0.0).astype(jnp.bfloat16) for b in range(4)]
    k_nears = [jnp.where(block == b, k_near, 0.0).astype(jnp.bfloat16) for b in range(4)]
    q_parts = [q_wide, *q_mids, *q_nears]
    k_parts = [k_wide, *k_mids, *k_nears]
    k_end = (k * end).astype(jnp.bfloat16)
    down_ids = lax.broadcasted_iota(jnp.int32, (tokens, tokens), 0)
    across_ids = lax.broadcasted_iota(jnp.int32, (tokens, tokens), 1)
    causal = down_ids >= across_ids
    first64 = lax.broadcasted_iota(jnp.int32, (KEY_CHANNELS, half), 1) < BLOCK
    lo, hi = (slice(0, half), slice(half, tokens))
    kc = KEY_CHANNELS
    for h in range(channels // kc):
        ks, vs = (slice(h * kc, (h + 1) * kc), slice(h * DV, (h + 1) * DV))
        q_seg = jnp.concatenate([p[ks] for p in q_parts], axis=0)
        k_seg = jnp.concatenate([p[ks] for p in k_parts], axis=0)
        grad_h, v_h = (grad[vs], v[vs])
        scores = jnp.where(causal, dot(q_seg, k_seg, TN), 0.0).astype(jnp.bfloat16)
        coupl = jnp.where(causal, dot(grad_h, v_h, TN), 0.0).astype(jnp.bfloat16)
        to_q = dot(k_seg, coupl, NT)
        to_k = dot(q_seg, coupl, NN)
        seg = lambda x, i, side: x[i * kc : (i + 1) * kc, side]
        state = state_ref[ks, :]
        later = later_ref[ks, :]
        dq = start[ks] * dot(state, grad_h, NN)
        dk = end[ks] * dot(later, v_h, NN)
        dq_lo = up[ks, lo] * jnp.where(first64, seg(to_q, 3, lo), seg(to_q, 4, lo))
        dq_lo += mid[ks, lo] * jnp.where(first64, 0.0, seg(to_q, 1, lo))
        dq_hi = up[ks, hi] * jnp.where(first64, seg(to_q, 5, hi), seg(to_q, 6, hi))
        dq_hi += mid[ks, hi] * jnp.where(first64, 0.0, seg(to_q, 2, hi))
        dq_hi += wide[ks, hi] * seg(to_q, 0, hi)
        dk_lo = down[ks, lo] * jnp.where(first64, seg(to_k, 3, lo), seg(to_k, 4, lo))
        dk_lo += mid[ks, lo] * jnp.where(first64, seg(to_k, 1, lo), 0.0)
        dk_lo += wide[ks, lo] * seg(to_k, 0, lo)
        dk_hi = down[ks, hi] * jnp.where(first64, seg(to_k, 5, hi), seg(to_k, 6, hi))
        dk_hi += mid[ks, hi] * jnp.where(first64, seg(to_k, 2, hi), 0.0)
        dq_s[ks, :] = dq + jnp.concatenate([dq_lo, dq_hi], axis=1)
        dk_s[ks, :] = dk + jnp.concatenate([dk_lo, dk_hi], axis=1)
        dv_s[vs, :] = dot(grad_h, scores, NN) + dot(later, k_end[ks], TN)
        at_end = whole[ks] * state + dot(k_end[ks], v_h, NT)
        cross_s[ks, :] = jnp.sum(at_end * later, axis=1, keepdims=True)
    dq, dk = (dq_s[...], dk_s[...])
    change = q * dq - k * dk
    decay = summed_by(change, triangle(tokens, lambda u, t: u >= t), 2) + cross_s[...]
    gq_ref[...] = dq.T.astype(jnp.bfloat16)
    gk_ref[...] = dk.T.astype(jnp.bfloat16)
    gv_ref[...] = dv_s[...].T.astype(jnp.bfloat16)
    gd_ref[...] = decay.T


def scan_kernel(terms_ref, totals_ref, turned_ref, out_ref):
    spans = terms_ref.shape[0]
    channels = totals_ref.shape[1]
    down_ids = lax.broadcasted_iota(jnp.int32, (spans, spans), 0)
    across_ids = lax.broadcasted_iota(jnp.int32, (spans, spans), 1)
    later = across_ids > down_ids
    up_to = jnp.where(down_ids >= across_ids, 1.0, 0.0)
    before = jnp.where(down_ids < across_ids, 1.0, 0.0)
    exact = lax.Precision.HIGHEST
    through = jnp.dot(up_to, totals_ref[...], precision=exact, preferred_element_type=F32)
    ahead = jnp.dot(turned_ref[...], before, precision=exact, preferred_element_type=F32)
    for c in range(channels):
        gap = ahead[c : c + 1, :] - through[:, c : c + 1]
        weight = jnp.where(later, jnp.exp(jnp.where(later, gap, 0.0)), 0.0)
        vs = slice(c * DV, (c + 1) * DV)
        out_ref[:, vs] = jnp.dot(
            weight, terms_ref[:, vs].astype(F32), precision=exact, preferred_element_type=F32
        ).astype(out_ref.dtype)


def project_kernel(rank_ref, mix_ref, proj_ref, mixer_ref, part_ref, grad_ref, total_ref):
    step = pl.program_id(0)
    mix = mix_ref[...]
    grads = dot(proj_ref[...], mix, NT)

    @pl.when(step == 0)
    def _():
        total_ref[...] = grads

    @pl.when(step > 0)
    def _():
        total_ref[...] += grads

    part = dot(mix, mixer_ref[...], TN).astype(BF16)
    lines = part_ref.shape[3]
    for x in range(part_ref.shape[1]):
        for c in range(2):
            at = (x * 2 + c) * lines
            part_ref[c, x, 0, :, :] = part[at : at + lines, :]

    @pl.when(step == pl.num_programs(0) - 1)
    def _():
        grad_ref[...] = total_ref[...].astype(BF16)


def turn_kernel(rank_ref, *refs):
    count = len(refs) // 2
    for k in range(count):
        refs[count + k][...] = refs[k][...]


def call(kernel, outs, *args, scratch=()):
    return pl.pallas_call(
        kernel,
        out_shape=[jax.ShapeDtypeStruct(shape, dtype) for shape, dtype in outs],
        scratch_shapes=[pltpu.VMEM(shape, F32) for shape in scratch],
    )(*args)


def quarters_turned(rank, sign, arrays, dims):
    in_specs, out_specs = ([], [])
    for a, dim in zip(arrays, dims):
        block = tuple(n // 4 if d == dim else n for d, n in enumerate(a.shape))

        def source(i, r, dim=dim):
            at = lax.rem(i + 4 + sign * r[0], 4)
            return tuple(at if d == dim else 0 for d in range(2))

        def target(i, r, dim=dim):
            return tuple(i if d == dim else 0 for d in range(2))

        in_specs.append(pl.BlockSpec(block, source))
        out_specs.append(pl.BlockSpec(block, target))
    return pl.pallas_call(
        turn_kernel,
        grid_spec=pltpu.PrefetchScalarGridSpec(
            num_scalar_prefetch=1, grid=(4,), in_specs=in_specs, out_specs=out_specs
        ),
        out_shape=[jax.ShapeDtypeStruct(a.shape, a.dtype) for a in arrays],
    )(rank, *arrays)


def routed(rank, routes, weights, moe_input, layer_cot, slots):
    tokens, width = layer_cot.shape
    part = width // 4
    whole = lambda shape: pl.BlockSpec(shape, lambda i, r: (0, 0))
    own = pl.BlockSpec((tokens, part), lambda i, r: (0, r[0]))
    return pl.pallas_call(
        route_kernel,
        grid_spec=pltpu.PrefetchScalarGridSpec(
            num_scalar_prefetch=1,
            grid=(1,),
            in_specs=[whole(routes.shape), whole(weights.shape), own, own],
            out_specs=[whole((slots, part)), whole((slots, part)), whole(routes.shape)],
        ),
        out_shape=[
            jax.ShapeDtypeStruct((slots, part), BF16),
            jax.ShapeDtypeStruct((slots, part), BF16),
            jax.ShapeDtypeStruct(routes.shape, jnp.int32),
        ],
    )(rank, routes, weights, moe_input, layer_cot)


def combined(rank, places, returned, layer_cot, chunk, chunks):
    tokens = layer_cot.shape[0]
    slots, width = returned.shape
    whole = lambda shape: pl.BlockSpec(shape, lambda i, r: (0, 0))
    return pl.pallas_call(
        combine_kernel,
        grid_spec=pltpu.PrefetchScalarGridSpec(
            num_scalar_prefetch=1,
            grid=(1,),
            in_specs=[
                whole(places.shape),
                whole(returned.shape),
                pl.BlockSpec((tokens, width), lambda i, r: (0, r[0] * chunks + chunk)),
            ],
            out_specs=whole((tokens, width)),
        ),
        out_shape=jax.ShapeDtypeStruct((tokens, width), BF16),
    )(rank, places, returned, layer_cot)


def projected(rank, mix, out_proj, mixer_out):
    tokens, width = mix.shape
    z_count, x_count, c_count = (lax.axis_size(axis) for axis in SP)
    cols = out_proj.shape[0]
    block = width // z_count
    per = z_count // 4
    lines = block // (x_count * c_count)
    return pl.pallas_call(
        project_kernel,
        grid_spec=pltpu.PrefetchScalarGridSpec(
            num_scalar_prefetch=1,
            grid=(z_count,),
            in_specs=[
                pl.BlockSpec(
                    (tokens, block), lambda z, r: (0, lax.rem(z // per + 4 - r[0], 4) * per + z % per)
                ),
                pl.BlockSpec((cols, block), lambda z, r: (0, z)),
                pl.BlockSpec(mixer_out.shape, lambda z, r: (0, 0)),
            ],
            out_specs=[
                pl.BlockSpec((c_count, x_count, 1, lines, cols), lambda z, r: (0, 0, z, 0, 0)),
                pl.BlockSpec((cols, tokens), lambda z, r: (0, 0)),
            ],
            scratch_shapes=[pltpu.VMEM((cols, tokens), F32)],
        ),
        out_shape=[
            jax.ShapeDtypeStruct((c_count, x_count, z_count, lines, cols), BF16),
            jax.ShapeDtypeStruct((cols, tokens), BF16),
        ],
    )(rank, mix, out_proj, mixer_out)


def shifted(x, axis, by):
    count = lax.axis_size(axis)
    return lax.ppermute(x, axis, [(i, (i + by) % count) for i in range(count)])


def gathered(x):
    half = x.shape[0] // 2
    before, after = (shifted(x, "tp", 1), shifted(x, "tp", -1))
    across = jnp.concatenate(
        [shifted(before[:half], "tp", 1), shifted(after[half:], "tp", -1)], axis=0
    )
    return x, after, across, before


def reduced(own, after, across, before):
    half = own.shape[0] // 2
    from_before = shifted(across[:half], "tp", 1)
    from_after = shifted(across[half:], "tp", -1)
    add = lambda a, b: (a.astype(F32) + b.astype(F32)).astype(BF16)
    to_after = jnp.concatenate([add(after[:half], from_before), after[half:]], axis=0)
    to_before = jnp.concatenate([before[:half], add(before[half:], from_after)], axis=0)
    left, right = (shifted(to_after, "tp", 1), shifted(to_before, "tp", -1))
    return (own.astype(F32) + left.astype(F32) + right.astype(F32)).astype(BF16)


def exchanged(x, axis):
    return lax.all_to_all(x, axis, split_axis=0, concat_axis=0, tiled=True)


def body(
    layer_cot,
    moe_input,
    routes,
    route_weights,
    gate_proj,
    up_proj,
    down_proj,
    out_proj,
    mixer_out,
    queries,
    key_rows,
    values,
    log_decay,
    saved_state,
):
    sp_count = lax.axis_size(SP)
    slots = sp_count * CAP
    tokens, model_width = layer_cot.shape
    quarter = model_width // 4
    chunks = 2
    rank = lax.axis_index("tp").astype(jnp.int32).reshape(1)
    rows_in, rows_cot, places = routed(
        rank, routes.T, route_weights.T, moe_input, layer_cot, slots
    )
    by_span = lambda x: x.reshape(sp_count, CAP, x.shape[-1])
    by_slot = lambda x: x.reshape(slots, x.shape[-1])
    gate_w, up_w, down_w = quarters_turned(
        rank, 1, (gate_proj[0], up_proj[0], down_proj[0]), (0, 0, 1)
    )
    got_in = jnp.concatenate(gathered(by_slot(exchanged(by_span(rows_in), SP))), axis=1)
    got_cot = jnp.concatenate(gathered(by_slot(exchanged(by_span(rows_cot), SP))), axis=1)
    pre_gate = dot(got_in, gate_w, NN)
    pre_up = dot(got_in, up_w, NN)
    sigmoid_gate = jax.nn.sigmoid(pre_gate)
    hidden = (pre_gate * sigmoid_gate * pre_up).astype(BF16)
    grad_hidden = dot(got_cot, down_w, NT)
    grad_pre_gate = (
        grad_hidden * pre_up * sigmoid_gate * (1.0 + pre_gate * (1.0 - sigmoid_gate))
    ).astype(BF16)
    grad_pre_up = (grad_hidden * pre_gate * sigmoid_gate).astype(BF16)
    wide = quarter // chunks
    mix_chunks = []
    places_col = places.T
    for chunk in range(chunks):
        parts = []
        for k in range(4):
            at = slice(k * quarter + chunk * wide, k * quarter + (chunk + 1) * wide)
            part = dot(grad_pre_gate, gate_w[at], NT) + dot(grad_pre_up, up_w[at], NT)
            parts.append(part.astype(BF16))
        summed = reduced(*parts)
        returned = by_slot(exchanged(by_span(summed), SP))
        mix_chunks.append(gathered(combined(rank, places_col, returned, layer_cot, chunk, chunks)))
    mix = jnp.concatenate([mix_chunks[c][k] for k in range(4) for c in range(chunks)], axis=1)
    grad_gate = dot(got_in, grad_pre_gate, TN).astype(BF16)
    grad_up = dot(got_in, grad_pre_up, TN).astype(BF16)
    grad_down = dot(hidden, got_cot, TN).astype(BF16)
    grad_gate, grad_up, grad_down = quarters_turned(
        rank, -1, (grad_gate, grad_up, grad_down), (0, 0, 1)
    )
    part, out_grad = projected(rank, mix, out_proj, mixer_out)

    core = lax.axis_index(SP[2])
    channels = queries.shape[1]
    term, total = call(
        span_kernel, [((channels, DV), F32), ((channels, 1), F32)], queries, log_decay, out_grad
    )
    span_totals = jnp.sum(log_decay, axis=0)
    totals = exchanged(span_totals.reshape(sp_count, -1), SP)
    terms = exchanged(term.astype(BF16).reshape(sp_count, 2, -1), SP)
    (laters,) = call(
        scan_kernel,
        [((sp_count, channels * DV // sp_count), BF16)],
        terms.reshape(sp_count, -1),
        totals,
        totals.T,
    )
    from_later = exchanged(laters.reshape(sp_count, 2, -1), SP).reshape(channels, DV).astype(F32)

    mine = lax.dynamic_index_in_dim(part, core, 0, keepdims=False)
    other = lax.dynamic_index_in_dim(part, 1 - core, 0, keepdims=False)
    pair = (mine.astype(F32) + shifted(other, SP[2], 1).astype(F32)).astype(BF16)
    row = jnp.sum(exchanged(pair, SP[1]).astype(F32), axis=0).astype(BF16)
    grad_outproj = jnp.sum(exchanged(row, SP[0]).astype(F32), axis=0)

    grad_queries, grad_keys, grad_values, grad_decay = call(
        mixer_kernel,
        [
            (queries.shape, BF16),
            (key_rows.shape, BF16),
            (values.shape, BF16),
            (log_decay.shape, F32),
        ],
        queries,
        key_rows,
        values,
        log_decay,
        out_grad,
        saved_state.reshape(channels, DV),
        from_later,
        scratch=(
            (channels, tokens),
            (channels, tokens),
            (values.shape[1], tokens),
            (channels, 1),
        ),
    )
    return (
        grad_gate[None],
        grad_up[None],
        grad_down[None],
        grad_outproj,
        grad_queries,
        grad_keys,
        grad_values,
        grad_decay,
    )


def solution(mesh):
    torus = Mesh(mesh.devices.reshape(8, 4, 2, mesh.shape["tp"]), ("sp_0", "sp_1", "sp_2", "tp"))
    return jax.shard_map(
        body,
        mesh=torus,
        in_specs=(
            P(SP, None),
            P(SP, None),
            P(SP, None),
            P(SP, None),
            P(SP, None, "tp"),
            P(SP, None, "tp"),
            P(SP, "tp", None),
            P("tp", None),
            P(SP, "tp"),
            P(SP, "tp"),
            P(SP, "tp"),
            P(SP, "tp"),
            P(SP, "tp"),
            P(SP, "tp", None, None),
        ),
        out_specs=(
            P(SP, None, "tp"),
            P(SP, None, "tp"),
            P(SP, "tp", None),
            P(SP, "tp"),
            P(SP, "tp"),
            P(SP, "tp"),
            P(SP, "tp"),
            P(SP, "tp"),
        ),
        check_vma=False,
    )
```

```python
import jax
import jax.numpy as jnp
from jax import lax
from jax.experimental import pallas as pl
from jax.experimental.pallas import tpu as pltpu
from jax.sharding import Mesh
from jax.sharding import PartitionSpec as P

KEY_CHANNELS = 32
DV = 64
BLOCK = 64
CAP = 12
SP = ("sp_0", "sp_1", "sp_2")
F32 = jnp.float32
BF16 = jnp.bfloat16


def dot(a, b, contract, dt=jnp.bfloat16):
    return lax.dot_general(
        a.astype(dt), b.astype(dt), (contract, ((), ())), preferred_element_type=jnp.float32
    )


NN = ((1,), (0,))
NT = ((1,), (1,))
TN = ((0,), (0,))


def summed_by(x, mask, pieces):
    total, rest = (None, x)
    for _ in range(pieces):
        part = rest.astype(jnp.bfloat16)
        rest = rest - part.astype(jnp.float32)
        term = dot(part, mask, NN)
        total = term if total is None else total + term
    return total


def triangle(length, keep):
    down = lax.broadcasted_iota(jnp.int32, (length, length), 0)
    across = lax.broadcasted_iota(jnp.int32, (length, length), 1)
    return jnp.where(keep(down, across), 1.0, 0.0).astype(jnp.bfloat16)


def route_kernel(rank_ref, routes_ref, weights_ref, in_ref, cot_ref, rows_in_ref, rows_cot_ref, places_ref):
    tokens = routes_ref.shape[1]
    slots = rows_in_ref.shape[0]
    experts = slots // CAP
    first, second = (routes_ref[0:1, :], routes_ref[1:2, :])
    expert_ids = lax.broadcasted_iota(jnp.int32, (experts, tokens), 0)
    named_first, named_second = (expert_ids == first, expert_ids == second)
    named = jnp.where(named_first | named_second, 1.0, 0.0)
    before = dot(named, triangle(tokens, lambda u, t: u < t), NN)

    def place(hit, route):
        rank = jnp.sum(jnp.where(hit, before, 0.0), axis=0, keepdims=True)
        return route * CAP + rank.astype(jnp.int32)

    place_a, place_b = (place(named_first, first), place(named_second, second))
    places_ref[0:1, :] = place_a
    places_ref[1:2, :] = place_b
    slot_ids = lax.broadcasted_iota(jnp.int32, (slots, tokens), 0)
    hit_a, hit_b = (slot_ids == place_a, slot_ids == place_b)
    chosen = jnp.where(hit_a | hit_b, 1.0, 0.0).astype(jnp.bfloat16)
    slot_weights = jnp.sum(
        jnp.where(hit_a, weights_ref[0:1, :], 0.0) + jnp.where(hit_b, weights_ref[1:2, :], 0.0),
        axis=1,
        keepdims=True,
    )
    rows_in_ref[...] = dot(chosen, in_ref[...], NN).astype(jnp.bfloat16)
    rows_cot_ref[...] = (slot_weights * dot(chosen, cot_ref[...], NN)).astype(jnp.bfloat16)


def combine_kernel(ranks_ref, places_ref, returned_ref, cot_ref, out_ref):
    tokens, slots = (cot_ref.shape[0], returned_ref.shape[0])
    slot_ids = lax.broadcasted_iota(jnp.int32, (tokens, slots), 1)
    hits = (slot_ids == places_ref[:, 0:1]) | (slot_ids == places_ref[:, 1:2])
    moe_grad = dot(jnp.where(hits, 1.0, 0.0), returned_ref[...], NN)
    out_ref[...] = (cot_ref[...].astype(F32) + moe_grad).astype(BF16)


def turned(x):
    return x.astype(jnp.float32).T


def start_kernel(q_ref, log_ref, start_ref, total_ref):
    tokens = q_ref.shape[0]
    cum = summed_by(turned(log_ref[...]), triangle(tokens, lambda u, t: u <= t), 3)
    rest = cum[:, tokens - 1 :]
    for k in range(3):
        piece = rest.astype(BF16)
        rest = rest - piece.astype(F32)
        total_ref[:, k : k + 1] = piece
    start_ref[...] = (turned(q_ref[...]) * jnp.exp(cum)).astype(BF16)


def mixer_kernel(
    q_ref, k_ref, v_ref, log_ref, grad_ref, state_ref, later_ref, gq_ref, gk_ref, gv_ref, gd_ref,
    dq_s, dk_s, dv_s, cross_s,
):
    tokens, channels = q_ref.shape
    half = tokens // 2
    cum = summed_by(turned(log_ref[...]), triangle(tokens, lambda u, t: u <= t), 3)
    q, k = (turned(q_ref[...]), turned(k_ref[...]))
    v = turned(v_ref[...]).astype(jnp.bfloat16)
    grad = grad_ref[...]
    lane = lax.broadcasted_iota(jnp.int32, (channels, tokens), 1)
    block = lane // BLOCK
    at = lambda t: cum[:, t : t + 1]
    near = jnp.where(
        block < 2,
        jnp.where(block == 0, at(31), at(95)),
        jnp.where(block == 2, at(159), at(223)),
    )
    wide = jnp.exp(-jnp.abs(cum - at(127)))
    mid = jnp.exp(-jnp.abs(cum - jnp.where(block < 2, at(63), at(191))))
    gap = cum - near
    up, down = (jnp.exp(gap), jnp.exp(-gap))
    start = jnp.exp(cum)
    end = jnp.exp(at(tokens - 1) - cum)
    whole = jnp.exp(at(tokens - 1))
    q_wide = jnp.where(block >= 2, q * wide, 0.0).astype(jnp.bfloat16)
    k_wide = jnp.where(block < 2, k * wide, 0.0).astype(jnp.bfloat16)
    q_mid, k_mid = ((q * mid), (k * mid))
    q_mids = [jnp.where(block == b, q_mid, 0.0).astype(jnp.bfloat16) for b in (1, 3)]
    k_mids = [jnp.where(block == b, k_mid, 0.0).astype(jnp.bfloat16) for b in (0, 2)]
    q_near, k_near = (q * up, k * down)
    q_nears = [jnp.where(block == b, q_near, 0.0).astype(jnp.bfloat16) for b in range(4)]
    k_nears = [jnp.where(block == b, k_near, 0.0).astype(jnp.bfloat16) for b in range(4)]
    q_parts = [q_wide, *q_mids, *q_nears]
    k_parts = [k_wide, *k_mids, *k_nears]
    k_end = (k * end).astype(jnp.bfloat16)
    down_ids = lax.broadcasted_iota(jnp.int32, (tokens, tokens), 0)
    across_ids = lax.broadcasted_iota(jnp.int32, (tokens, tokens), 1)
    causal = down_ids >= across_ids
    first64 = lax.broadcasted_iota(jnp.int32, (KEY_CHANNELS, half), 1) < BLOCK
    lo, hi = (slice(0, half), slice(half, tokens))
    kc = KEY_CHANNELS
    for h in range(channels // kc):
        ks, vs = (slice(h * kc, (h + 1) * kc), slice(h * DV, (h + 1) * DV))
        q_seg = jnp.concatenate([p[ks] for p in q_parts], axis=0)
        k_seg = jnp.concatenate([p[ks] for p in k_parts], axis=0)
        grad_h, v_h = (grad[vs], v[vs])
        scores = jnp.where(causal, dot(q_seg, k_seg, TN), 0.0).astype(jnp.bfloat16)
        coupl = jnp.where(causal, dot(grad_h, v_h, TN), 0.0).astype(jnp.bfloat16)
        to_q = dot(k_seg, coupl, NT)
        to_k = dot(q_seg, coupl, NN)
        seg = lambda x, i, side: x[i * kc : (i + 1) * kc, side]
        state = state_ref[ks, :]
        later = later_ref[ks, :]
        dq = start[ks] * dot(state, grad_h, NN)
        dk = end[ks] * dot(later, v_h, NN)
        dq_lo = up[ks, lo] * jnp.where(first64, seg(to_q, 3, lo), seg(to_q, 4, lo))
        dq_lo += mid[ks, lo] * jnp.where(first64, 0.0, seg(to_q, 1, lo))
        dq_hi = up[ks, hi] * jnp.where(first64, seg(to_q, 5, hi), seg(to_q, 6, hi))
        dq_hi += mid[ks, hi] * jnp.where(first64, 0.0, seg(to_q, 2, hi))
        dq_hi += wide[ks, hi] * seg(to_q, 0, hi)
        dk_lo = down[ks, lo] * jnp.where(first64, seg(to_k, 3, lo), seg(to_k, 4, lo))
        dk_lo += mid[ks, lo] * jnp.where(first64, seg(to_k, 1, lo), 0.0)
        dk_lo += wide[ks, lo] * seg(to_k, 0, lo)
        dk_hi = down[ks, hi] * jnp.where(first64, seg(to_k, 5, hi), seg(to_k, 6, hi))
        dk_hi += mid[ks, hi] * jnp.where(first64, seg(to_k, 2, hi), 0.0)
        dq_s[ks, :] = dq + jnp.concatenate([dq_lo, dq_hi], axis=1)
        dk_s[ks, :] = dk + jnp.concatenate([dk_lo, dk_hi], axis=1)
        dv_s[vs, :] = dot(grad_h, scores, NN) + dot(later, k_end[ks], TN)
        at_end = whole[ks] * state + dot(k_end[ks], v_h, NT)
        cross_s[ks, :] = jnp.sum(at_end * later, axis=1, keepdims=True)
    dq, dk = (dq_s[...], dk_s[...])
    change = q * dq - k * dk
    decay = summed_by(change, triangle(tokens, lambda u, t: u >= t), 2) + cross_s[...]
    gq_ref[...] = dq.T.astype(jnp.bfloat16)
    gk_ref[...] = dk.T.astype(jnp.bfloat16)
    gv_ref[...] = dv_s[...].T.astype(jnp.bfloat16)
    gd_ref[...] = decay.T


def scan_kernel(terms_ref, out_ref):
    spans, width = out_ref.shape
    channels = width // DV
    down_ids = lax.broadcasted_iota(jnp.int32, (spans, spans), 0)
    across_ids = lax.broadcasted_iota(jnp.int32, (spans, spans), 1)
    later = across_ids > down_ids
    up_to = jnp.where(down_ids >= across_ids, 1.0, 0.0)
    before = jnp.where(down_ids < across_ids, 1.0, 0.0)
    exact = lax.Precision.HIGHEST
    terms = terms_ref[...].astype(F32)
    pieces = [terms[:, width + k * channels : width + (k + 1) * channels] for k in range(3)]
    totals = pieces[0] + pieces[1] + pieces[2]
    through = jnp.dot(up_to, totals, precision=exact, preferred_element_type=F32)
    ahead = lax.dot_general(
        totals, before, (TN, ((), ())), precision=exact, preferred_element_type=F32
    )
    for c in range(channels):
        gap = ahead[c : c + 1, :] - through[:, c : c + 1]
        weight = jnp.where(later, jnp.exp(jnp.where(later, gap, 0.0)), 0.0)
        vs = slice(c * DV, (c + 1) * DV)
        out_ref[:, vs] = jnp.dot(
            weight, terms[:, vs], precision=exact, preferred_element_type=F32
        ).astype(out_ref.dtype)


def quarter_of(rank, k, width):
    return pl.ds(pl.multiple_of(lax.rem(rank + k, 4) * width, width), width)


def parted_kernel(ranks_ref, down_ref, *outs):
    width = down_ref.shape[1] // 4
    for k in range(4):
        outs[k][...] = down_ref[:, quarter_of(ranks_ref[0], k, width)]


def cot_kernel(cot_ref, d0, d1, d2, d3, own_ref, after_ref, across_ref, before_ref):
    cot = cot_ref[...]
    own_ref[...] = dot(cot, d0[...], NT)
    for out, part in ((after_ref, d1), (across_ref, d2), (before_ref, d3)):
        out[...] = dot(cot, part[...], NT).astype(BF16)


def in_kernel(ranks_ref, x0, x1, x2, x3, x4, gate_ref, up_ref, hidden_ref, to_gate_ref, to_up_ref):
    rank = ranks_ref[0]
    width = x0.shape[1]

    def product(w_ref):
        w = [w_ref[quarter_of(rank, k, width), :] for k in range(4)]
        across = jnp.concatenate([dot(x2[...], w[2], NN), dot(x3[...], w[2], NN)], axis=0)
        return dot(x0[...], w[0], NN) + dot(x1[...], w[1], NN) + across + dot(x4[...], w[3], NN)

    gate, up = (product(gate_ref), product(up_ref))
    sigmoid = jax.nn.sigmoid(gate)
    active = gate * sigmoid
    hidden_ref[...] = (active * up).astype(BF16)
    to_up_ref[...] = active
    to_gate_ref[...] = up * sigmoid * (1.0 + gate * (1.0 - sigmoid))


def grads_kernel(
    ranks_ref, own_ref, left_ref, right_ref, to_gate_ref, to_up_ref, gate_ref, up_ref,
    both_ref, p0, p1, p2, p3,
):
    rank = ranks_ref[0]
    width = p0.shape[1]
    half = gate_ref.shape[1]
    grad_hidden = own_ref[...] + left_ref[...].astype(F32) + right_ref[...].astype(F32)
    both_ref[:, :half] = (grad_hidden * to_gate_ref[...]).astype(BF16)
    both_ref[:, half:] = (grad_hidden * to_up_ref[...]).astype(BF16)
    both = both_ref[...]
    for k, out in ((2, p2), (1, p1), (3, p3), (0, p0)):
        at = quarter_of(rank, k, width)
        w = jnp.concatenate([gate_ref[at, :], up_ref[at, :]], axis=1)
        out[...] = dot(both, w, NT).astype(BF16)


def weights_kernel(ranks_ref, x0, x1, x2, x3, x4, both_ref, gate_ref, up_ref):
    rank = ranks_ref[0]
    width = x0.shape[1]
    half, rows = (gate_ref.shape[1], x2.shape[0])

    def put(k, grads):
        at = quarter_of(rank, k, width)
        gate_ref[at, :] = grads[:, :half].astype(BF16)
        up_ref[at, :] = grads[:, half:].astype(BF16)

    for k, x in ((0, x0), (1, x1), (3, x4)):
        put(k, dot(x[...], both_ref[...], TN))
    put(2, dot(x2[...], both_ref[:rows, :], TN) + dot(x3[...], both_ref[rows:, :], TN))


def down_kernel(ranks_ref, c0, c1, c2, c3, c4, hidden_ref, down_ref):
    rank = ranks_ref[0]
    width = c0.shape[1]
    rows = c2.shape[0]
    hidden = hidden_ref[...]
    for k, c in ((0, c0), (1, c1), (3, c4)):
        down_ref[:, quarter_of(rank, k, width)] = dot(hidden, c[...], TN).astype(BF16)
    across = dot(hidden[:rows], c2[...], TN) + dot(hidden[rows:], c3[...], TN)
    down_ref[:, quarter_of(rank, 2, width)] = across.astype(BF16)


def out_kernel(ranks_ref, m0, m1, m2, m3, m4, proj_ref, start_ref, grad_ref, term_ref):
    rank = ranks_ref[0]
    width = m0.shape[1]
    w = [proj_ref[:, quarter_of(rank, k, width)] for k in range(4)]
    across = jnp.concatenate([dot(w[2], m2[...], NT), dot(w[2], m3[...], NT)], axis=1)
    total = dot(w[0], m0[...], NT) + dot(w[1], m1[...], NT) + across + dot(w[3], m4[...], NT)
    grad = total.astype(BF16)
    grad_ref[...] = grad
    for h in range(start_ref.shape[0] // KEY_CHANNELS):
        ks, vs = (slice(h * KEY_CHANNELS, (h + 1) * KEY_CHANNELS), slice(h * DV, (h + 1) * DV))
        term_ref[ks, :] = dot(start_ref[ks, :], grad[vs], NT).astype(BF16)


def part_kernel(ranks_ref, m0, m1, m2, m3, m4, mixer_ref, mine_ref, other_ref):
    rank, z, x, core = (ranks_ref[k] for k in range(4))
    x_count, z_count, lines, _ = mine_ref.shape
    half = m2.shape[0]
    mixer = mixer_ref[...]

    def put(k, part):
        part = part.astype(BF16)
        quarter = lax.rem(rank + k, 4)
        per = z_count // 4
        for i in range(per * x_count):
            first = part[2 * i * lines : (2 * i + 1) * lines]
            second = part[(2 * i + 1) * lines : (2 * i + 2) * lines]
            to_z = lax.rem(quarter * per + i // x_count + z_count - z, z_count)
            to_x = lax.rem(i % x_count + x_count - x, x_count)
            mine_ref[to_x, to_z, :, :] = jnp.where(core == 0, first, second)
            other_ref[to_x, to_z, :, :] = jnp.where(core == 0, second, first)

    for k, m in ((0, m0), (1, m1), (3, m4)):
        put(k, dot(m[...], mixer, TN))
    put(2, dot(m2[...], mixer[:half], TN) + dot(m3[...], mixer[half:], TN))


def call(kernel, outs, *args, scratch=(), ranks=None, flops=None):
    specs = [pl.BlockSpec(memory_space=pltpu.VMEM) for _ in args]
    if ranks is not None:
        specs, args = ([pl.BlockSpec(memory_space=pltpu.SMEM), *specs], (ranks, *args))
    cost = flops and pl.CostEstimate(flops=flops, bytes_accessed=0, transcendentals=0)
    return pl.pallas_call(
        kernel,
        in_specs=specs,
        out_specs=[pl.BlockSpec(memory_space=pltpu.VMEM) for _ in outs],
        out_shape=[jax.ShapeDtypeStruct(shape, dtype) for shape, dtype in outs],
        scratch_shapes=[pltpu.VMEM(shape, F32) for shape in scratch],
        cost_estimate=cost,
    )(*args)


def routed(rank, routes, weights, moe_input, layer_cot, slots):
    tokens, width = layer_cot.shape
    part = width // 4
    whole = lambda shape: pl.BlockSpec(shape, lambda i, r: (0, 0))
    own = pl.BlockSpec((tokens, part), lambda i, r: (0, r[0]))
    return pl.pallas_call(
        route_kernel,
        grid_spec=pltpu.PrefetchScalarGridSpec(
            num_scalar_prefetch=1,
            grid=(1,),
            in_specs=[whole(routes.shape), whole(weights.shape), own, own],
            out_specs=[whole((slots, part)), whole((slots, part)), whole(routes.shape)],
        ),
        out_shape=[
            jax.ShapeDtypeStruct((slots, part), BF16),
            jax.ShapeDtypeStruct((slots, part), BF16),
            jax.ShapeDtypeStruct(routes.shape, jnp.int32),
        ],
    )(rank, routes, weights, moe_input, layer_cot)


def combined(rank, places, returned, layer_cot):
    tokens = layer_cot.shape[0]
    slots, width = returned.shape
    whole = lambda shape: pl.BlockSpec(shape, lambda i, r: (0, 0))
    return pl.pallas_call(
        combine_kernel,
        grid_spec=pltpu.PrefetchScalarGridSpec(
            num_scalar_prefetch=1,
            grid=(1,),
            in_specs=[
                whole(places.shape),
                whole(returned.shape),
                pl.BlockSpec((tokens, width), lambda i, r: (0, r[0])),
            ],
            out_specs=whole((tokens, width)),
        ),
        out_shape=jax.ShapeDtypeStruct((tokens, width), BF16),
    )(rank, places, returned, layer_cot)


def shifted(x, axis, by):
    count = lax.axis_size(axis)
    return lax.ppermute(x, axis, [(i, (i + by) % count) for i in range(count)])


def gathered(x):
    half = x.shape[0] // 2
    before, after = (shifted(x, "tp", 1), shifted(x, "tp", -1))
    return x, after, shifted(before[:half], "tp", 1), shifted(after[half:], "tp", -1), before


def reduced(after, across, before):
    half = after.shape[0] // 2
    from_before = shifted(across[:half], "tp", 1)
    from_after = shifted(across[half:], "tp", -1)
    add = lambda a, b: (a.astype(F32) + b.astype(F32)).astype(BF16)
    to_after = jnp.concatenate([add(after[:half], from_before), after[half:]], axis=0)
    to_before = jnp.concatenate([before[:half], add(before[half:], from_after)], axis=0)
    return shifted(to_after, "tp", 1), shifted(to_before, "tp", -1)


def exchanged(x, axis):
    return lax.all_to_all(x, axis, split_axis=0, concat_axis=0, tiled=True)


def summed_over(x, axis):
    parts = [shifted(x[k], axis, k) for k in range(1, lax.axis_size(axis))]
    total = x[0].astype(F32)
    for part in parts:
        total = total + part.astype(F32)
    return total


def body(
    layer_cot,
    moe_input,
    routes,
    route_weights,
    gate_proj,
    up_proj,
    down_proj,
    out_proj,
    mixer_out,
    queries,
    key_rows,
    values,
    log_decay,
    saved_state,
):
    sp_count = lax.axis_size(SP)
    slots = sp_count * CAP
    tokens, model_width = layer_cot.shape
    quarter = model_width // 4
    hidden_units = gate_proj.shape[2]
    channels = queries.shape[1]
    cols = mixer_out.shape[1]
    rank = lax.axis_index("tp").astype(jnp.int32).reshape(1)
    ranks = jnp.stack([lax.axis_index(axis).astype(jnp.int32) for axis in ("tp", *SP)])
    gate_w, up_w, down_w = (gate_proj[0], up_proj[0], down_proj[0])
    by_span = lambda x: x.reshape(sp_count, CAP, x.shape[-1])
    by_slot = lambda x: x.reshape(slots, x.shape[-1])
    rows_in, rows_cot, places = routed(
        rank, routes.T, route_weights.T, moe_input, layer_cot, slots
    )
    down_part = (hidden_units, quarter)
    s0, s1, s2, s3 = call(parted_kernel, [(down_part, BF16)] * 4, down_w, ranks=ranks)
    d1, d2, d3 = (shifted(s3, "tp", -1), shifted(s2, "tp", 2), shifted(s1, "tp", 1))
    got_in = by_slot(exchanged(by_span(rows_in), SP))
    got_in, rows_cot, d1, d2, d3 = lax.optimization_barrier((got_in, rows_cot, d1, d2, d3))
    x = gathered(got_in)
    cot = by_slot(exchanged(by_span(rows_cot), SP))
    start, pieces = call(
        start_kernel, [((channels, tokens), BF16), ((channels, 3), BF16)], queries, log_decay
    )
    cot, start, pieces, *x = lax.optimization_barrier((cot, start, pieces, *x))
    rows = (slots, hidden_units)
    own, after, across, before = call(
        cot_kernel,
        [(rows, F32), (rows, BF16), (rows, BF16), (rows, BF16)],
        cot, s0, d1, d2, d3,
    )
    totals = pieces.T.reshape(3, sp_count, -1).transpose(1, 0, 2).reshape(sp_count, -1)
    totals = jnp.pad(totals, ((0, 0), (0, 128 - totals.shape[1])))
    left, right = reduced(after, across, before)
    hidden, to_gate, to_up = call(
        in_kernel, [(rows, BF16), (rows, F32), (rows, F32)], *x, gate_w, up_w, ranks=ranks, flops=2 * 10**9
    )
    left, right, hidden, totals = lax.optimization_barrier((left, right, hidden, totals))
    wide = (slots, quarter)
    both, own, after, across, before = call(
        grads_kernel,
        [((slots, 2 * hidden_units), BF16)] + [(wide, BF16)] * 4,
        own, left, right, to_gate, to_up, gate_w, up_w,
        ranks=ranks,
    )
    left, right = reduced(after, across, before)
    weight = (model_width, hidden_units)
    grad_gate, grad_up = call(
        weights_kernel, [(weight, BF16)] * 2, *x, both, ranks=ranks, flops=3 * 10**9
    )
    left, right, grad_gate, grad_up = lax.optimization_barrier((left, right, grad_gate, grad_up))
    summed = (own.astype(F32) + left.astype(F32) + right.astype(F32)).astype(BF16)
    summed, late_cot = lax.optimization_barrier((summed, cot))
    returned = by_slot(exchanged(by_span(summed), SP))
    c_before, c_after = (shifted(late_cot, "tp", 1), shifted(late_cot, "tp", -1))
    returned, c_before, c_after = lax.optimization_barrier((returned, c_before, c_after))
    mix = gathered(combined(rank, places.T, returned, layer_cot))
    out_grad, term = call(
        out_kernel,
        [((cols, tokens), BF16), ((channels, DV), BF16)],
        *mix, out_proj, start,
        ranks=ranks,
    )
    out_grad, term, mix, c_before, c_after = lax.optimization_barrier(
        (out_grad, term, mix, c_before, c_after)
    )
    terms = jnp.concatenate([term.reshape(sp_count, -1), totals], axis=1)
    terms = exchanged(terms.reshape(sp_count, 3, -1), SP)
    half = slots // 2
    c = (
        cot, c_after, shifted(c_before[:half], "tp", 1), shifted(c_after[half:], "tp", -1), c_before
    )
    x_count, z_count = (lax.axis_size(SP[1]), lax.axis_size(SP[0]))
    part = (x_count, z_count, model_width // sp_count, cols)
    mine, other = call(part_kernel, [(part, BF16)] * 2, *mix, mixer_out, ranks=ranks, flops=4 * 10**9)
    pair = (mine.astype(F32) + shifted(other, SP[2], 1).astype(F32)).astype(BF16)
    grad_outproj = summed_over(summed_over(pair, SP[1]).astype(BF16), SP[0])
    (laters,) = call(
        scan_kernel,
        [((sp_count, channels * DV // sp_count), BF16)],
        terms.reshape(sp_count, -1),
    )
    (grad_down,) = call(
        down_kernel,
        [(down_w.shape, BF16)],
        *c, hidden,
        ranks=ranks,
        flops=2 * 10**9,
    )
    from_later = exchanged(laters.reshape(sp_count, 2, -1), SP).reshape(channels, DV).astype(F32)
    from_later, grad_down = lax.optimization_barrier((from_later, grad_down))

    grad_queries, grad_keys, grad_values, grad_decay = call(
        mixer_kernel,
        [
            (queries.shape, BF16),
            (key_rows.shape, BF16),
            (values.shape, BF16),
            (log_decay.shape, F32),
        ],
        queries,
        key_rows,
        values,
        log_decay,
        out_grad,
        saved_state.reshape(channels, DV),
        from_later,
        scratch=(
            (channels, tokens),
            (channels, tokens),
            (values.shape[1], tokens),
            (channels, 1),
        ),
    )
    return (
        grad_gate[None],
        grad_up[None],
        grad_down[None],
        grad_outproj,
        grad_queries,
        grad_keys,
        grad_values,
        grad_decay,
    )


def solution(mesh):
    torus = Mesh(mesh.devices.reshape(8, 4, 2, mesh.shape["tp"]), ("sp_0", "sp_1", "sp_2", "tp"))
    return jax.shard_map(
        body,
        mesh=torus,
        in_specs=(
            P(SP, None),
            P(SP, None),
            P(SP, None),
            P(SP, None),
            P(SP, None, "tp"),
            P(SP, None, "tp"),
            P(SP, "tp", None),
            P("tp", None),
            P(SP, "tp"),
            P(SP, "tp"),
            P(SP, "tp"),
            P(SP, "tp"),
            P(SP, "tp"),
            P(SP, "tp", None, None),
        ),
        out_specs=(
            P(SP, None, "tp"),
            P(SP, None, "tp"),
            P(SP, "tp", None),
            P(SP, "tp"),
            P(SP, "tp"),
            P(SP, "tp"),
            P(SP, "tp"),
            P(SP, "tp"),
        ),
        check_vma=False,
    )
```

```python
import jax
import jax.numpy as jnp
from jax import lax
from jax.experimental import pallas as pl
from jax.experimental.pallas import tpu as pltpu
from jax.sharding import Mesh
from jax.sharding import PartitionSpec as P


KEY_CHANNELS = 32
DV = 64
BLOCK = 64
CAP = 12
SP = ("sp_0", "sp_1", "sp_2")
F32 = jnp.float32
BF16 = jnp.bfloat16


def dot(a, b, contract, dt=jnp.bfloat16):
    return lax.dot_general(
        a.astype(dt), b.astype(dt), (contract, ((), ())), preferred_element_type=jnp.float32
    )


NN = ((1,), (0,))
NT = ((1,), (1,))
TN = ((0,), (0,))


def summed_by(x, mask, pieces):
    total, rest = (None, x)
    for _ in range(pieces):
        part = rest.astype(jnp.bfloat16)
        rest = rest - part.astype(jnp.float32)
        term = dot(part, mask, NN)
        total = term if total is None else total + term
    return total


def triangle(length, keep):
    down = lax.broadcasted_iota(jnp.int32, (length, length), 0)
    across = lax.broadcasted_iota(jnp.int32, (length, length), 1)
    return jnp.where(keep(down, across), 1.0, 0.0).astype(jnp.bfloat16)


def route_kernel(rank_ref, routes_ref, weights_ref, in_ref, cot_ref, rows_in_ref, rows_cot_ref, places_ref):
    tokens = routes_ref.shape[1]
    slots = rows_in_ref.shape[0]
    experts = slots // CAP
    first, second = (routes_ref[0:1, :], routes_ref[1:2, :])
    expert_ids = lax.broadcasted_iota(jnp.int32, (experts, tokens), 0)
    named_first, named_second = (expert_ids == first, expert_ids == second)
    named = jnp.where(named_first | named_second, 1.0, 0.0)
    before = dot(named, triangle(tokens, lambda u, t: u < t), NN)

    def place(hit, route):
        rank = jnp.sum(jnp.where(hit, before, 0.0), axis=0, keepdims=True)
        return route * CAP + rank.astype(jnp.int32)

    place_a, place_b = (place(named_first, first), place(named_second, second))
    places_ref[0:1, :] = place_a
    places_ref[1:2, :] = place_b
    slot_ids = lax.broadcasted_iota(jnp.int32, (slots, tokens), 0)
    hit_a, hit_b = (slot_ids == place_a, slot_ids == place_b)
    chosen = jnp.where(hit_a | hit_b, 1.0, 0.0).astype(jnp.bfloat16)
    slot_weights = jnp.sum(
        jnp.where(hit_a, weights_ref[0:1, :], 0.0) + jnp.where(hit_b, weights_ref[1:2, :], 0.0),
        axis=1,
        keepdims=True,
    )
    rows_in_ref[...] = dot(chosen, in_ref[...], NN).astype(jnp.bfloat16)
    rows_cot_ref[...] = (slot_weights * dot(chosen, cot_ref[...], NN)).astype(jnp.bfloat16)


def combine_kernel(ranks_ref, places_ref, returned_ref, cot_ref, out_ref):
    tokens, slots = (cot_ref.shape[0], returned_ref.shape[0])
    slot_ids = lax.broadcasted_iota(jnp.int32, (tokens, slots), 1)
    hits = (slot_ids == places_ref[:, 0:1]) | (slot_ids == places_ref[:, 1:2])
    moe_grad = dot(jnp.where(hits, 1.0, 0.0), returned_ref[...], NN)
    out_ref[...] = (cot_ref[...].astype(F32) + moe_grad).astype(BF16)


def turned(x):
    return x.astype(jnp.float32).T


def start_kernel(q_ref, log_ref, start_ref, total_ref):
    tokens = q_ref.shape[0]
    cum = summed_by(turned(log_ref[...]), triangle(tokens, lambda u, t: u <= t), 3)
    rest = cum[:, tokens - 1 :]
    for k in range(3):
        piece = rest.astype(BF16)
        rest = rest - piece.astype(F32)
        total_ref[:, k : k + 1] = piece
    start_ref[...] = (turned(q_ref[...]) * jnp.exp(cum)).astype(BF16)


def mixer_kernel(
    q_ref, k_ref, v_ref, log_ref, grad_ref, state_ref, later_ref, gq_ref, gk_ref, gv_ref, gd_ref,
    dq_s, dk_s, dv_s, cross_s,
):
    tokens, channels = q_ref.shape
    half = tokens // 2
    cum = summed_by(turned(log_ref[...]), triangle(tokens, lambda u, t: u <= t), 3)
    q, k = (turned(q_ref[...]), turned(k_ref[...]))
    v = turned(v_ref[...]).astype(jnp.bfloat16)
    grad = grad_ref[...]
    lane = lax.broadcasted_iota(jnp.int32, (channels, tokens), 1)
    block = lane // BLOCK
    at = lambda t: cum[:, t : t + 1]
    near = jnp.where(
        block < 2,
        jnp.where(block == 0, at(31), at(95)),
        jnp.where(block == 2, at(159), at(223)),
    )
    wide = jnp.exp(-jnp.abs(cum - at(127)))
    mid = jnp.exp(-jnp.abs(cum - jnp.where(block < 2, at(63), at(191))))
    gap = cum - near
    up, down = (jnp.exp(gap), jnp.exp(-gap))
    start = jnp.exp(cum)
    end = jnp.exp(at(tokens - 1) - cum)
    whole = jnp.exp(at(tokens - 1))
    q_wide = jnp.where(block >= 2, q * wide, 0.0).astype(jnp.bfloat16)
    k_wide = jnp.where(block < 2, k * wide, 0.0).astype(jnp.bfloat16)
    q_mid, k_mid = ((q * mid), (k * mid))
    q_mids = [jnp.where(block == b, q_mid, 0.0).astype(jnp.bfloat16) for b in (1, 3)]
    k_mids = [jnp.where(block == b, k_mid, 0.0).astype(jnp.bfloat16) for b in (0, 2)]
    q_near, k_near = (q * up, k * down)
    q_nears = [jnp.where(block == b, q_near, 0.0).astype(jnp.bfloat16) for b in range(4)]
    k_nears = [jnp.where(block == b, k_near, 0.0).astype(jnp.bfloat16) for b in range(4)]
    q_parts = [q_wide, *q_mids, *q_nears]
    k_parts = [k_wide, *k_mids, *k_nears]
    k_end = (k * end).astype(jnp.bfloat16)
    down_ids = lax.broadcasted_iota(jnp.int32, (tokens, tokens), 0)
    across_ids = lax.broadcasted_iota(jnp.int32, (tokens, tokens), 1)
    causal = down_ids >= across_ids
    first64 = lax.broadcasted_iota(jnp.int32, (KEY_CHANNELS, half), 1) < BLOCK
    lo, hi = (slice(0, half), slice(half, tokens))
    kc = KEY_CHANNELS
    for h in range(channels // kc):
        ks, vs = (slice(h * kc, (h + 1) * kc), slice(h * DV, (h + 1) * DV))
        q_seg = jnp.concatenate([p[ks] for p in q_parts], axis=0)
        k_seg = jnp.concatenate([p[ks] for p in k_parts], axis=0)
        grad_h, v_h = (grad[vs], v[vs])
        scores = jnp.where(causal, dot(q_seg, k_seg, TN), 0.0).astype(jnp.bfloat16)
        coupl = jnp.where(causal, dot(grad_h, v_h, TN), 0.0).astype(jnp.bfloat16)
        to_q = dot(k_seg, coupl, NT)
        to_k = dot(q_seg, coupl, NN)
        seg = lambda x, i, side: x[i * kc : (i + 1) * kc, side]
        state = state_ref[ks, :]
        later = later_ref[ks, :]
        dq = start[ks] * dot(state, grad_h, NN)
        dk = end[ks] * dot(later, v_h, NN)
        dq_lo = up[ks, lo] * jnp.where(first64, seg(to_q, 3, lo), seg(to_q, 4, lo))
        dq_lo += mid[ks, lo] * jnp.where(first64, 0.0, seg(to_q, 1, lo))
        dq_hi = up[ks, hi] * jnp.where(first64, seg(to_q, 5, hi), seg(to_q, 6, hi))
        dq_hi += mid[ks, hi] * jnp.where(first64, 0.0, seg(to_q, 2, hi))
        dq_hi += wide[ks, hi] * seg(to_q, 0, hi)
        dk_lo = down[ks, lo] * jnp.where(first64, seg(to_k, 3, lo), seg(to_k, 4, lo))
        dk_lo += mid[ks, lo] * jnp.where(first64, seg(to_k, 1, lo), 0.0)
        dk_lo += wide[ks, lo] * seg(to_k, 0, lo)
        dk_hi = down[ks, hi] * jnp.where(first64, seg(to_k, 5, hi), seg(to_k, 6, hi))
        dk_hi += mid[ks, hi] * jnp.where(first64, seg(to_k, 2, hi), 0.0)
        dq_s[ks, :] = dq + jnp.concatenate([dq_lo, dq_hi], axis=1)
        dk_s[ks, :] = dk + jnp.concatenate([dk_lo, dk_hi], axis=1)
        dv_s[vs, :] = dot(grad_h, scores, NN) + dot(later, k_end[ks], TN)
        at_end = whole[ks] * state + dot(k_end[ks], v_h, NT)
        cross_s[ks, :] = jnp.sum(at_end * later, axis=1, keepdims=True)
    dq, dk = (dq_s[...], dk_s[...])
    change = q * dq - k * dk
    decay = summed_by(change, triangle(tokens, lambda u, t: u >= t), 2) + cross_s[...]
    gq_ref[...] = dq.T.astype(jnp.bfloat16)
    gk_ref[...] = dk.T.astype(jnp.bfloat16)
    gv_ref[...] = dv_s[...].T.astype(jnp.bfloat16)
    gd_ref[...] = decay.T


def scan_kernel(terms_ref, out_ref):
    spans, width = out_ref.shape
    channels = width // DV
    down_ids = lax.broadcasted_iota(jnp.int32, (spans, spans), 0)
    across_ids = lax.broadcasted_iota(jnp.int32, (spans, spans), 1)
    later = across_ids > down_ids
    up_to = jnp.where(down_ids >= across_ids, 1.0, 0.0)
    before = jnp.where(down_ids < across_ids, 1.0, 0.0)
    exact = lax.Precision.HIGHEST
    terms = terms_ref[...].astype(F32)
    pieces = [terms[:, width + k * channels : width + (k + 1) * channels] for k in range(3)]
    totals = pieces[0] + pieces[1] + pieces[2]
    through = jnp.dot(up_to, totals, precision=exact, preferred_element_type=F32)
    ahead = lax.dot_general(
        totals, before, (TN, ((), ())), precision=exact, preferred_element_type=F32
    )
    for c in range(channels):
        gap = ahead[c : c + 1, :] - through[:, c : c + 1]
        weight = jnp.where(later, jnp.exp(jnp.where(later, gap, 0.0)), 0.0)
        vs = slice(c * DV, (c + 1) * DV)
        out_ref[:, vs] = jnp.dot(
            weight, terms[:, vs], precision=exact, preferred_element_type=F32
        ).astype(out_ref.dtype)


def quarter_of(rank, k, width):
    return pl.ds(pl.multiple_of(lax.rem(rank + k, 4) * width, width), width)


def parted_kernel(ranks_ref, down_ref, *outs):
    width = down_ref.shape[1] // 4
    for k in range(4):
        outs[k][...] = down_ref[:, quarter_of(ranks_ref[0], k, width)]


def cot_kernel(cot_ref, d0, d1, d2, d3, own_ref, after_ref, a2_ref, a3_ref, before_ref):
    cot = cot_ref[...]
    half = a2_ref.shape[0]
    across = dot(cot, d2[...], NT).astype(BF16)
    a2_ref[...] = across[:half]
    a3_ref[...] = across[half:]
    after_ref[...] = dot(cot, d1[...], NT).astype(BF16)
    before_ref[...] = dot(cot, d3[...], NT).astype(BF16)
    own_ref[...] = dot(cot, d0[...], NT)


def in_kernel(ranks_ref, x0, x1, x2, x3, x4, gate_ref, up_ref, hidden_ref, to_gate_ref, to_up_ref):
    rank = ranks_ref[0]
    width = x0.shape[1]

    def product(w_ref):
        w = [w_ref[quarter_of(rank, k, width), :] for k in range(4)]
        across = jnp.concatenate([dot(x2[...], w[2], NN), dot(x3[...], w[2], NN)], axis=0)
        return dot(x0[...], w[0], NN) + dot(x1[...], w[1], NN) + across + dot(x4[...], w[3], NN)

    gate, up = (product(gate_ref), product(up_ref))
    sigmoid = jax.nn.sigmoid(gate)
    active = gate * sigmoid
    hidden_ref[...] = (active * up).astype(BF16)
    to_up_ref[...] = active
    to_gate_ref[...] = up * sigmoid * (1.0 + gate * (1.0 - sigmoid))


def grads_kernel(
    ranks_ref, own_ref, left_ref, right_ref, to_gate_ref, to_up_ref, gate_ref, up_ref,
    both_ref, p0, p1, p2, p3, p4,
):
    rank = ranks_ref[0]
    width = p0.shape[1]
    half = gate_ref.shape[1]
    grad_hidden = own_ref[...] + left_ref[...].astype(F32) + right_ref[...].astype(F32)
    both_ref[:, :half] = (grad_hidden * to_gate_ref[...]).astype(BF16)
    both_ref[:, half:] = (grad_hidden * to_up_ref[...]).astype(BF16)
    both = both_ref[...]
    rows = p2.shape[0]
    for k in (2, 1, 3, 0):
        at = quarter_of(rank, k, width)
        w = jnp.concatenate([gate_ref[at, :], up_ref[at, :]], axis=1)
        part = dot(both, w, NT).astype(BF16)
        if k == 2:
            p2[...] = part[:rows]
            p3[...] = part[rows:]
        else:
            (p0, p1, None, p4)[k][...] = part


def weights_kernel(ranks_ref, x0, x1, x2, x3, x4, both_ref, gate_ref, up_ref):
    rank = ranks_ref[0]
    width = x0.shape[1]
    half, rows = (gate_ref.shape[1], x2.shape[0])

    def put(k, grads):
        at = quarter_of(rank, k, width)
        gate_ref[at, :] = grads[:, :half].astype(BF16)
        up_ref[at, :] = grads[:, half:].astype(BF16)

    for k, x in ((0, x0), (1, x1), (3, x4)):
        put(k, dot(x[...], both_ref[...], TN))
    put(2, dot(x2[...], both_ref[:rows, :], TN) + dot(x3[...], both_ref[rows:, :], TN))


def down_kernel(ranks_ref, c0, c1, c2, c3, c4, hidden_ref, down_ref):
    rank = ranks_ref[0]
    width = c0.shape[1]
    rows = c2.shape[0]
    hidden = hidden_ref[...]
    for k, c in ((0, c0), (1, c1), (3, c4)):
        down_ref[:, quarter_of(rank, k, width)] = dot(hidden, c[...], TN).astype(BF16)
    across = dot(hidden[:rows], c2[...], TN) + dot(hidden[rows:], c3[...], TN)
    down_ref[:, quarter_of(rank, 2, width)] = across.astype(BF16)


def out_kernel(ranks_ref, m0, m1, m2, m3, m4, proj_ref, start_ref, grad_ref, term_ref):
    rank = ranks_ref[0]
    width = m0.shape[1]
    w = [proj_ref[:, quarter_of(rank, k, width)] for k in range(4)]
    across = jnp.concatenate([dot(w[2], m2[...], NT), dot(w[2], m3[...], NT)], axis=1)
    total = dot(w[0], m0[...], NT) + dot(w[1], m1[...], NT) + across + dot(w[3], m4[...], NT)
    grad = total.astype(BF16)
    grad_ref[...] = grad
    for h in range(start_ref.shape[0] // KEY_CHANNELS):
        ks, vs = (slice(h * KEY_CHANNELS, (h + 1) * KEY_CHANNELS), slice(h * DV, (h + 1) * DV))
        term_ref[ks, :] = dot(start_ref[ks, :], grad[vs], NT).astype(BF16)


def part_kernel(ranks_ref, m0, m1, m2, m3, m4, mixer_ref, mine_ref, other_ref):
    rank, z, x, core = (ranks_ref[k] for k in range(4))
    x_count, z_count, lines, _ = mine_ref.shape
    half = m2.shape[0]
    mixer = mixer_ref[...]

    def put(k, part):
        part = part.astype(BF16)
        quarter = lax.rem(rank + k, 4)
        per = z_count // 4
        for i in range(per * x_count):
            first = part[2 * i * lines : (2 * i + 1) * lines]
            second = part[(2 * i + 1) * lines : (2 * i + 2) * lines]
            to_z = lax.rem(quarter * per + i // x_count + z_count - z, z_count)
            to_x = lax.rem(i % x_count + x_count - x, x_count)
            mine_ref[to_x, to_z, :, :] = jnp.where(core == 0, first, second)
            other_ref[to_x, to_z, :, :] = jnp.where(core == 0, second, first)

    for k, m in ((0, m0), (1, m1), (3, m4)):
        put(k, dot(m[...], mixer, TN))
    put(2, dot(m2[...], mixer[:half], TN) + dot(m3[...], mixer[half:], TN))


def pair_kernel(mine_ref, swapped_ref, *outs):
    for k, out in enumerate(outs):
        out[...] = (mine_ref[k].astype(F32) + swapped_ref[k].astype(F32)).astype(BF16)


def row_kernel(*refs):
    count = refs[0].shape[0]
    lines, outs = (refs[:-count], refs[-count:])
    for z, out in enumerate(outs):
        total = lines[0][z].astype(F32)
        for line in lines[1:]:
            total = total + line[z].astype(F32)
        out[...] = total.astype(out.dtype)


def call(kernel, outs, *args, scratch=(), ranks=None, flops=None):
    specs = [pl.BlockSpec(memory_space=pltpu.VMEM) for _ in args]
    if ranks is not None:
        specs, args = ([pl.BlockSpec(memory_space=pltpu.SMEM), *specs], (ranks, *args))
    cost = flops and pl.CostEstimate(flops=flops, bytes_accessed=0, transcendentals=0)
    return pl.pallas_call(
        kernel,
        in_specs=specs,
        out_specs=[pl.BlockSpec(memory_space=pltpu.VMEM) for _ in outs],
        out_shape=[jax.ShapeDtypeStruct(shape, dtype) for shape, dtype in outs],
        scratch_shapes=[pltpu.VMEM(shape, F32) for shape in scratch],
        cost_estimate=cost,
    )(*args)


def routed(rank, routes, weights, moe_input, layer_cot, slots):
    tokens, width = layer_cot.shape
    part = width // 4
    whole = lambda shape: pl.BlockSpec(shape, lambda i, r: (0, 0))
    own = pl.BlockSpec((tokens, part), lambda i, r: (0, r[0]))
    return pl.pallas_call(
        route_kernel,
        grid_spec=pltpu.PrefetchScalarGridSpec(
            num_scalar_prefetch=1,
            grid=(1,),
            in_specs=[whole(routes.shape), whole(weights.shape), own, own],
            out_specs=[whole((slots, part)), whole((slots, part)), whole(routes.shape)],
        ),
        out_shape=[
            jax.ShapeDtypeStruct((slots, part), BF16),
            jax.ShapeDtypeStruct((slots, part), BF16),
            jax.ShapeDtypeStruct(routes.shape, jnp.int32),
        ],
    )(rank, routes, weights, moe_input, layer_cot)


def combined(rank, places, returned, layer_cot):
    tokens = layer_cot.shape[0]
    _, width = returned.shape
    whole = lambda shape: pl.BlockSpec(shape, lambda i, r: (0, 0))
    return pl.pallas_call(
        combine_kernel,
        grid_spec=pltpu.PrefetchScalarGridSpec(
            num_scalar_prefetch=1,
            grid=(1,),
            in_specs=[
                whole(places.shape),
                whole(returned.shape),
                pl.BlockSpec((tokens, width), lambda i, r: (0, r[0])),
            ],
            out_specs=whole((tokens, width)),
        ),
        out_shape=jax.ShapeDtypeStruct((tokens, width), BF16),
    )(rank, places, returned, layer_cot)


def shifted(x, axis, by):
    count = lax.axis_size(axis)
    return lax.ppermute(x, axis, [(i, (i + by) % count) for i in range(count)])


def gathered(x):
    half = x.shape[0] // 2
    before, after = (shifted(x, "tp", 1), shifted(x, "tp", -1))
    return x, after, shifted(before[:half], "tp", 1), shifted(after[half:], "tp", -1), before


def reduced(after, across_a, across_b, before):
    half = across_a.shape[0]
    from_before = shifted(across_a, "tp", 1)
    from_after = shifted(across_b, "tp", -1)
    add = lambda a, b: (a.astype(F32) + b.astype(F32)).astype(BF16)
    to_after = after.at[:half].set(add(after[:half], from_before))
    to_before = before.at[half:].set(add(before[half:], from_after))
    return shifted(to_after, "tp", 1), shifted(to_before, "tp", -1)


def exchanged(x, axis):
    return lax.all_to_all(x, axis, split_axis=0, concat_axis=0, tiled=True)


def body(
    layer_cot,
    moe_input,
    routes,
    route_weights,
    gate_proj,
    up_proj,
    down_proj,
    out_proj,
    mixer_out,
    queries,
    key_rows,
    values,
    log_decay,
    saved_state,
):
    sp_count = lax.axis_size(SP)
    slots = sp_count * CAP
    tokens, model_width = layer_cot.shape
    quarter = model_width // 4
    hidden_units = gate_proj.shape[2]
    channels = queries.shape[1]
    cols = mixer_out.shape[1]
    rank = lax.axis_index("tp").astype(jnp.int32).reshape(1)
    ranks = jnp.stack([lax.axis_index(axis).astype(jnp.int32) for axis in ("tp", *SP)])
    gate_w, up_w, down_w = (gate_proj[0], up_proj[0], down_proj[0])
    by_span = lambda x: x.reshape(sp_count, CAP, x.shape[-1])
    by_slot = lambda x: x.reshape(slots, x.shape[-1])
    rows_in, rows_cot, places = routed(
        rank, routes.T, route_weights.T, moe_input, layer_cot, slots
    )
    down_part = (hidden_units, quarter)
    s0, s1, s2, s3 = call(parted_kernel, [(down_part, BF16)] * 4, down_w, ranks=ranks)
    d1, d2, d3 = (shifted(s3, "tp", -1), shifted(s2, "tp", 2), shifted(s1, "tp", 1))
    got_in = by_slot(exchanged(by_span(rows_in), SP))
    got_in, rows_cot, d1, d2, d3 = lax.optimization_barrier((got_in, rows_cot, d1, d2, d3))
    x = gathered(got_in)
    cot = by_slot(exchanged(by_span(rows_cot), SP))
    start, pieces = call(
        start_kernel, [((channels, tokens), BF16), ((channels, 3), BF16)], queries, log_decay
    )
    cot, start, pieces, *x = lax.optimization_barrier((cot, start, pieces, *x))
    rows = (slots, hidden_units)
    half = slots // 2
    piece = (half, hidden_units)
    own, *parts = call(
        cot_kernel,
        [(rows, F32), (rows, BF16), (piece, BF16), (piece, BF16), (rows, BF16)],
        cot, s0, d1, d2, d3,
    )
    totals = pieces.T.reshape(3, sp_count, -1).transpose(1, 0, 2).reshape(sp_count, -1)
    totals = jnp.pad(totals, ((0, 0), (0, 128 - totals.shape[1])))
    left, right = reduced(*parts)
    hidden, to_gate, to_up = call(
        in_kernel, [(rows, BF16), (rows, F32), (rows, F32)], *x, gate_w, up_w, ranks=ranks, flops=2 * 10**9
    )
    left, right, hidden, totals = lax.optimization_barrier((left, right, hidden, totals))
    wide = (slots, quarter)
    piece = (half, quarter)
    both, own, *parts = call(
        grads_kernel,
        [((slots, 2 * hidden_units), BF16)]
        + [(shape, BF16) for shape in (wide, wide, piece, piece, wide)],
        own, left, right, to_gate, to_up, gate_w, up_w,
        ranks=ranks,
    )
    left, right = reduced(*parts)
    weight = (model_width, hidden_units)
    grad_gate, grad_up = call(
        weights_kernel, [(weight, BF16)] * 2, *x, both, ranks=ranks, flops=3 * 10**9
    )
    left, right, grad_gate, grad_up = lax.optimization_barrier((left, right, grad_gate, grad_up))
    summed = (own.astype(F32) + left.astype(F32) + right.astype(F32)).astype(BF16)
    returned = by_slot(exchanged(by_span(summed), SP))
    mix = gathered(combined(rank, places.T, returned, layer_cot))
    out_grad, term = call(
        out_kernel,
        [((cols, tokens), BF16), ((channels, DV), BF16)],
        *mix, out_proj, start,
        ranks=ranks,
    )
    terms = jnp.concatenate([term.reshape(sp_count, -1), totals], axis=1)
    terms, mix, out_grad, cot = lax.optimization_barrier((terms, mix, out_grad, cot))
    c_before, c_after = (shifted(cot, "tp", 1), shifted(cot, "tp", -1))
    terms = exchanged(terms.reshape(sp_count, 3, -1), SP)
    x_count, z_count = (lax.axis_size(SP[1]), lax.axis_size(SP[0]))
    part = (x_count, z_count, model_width // sp_count, cols)
    mine, other = call(
        part_kernel, [(part, BF16)] * 2, *mix, mixer_out, ranks=ranks, flops=4 * 10**9
    )
    swapped = shifted(other, SP[2], 1)
    line = part[1:]
    pairs = call(pair_kernel, [(line, BF16)] * x_count, mine, swapped)
    lines = [shifted(pairs[k], SP[1], k) for k in range(1, x_count)]
    (laters,) = call(
        scan_kernel,
        [((sp_count, channels * DV // sp_count), BF16)],
        terms.reshape(sp_count, -1),
    )
    laters, c_before, c_after = lax.optimization_barrier((laters, c_before, c_after))
    c = (shifted(c_before[:half], "tp", 1), shifted(c_after[half:], "tp", -1))
    c = (cot, c_after, *c, c_before)
    laters = exchanged(laters.reshape(sp_count, 2, -1), SP)
    rows = call(row_kernel, [(line[1:], F32)] + [(line[1:], BF16)] * (z_count - 1), pairs[0], *lines)
    grad_outproj = rows[0]
    for got in [shifted(rows[k], SP[0], k) for k in range(1, z_count)]:
        grad_outproj = grad_outproj + got.astype(F32)
    from_later = laters.reshape(channels, DV).astype(F32)
    (grad_down,) = call(
        down_kernel, [(down_w.shape, BF16)], *c, hidden, ranks=ranks, flops=2 * 10**9
    )
    from_later, grad_outproj, grad_down = lax.optimization_barrier(
        (from_later, grad_outproj, grad_down)
    )

    grad_queries, grad_keys, grad_values, grad_decay = call(
        mixer_kernel,
        [
            (queries.shape, BF16),
            (key_rows.shape, BF16),
            (values.shape, BF16),
            (log_decay.shape, F32),
        ],
        queries,
        key_rows,
        values,
        log_decay,
        out_grad,
        saved_state.reshape(channels, DV),
        from_later,
        scratch=(
            (channels, tokens),
            (channels, tokens),
            (values.shape[1], tokens),
            (channels, 1),
        ),
    )
    return (
        grad_gate[None],
        grad_up[None],
        grad_down[None],
        grad_outproj,
        grad_queries,
        grad_keys,
        grad_values,
        grad_decay,
    )


def solution(mesh):
    torus = Mesh(mesh.devices.reshape(8, 4, 2, mesh.shape["tp"]), ("sp_0", "sp_1", "sp_2", "tp"))

    return jax.shard_map(
        body,
        mesh=torus,
        in_specs=(
            P(SP, None),
            P(SP, None),
            P(SP, None),
            P(SP, None),
            P(SP, None, "tp"),
            P(SP, None, "tp"),
            P(SP, "tp", None),
            P("tp", None),
            P(SP, "tp"),
            P(SP, "tp"),
            P(SP, "tp"),
            P(SP, "tp"),
            P(SP, "tp"),
            P(SP, "tp", None, None),
        ),
        out_specs=(
            P(SP, None, "tp"),
            P(SP, None, "tp"),
            P(SP, "tp", None),
            P(SP, "tp"),
            P(SP, "tp"),
            P(SP, "tp"),
            P(SP, "tp"),
            P(SP, "tp"),
        ),
        check_vma=False,
    )
```

```python
import jax
import jax.numpy as jnp
from jax import lax
from jax.experimental import pallas as pl
from jax.experimental.pallas import tpu as pltpu
from jax.sharding import Mesh
from jax.sharding import PartitionSpec as P


KEY_CHANNELS = 32
DV = 64
BLOCK = 64
CAP = 12
SP = ("sp_0", "sp_1", "sp_2")
F32 = jnp.float32
BF16 = jnp.bfloat16


def dot(a, b, contract, dt=jnp.bfloat16):
    return lax.dot_general(
        a.astype(dt), b.astype(dt), (contract, ((), ())), preferred_element_type=jnp.float32
    )


NN = ((1,), (0,))
NT = ((1,), (1,))
TN = ((0,), (0,))


def summed_by(x, mask, pieces):
    total, rest = (None, x)
    for _ in range(pieces):
        part = rest.astype(jnp.bfloat16)
        rest = rest - part.astype(jnp.float32)
        term = dot(part, mask, NN)
        total = term if total is None else total + term
    return total


def triangle(length, keep):
    down = lax.broadcasted_iota(jnp.int32, (length, length), 0)
    across = lax.broadcasted_iota(jnp.int32, (length, length), 1)
    return jnp.where(keep(down, across), 1.0, 0.0).astype(jnp.bfloat16)


def route_kernel(rank_ref, routes_ref, weights_ref, in_ref, cot_ref, in_out, cot_out, places_ref):
    tokens = routes_ref.shape[1]
    experts = in_out.shape[0]
    routes = [routes_ref[k : k + 1, :] for k in range(2)]
    weights = [weights_ref[k : k + 1, :] for k in range(2)]
    expert_ids = lax.broadcasted_iota(jnp.int32, (experts, tokens), 0)
    named = [expert_ids == route for route in routes]
    before = dot(
        jnp.where(named[0] | named[1], 1.0, 0.0), triangle(tokens, lambda u, t: u < t), NN
    )
    low, high = ([], [])
    for k in range(2):
        slot = jnp.sum(jnp.where(named[k], before, 0.0), axis=0, keepdims=True).astype(jnp.int32)
        low.append(jnp.where(slot < 8, routes[k] * 8 + slot, -8))
        high.append(jnp.where(slot < 8, -8, routes[k] * 8 + slot - 8))
        places_ref[k : k + 1, :] = low[k]
        places_ref[k + 2 : k + 3, :] = high[k]
    row = lax.broadcasted_iota(jnp.int32, (experts * 8, tokens), 0)
    upper = (row & 4) == 4
    hits_low = [row == low[k] for k in range(2)]
    hits_high = [(row - jnp.where(upper, 4, 0)) == high[k] for k in range(2)]

    def chosen(hits):
        weight = jnp.where(hits[0], weights[0], 0.0) + jnp.where(hits[1], weights[1], 0.0)
        return (
            jnp.where(hits[0] | hits[1], 1.0, 0.0).astype(BF16),
            jnp.sum(weight, axis=1, keepdims=True),
        )

    picks = (chosen(hits_low), chosen(hits_high))
    first = lax.broadcasted_iota(jnp.int32, (experts * 8, 128), 0) & 4
    for x_ref, out, weighted in ((in_ref, in_out, False), (cot_ref, cot_out, True)):
        x = x_ref[...]
        got = [dot(hot, x, NN) * (weight if weighted else 1.0) for hot, weight in picks]
        blocks = x.shape[1] // 128
        lanes = lambda g, i: g[:, i * 128 : (i + 1) * 128]
        for i in range(blocks):
            out[:, i * 8 : (i + 1) * 8, :] = lanes(got[0], i).astype(BF16).reshape(experts, 8, 128)
        for i in range(0, blocks, 2):
            at = blocks * 8 + i * 4
            pair = jnp.where(first == 0, lanes(got[1], i), lanes(got[1], i + 1))
            out[:, at : at + 8, :] = pair.astype(BF16).reshape(experts, 8, 128)


def unpack_kernel(got_ref, out_ref):
    spans = got_ref.shape[0]
    blocks = out_ref.shape[1] // 128
    low = spans * 8
    lanes = lambda i: slice(i * 128, (i + 1) * 128)
    for i in range(blocks):
        out_ref[:low, lanes(i)] = got_ref[:, i * 8 : (i + 1) * 8, :].reshape(low, 128)
    first = lax.broadcasted_iota(jnp.int32, (spans // 2, 8, 128), 1) < 4
    for i in range(0, blocks, 2):
        at = blocks * 8 + i * 4
        pair = got_ref[:, at : at + 8, :].astype(F32).reshape(spans // 2, 2, 8, 128)
        a, b = (pair[:, 0], pair[:, 1])
        even = jnp.where(first, a, pltpu.roll(b, 4, 1))
        odd = jnp.where(first, pltpu.roll(a, 4, 1), b)
        out_ref[low:, lanes(i)] = even.reshape(low // 2, 128).astype(BF16)
        out_ref[low:, lanes(i + 1)] = odd.reshape(low // 2, 128).astype(BF16)


def pack_kernel(own_ref, left_ref, right_ref, out_ref):
    spans = out_ref.shape[0]
    blocks = own_ref.shape[1] // 128
    low = spans * 8
    total = lambda rows, i: sum(
        ref[rows, i * 128 : (i + 1) * 128].astype(F32) for ref in (own_ref, left_ref, right_ref)
    )
    for i in range(blocks):
        rows = total(slice(0, low), i).astype(BF16)
        out_ref[:, i * 8 : (i + 1) * 8, :] = rows.reshape(spans, 8, 128)
    first = lax.broadcasted_iota(jnp.int32, (spans // 2, 8, 128), 1) < 4
    for i in range(0, blocks, 2):
        at = blocks * 8 + i * 4
        even, odd = (total(slice(low, low + low // 2), j).reshape(spans // 2, 8, 128) for j in (i, i + 1))
        a = jnp.where(first, even, pltpu.roll(odd, 4, 1))
        b = jnp.where(first, pltpu.roll(even, 4, 1), odd)
        pair = jnp.stack([a, b], axis=1).reshape(spans, 8, 128)
        out_ref[:, at : at + 8, :] = pair.astype(BF16)


def combine_kernel(ranks_ref, places_ref, returned_ref, cot_ref, out_ref):
    tokens = cot_ref.shape[0]
    experts = returned_ref.shape[0]
    blocks = cot_ref.shape[1] // 128
    row = lax.broadcasted_iota(jnp.int32, (tokens, experts * 8), 1)
    place = [places_ref[:, k : k + 1] for k in range(4)]
    hot = lambda a, b: jnp.where((row == a) | (row == b), 1.0, 0.0).astype(BF16)
    low = hot(place[0], place[1])
    high = (hot(place[2], place[3]), hot(place[2] + 4, place[3] + 4))
    flat = lambda at: returned_ref[:, at : at + 8, :].reshape(experts * 8, 128)
    for i in range(blocks):
        moe_grad = dot(low, flat(i * 8), NN)
        moe_grad += dot(high[i % 2], flat(blocks * 8 + (i // 2) * 8), NN)
        lanes = slice(i * 128, (i + 1) * 128)
        out_ref[:, lanes] = (cot_ref[:, lanes].astype(F32) + moe_grad).astype(BF16)


def turned(x):
    return x.astype(jnp.float32).T


def start_kernel(q_ref, log_ref, start_ref, total_ref):
    tokens = q_ref.shape[0]
    cum = summed_by(turned(log_ref[...]), triangle(tokens, lambda u, t: u <= t), 3)
    rest = cum[:, tokens - 1 :]
    for k in range(3):
        piece = rest.astype(BF16)
        rest = rest - piece.astype(F32)
        total_ref[:, k : k + 1] = piece
    start_ref[...] = (turned(q_ref[...]) * jnp.exp(cum)).astype(BF16)


def mixer_kernel(
    q_ref, k_ref, v_ref, log_ref, grad_ref, state_ref, later_ref, gq_ref, gk_ref, gv_ref, gd_ref,
    dq_s, dk_s, dv_s, cross_s,
):
    tokens, channels = q_ref.shape
    half = tokens // 2
    cum = summed_by(turned(log_ref[...]), triangle(tokens, lambda u, t: u <= t), 3)
    q, k = (turned(q_ref[...]), turned(k_ref[...]))
    v = turned(v_ref[...]).astype(jnp.bfloat16)
    grad = grad_ref[...]
    lane = lax.broadcasted_iota(jnp.int32, (channels, tokens), 1)
    block = lane // BLOCK
    at = lambda t: cum[:, t : t + 1]
    near = jnp.where(
        block < 2,
        jnp.where(block == 0, at(31), at(95)),
        jnp.where(block == 2, at(159), at(223)),
    )
    wide = jnp.exp(-jnp.abs(cum - at(127)))
    mid = jnp.exp(-jnp.abs(cum - jnp.where(block < 2, at(63), at(191))))
    gap = cum - near
    up, down = (jnp.exp(gap), jnp.exp(-gap))
    start = jnp.exp(cum)
    end = jnp.exp(at(tokens - 1) - cum)
    whole = jnp.exp(at(tokens - 1))
    q_wide = jnp.where(block >= 2, q * wide, 0.0).astype(jnp.bfloat16)
    k_wide = jnp.where(block < 2, k * wide, 0.0).astype(jnp.bfloat16)
    q_mid, k_mid = ((q * mid), (k * mid))
    q_mids = [jnp.where(block == b, q_mid, 0.0).astype(jnp.bfloat16) for b in (1, 3)]
    k_mids = [jnp.where(block == b, k_mid, 0.0).astype(jnp.bfloat16) for b in (0, 2)]
    q_near, k_near = (q * up, k * down)
    q_nears = [jnp.where(block == b, q_near, 0.0).astype(jnp.bfloat16) for b in range(4)]
    k_nears = [jnp.where(block == b, k_near, 0.0).astype(jnp.bfloat16) for b in range(4)]
    q_parts = [q_wide, *q_mids, *q_nears]
    k_parts = [k_wide, *k_mids, *k_nears]
    k_end = (k * end).astype(jnp.bfloat16)
    down_ids = lax.broadcasted_iota(jnp.int32, (tokens, tokens), 0)
    across_ids = lax.broadcasted_iota(jnp.int32, (tokens, tokens), 1)
    causal = down_ids >= across_ids
    first64 = lax.broadcasted_iota(jnp.int32, (KEY_CHANNELS, half), 1) < BLOCK
    lo, hi = (slice(0, half), slice(half, tokens))
    kc = KEY_CHANNELS
    for h in range(channels // kc):
        ks, vs = (slice(h * kc, (h + 1) * kc), slice(h * DV, (h + 1) * DV))
        q_seg = jnp.concatenate([p[ks] for p in q_parts], axis=0)
        k_seg = jnp.concatenate([p[ks] for p in k_parts], axis=0)
        grad_h, v_h = (grad[vs], v[vs])
        scores = jnp.where(causal, dot(q_seg, k_seg, TN), 0.0).astype(jnp.bfloat16)
        coupl = jnp.where(causal, dot(grad_h, v_h, TN), 0.0).astype(jnp.bfloat16)
        to_q = dot(k_seg, coupl, NT)
        to_k = dot(q_seg, coupl, NN)
        seg = lambda x, i, side: x[i * kc : (i + 1) * kc, side]
        state = state_ref[ks, :]
        later = later_ref[ks, :]
        dq = start[ks] * dot(state, grad_h, NN)
        dk = end[ks] * dot(later, v_h, NN)
        dq_lo = up[ks, lo] * jnp.where(first64, seg(to_q, 3, lo), seg(to_q, 4, lo))
        dq_lo += mid[ks, lo] * jnp.where(first64, 0.0, seg(to_q, 1, lo))
        dq_hi = up[ks, hi] * jnp.where(first64, seg(to_q, 5, hi), seg(to_q, 6, hi))
        dq_hi += mid[ks, hi] * jnp.where(first64, 0.0, seg(to_q, 2, hi))
        dq_hi += wide[ks, hi] * seg(to_q, 0, hi)
        dk_lo = down[ks, lo] * jnp.where(first64, seg(to_k, 3, lo), seg(to_k, 4, lo))
        dk_lo += mid[ks, lo] * jnp.where(first64, seg(to_k, 1, lo), 0.0)
        dk_lo += wide[ks, lo] * seg(to_k, 0, lo)
        dk_hi = down[ks, hi] * jnp.where(first64, seg(to_k, 5, hi), seg(to_k, 6, hi))
        dk_hi += mid[ks, hi] * jnp.where(first64, seg(to_k, 2, hi), 0.0)
        dq_s[ks, :] = dq + jnp.concatenate([dq_lo, dq_hi], axis=1)
        dk_s[ks, :] = dk + jnp.concatenate([dk_lo, dk_hi], axis=1)
        dv_s[vs, :] = dot(grad_h, scores, NN) + dot(later, k_end[ks], TN)
        at_end = whole[ks] * state + dot(k_end[ks], v_h, NT)
        cross_s[ks, :] = jnp.sum(at_end * later, axis=1, keepdims=True)
    dq, dk = (dq_s[...], dk_s[...])
    change = q * dq - k * dk
    decay = summed_by(change, triangle(tokens, lambda u, t: u >= t), 2) + cross_s[...]
    gq_ref[...] = dq.T.astype(jnp.bfloat16)
    gk_ref[...] = dk.T.astype(jnp.bfloat16)
    gv_ref[...] = dv_s[...].T.astype(jnp.bfloat16)
    gd_ref[...] = decay.T


def scan_kernel(terms_ref, out_ref):
    spans, width = out_ref.shape
    channels = width // DV
    down_ids = lax.broadcasted_iota(jnp.int32, (spans, spans), 0)
    across_ids = lax.broadcasted_iota(jnp.int32, (spans, spans), 1)
    later = across_ids > down_ids
    up_to = jnp.where(down_ids >= across_ids, 1.0, 0.0)
    before = jnp.where(down_ids < across_ids, 1.0, 0.0)
    exact = lax.Precision.HIGHEST
    terms = terms_ref[...].astype(F32)
    pieces = [terms[:, width + k * channels : width + (k + 1) * channels] for k in range(3)]
    totals = pieces[0] + pieces[1] + pieces[2]
    through = jnp.dot(up_to, totals, precision=exact, preferred_element_type=F32)
    ahead = lax.dot_general(
        totals, before, (TN, ((), ())), precision=exact, preferred_element_type=F32
    )
    for c in range(channels):
        gap = ahead[c : c + 1, :] - through[:, c : c + 1]
        weight = jnp.where(later, jnp.exp(jnp.where(later, gap, 0.0)), 0.0)
        vs = slice(c * DV, (c + 1) * DV)
        out_ref[:, vs] = jnp.dot(
            weight, terms[:, vs], precision=exact, preferred_element_type=F32
        ).astype(out_ref.dtype)


def quarter_of(rank, k, width):
    return pl.ds(pl.multiple_of(lax.rem(rank + k, 4) * width, width), width)


def parted_kernel(ranks_ref, down_ref, *outs):
    width = down_ref.shape[1] // 4
    for k in range(4):
        outs[k][...] = down_ref[:, quarter_of(ranks_ref[0], k, width)]


def cot_kernel(cot_ref, d0, d1, d2, d3, own_ref, after_ref, a2_ref, a3_ref, before_ref):
    cot = cot_ref[...]
    half = a2_ref.shape[0]
    across = dot(cot, d2[...], NT).astype(BF16)
    a2_ref[...] = across[:half]
    a3_ref[...] = across[half:]
    after_ref[...] = dot(cot, d1[...], NT).astype(BF16)
    before_ref[...] = dot(cot, d3[...], NT).astype(BF16)
    own_ref[...] = dot(cot, d0[...], NT)


def in_kernel(ranks_ref, x0, x1, x2, x3, x4, gate_ref, up_ref, hidden_ref, to_gate_ref, to_up_ref):
    rank = ranks_ref[0]
    width = x0.shape[1]

    def product(w_ref):
        w = [w_ref[quarter_of(rank, k, width), :] for k in range(4)]
        across = jnp.concatenate([dot(x2[...], w[2], NN), dot(x3[...], w[2], NN)], axis=0)
        return dot(x0[...], w[0], NN) + dot(x1[...], w[1], NN) + across + dot(x4[...], w[3], NN)

    gate, up = (product(gate_ref), product(up_ref))
    sigmoid = jax.nn.sigmoid(gate)
    active = gate * sigmoid
    hidden_ref[...] = (active * up).astype(BF16)
    to_up_ref[...] = active
    to_gate_ref[...] = up * sigmoid * (1.0 + gate * (1.0 - sigmoid))


def grads_kernel(
    ranks_ref, own_ref, left_ref, right_ref, to_gate_ref, to_up_ref, gate_ref, up_ref,
    both_ref, p0, p1, p2, p3, p4,
):
    rank = ranks_ref[0]
    width = p0.shape[1]
    half = gate_ref.shape[1]
    grad_hidden = own_ref[...] + left_ref[...].astype(F32) + right_ref[...].astype(F32)
    both_ref[:, :half] = (grad_hidden * to_gate_ref[...]).astype(BF16)
    both_ref[:, half:] = (grad_hidden * to_up_ref[...]).astype(BF16)
    both = both_ref[...]
    rows = p2.shape[0]
    for k in (2, 1, 3, 0):
        at = quarter_of(rank, k, width)
        w = jnp.concatenate([gate_ref[at, :], up_ref[at, :]], axis=1)
        part = dot(both, w, NT).astype(BF16)
        if k == 2:
            p2[...] = part[:rows]
            p3[...] = part[rows:]
        else:
            (p0, p1, None, p4)[k][...] = part


def weights_kernel(ranks_ref, x0, x1, x2, x3, x4, both_ref, gate_ref, up_ref):
    rank = ranks_ref[0]
    width = x0.shape[1]
    half, rows = (gate_ref.shape[1], x2.shape[0])

    def put(k, grads):
        at = quarter_of(rank, k, width)
        gate_ref[at, :] = grads[:, :half].astype(BF16)
        up_ref[at, :] = grads[:, half:].astype(BF16)

    for k, x in ((0, x0), (1, x1), (3, x4)):
        put(k, dot(x[...], both_ref[...], TN))
    put(2, dot(x2[...], both_ref[:rows, :], TN) + dot(x3[...], both_ref[rows:, :], TN))


def down_kernel(ranks_ref, c0, c1, c2, c3, c4, hidden_ref, down_ref):
    rank = ranks_ref[0]
    width = c0.shape[1]
    rows = c2.shape[0]
    hidden = hidden_ref[...]
    for k, c in ((0, c0), (1, c1), (3, c4)):
        down_ref[:, quarter_of(rank, k, width)] = dot(hidden, c[...], TN).astype(BF16)
    across = dot(hidden[:rows], c2[...], TN) + dot(hidden[rows:], c3[...], TN)
    down_ref[:, quarter_of(rank, 2, width)] = across.astype(BF16)


def out_kernel(ranks_ref, m0, m1, m2, m3, m4, proj_ref, start_ref, grad_ref, term_ref):
    rank = ranks_ref[0]
    width = m0.shape[1]
    w = [proj_ref[:, quarter_of(rank, k, width)] for k in range(4)]
    across = jnp.concatenate([dot(w[2], m2[...], NT), dot(w[2], m3[...], NT)], axis=1)
    total = dot(w[0], m0[...], NT) + dot(w[1], m1[...], NT) + across + dot(w[3], m4[...], NT)
    grad = total.astype(BF16)
    grad_ref[...] = grad
    for h in range(start_ref.shape[0] // KEY_CHANNELS):
        ks, vs = (slice(h * KEY_CHANNELS, (h + 1) * KEY_CHANNELS), slice(h * DV, (h + 1) * DV))
        term_ref[ks, :] = dot(start_ref[ks, :], grad[vs], NT).astype(BF16)


def part_kernel(ranks_ref, m0, m1, m2, m3, m4, mixer_ref, mine_ref, other_ref):
    rank, x, core = (ranks_ref[k] for k in (0, 2, 3))
    x_count, z_count, lines, _ = mine_ref.shape
    half = m2.shape[0]
    mixer = mixer_ref[...]

    def put(k, part):
        part = part.astype(BF16)
        quarter = lax.rem(rank + k, 4)
        per = z_count // 4
        for i in range(per * x_count):
            first = part[2 * i * lines : (2 * i + 1) * lines]
            second = part[(2 * i + 1) * lines : (2 * i + 2) * lines]
            to_z = quarter * per + i // x_count
            to_x = lax.rem(i % x_count + x_count - x, x_count)
            mine_ref[to_x, to_z, :, :] = jnp.where(core == 0, first, second)
            other_ref[to_x, to_z, :, :] = jnp.where(core == 0, second, first)

    for k, m in ((0, m0), (1, m1), (3, m4)):
        put(k, dot(m[...], mixer, TN))
    put(2, dot(m2[...], mixer[:half], TN) + dot(m3[...], mixer[half:], TN))


def pair_kernel(mine_ref, swapped_ref, *outs):
    for k, out in enumerate(outs):
        out[...] = (mine_ref[k].astype(F32) + swapped_ref[k].astype(F32)).astype(BF16)


def row_kernel(*refs):
    total = refs[0][...].astype(F32)
    for ref in refs[1:-1]:
        total = total + ref[...].astype(F32)
    refs[-1][...] = total.astype(BF16)


def call(kernel, outs, *args, scratch=(), ranks=None, flops=None):
    specs = [pl.BlockSpec(memory_space=pltpu.VMEM) for _ in args]
    if ranks is not None:
        specs, args = ([pl.BlockSpec(memory_space=pltpu.SMEM), *specs], (ranks, *args))
    cost = flops and pl.CostEstimate(flops=flops, bytes_accessed=0, transcendentals=0)
    return pl.pallas_call(
        kernel,
        in_specs=specs,
        out_specs=[pl.BlockSpec(memory_space=pltpu.VMEM) for _ in outs],
        out_shape=[jax.ShapeDtypeStruct(shape, dtype) for shape, dtype in outs],
        scratch_shapes=[pltpu.VMEM(shape, F32) for shape in scratch],
        cost_estimate=cost,
    )(*args)


def routed(rank, routes, weights, moe_input, layer_cot, experts):
    tokens, width = layer_cot.shape
    part = width // 4
    whole = lambda shape: pl.BlockSpec(shape, lambda i, r: (0,) * len(shape))
    own = pl.BlockSpec((tokens, part), lambda i, r: (0, r[0]))
    chunk = (experts, CAP * part // 128, 128)
    places = (4, tokens)
    return pl.pallas_call(
        route_kernel,
        grid_spec=pltpu.PrefetchScalarGridSpec(
            num_scalar_prefetch=1,
            grid=(1,),
            in_specs=[whole(routes.shape), whole(weights.shape), own, own],
            out_specs=[whole(chunk), whole(chunk), whole(places)],
        ),
        out_shape=[
            jax.ShapeDtypeStruct(chunk, BF16),
            jax.ShapeDtypeStruct(chunk, BF16),
            jax.ShapeDtypeStruct(places, jnp.int32),
        ],
    )(rank, routes, weights, moe_input, layer_cot)


def combined(rank, places, returned, layer_cot):
    tokens, width = layer_cot.shape
    part = width // 4
    whole = lambda shape: pl.BlockSpec(shape, lambda i, r: (0,) * len(shape))
    return pl.pallas_call(
        combine_kernel,
        grid_spec=pltpu.PrefetchScalarGridSpec(
            num_scalar_prefetch=1,
            grid=(1,),
            in_specs=[
                whole(places.shape),
                whole(returned.shape),
                pl.BlockSpec((tokens, part), lambda i, r: (0, r[0])),
            ],
            out_specs=whole((tokens, part)),
        ),
        out_shape=jax.ShapeDtypeStruct((tokens, part), BF16),
    )(rank, places, returned, layer_cot)


def shifted(x, axis, by):
    count = lax.axis_size(axis)
    return lax.ppermute(x, axis, [(i, (i + by) % count) for i in range(count)])


def gathered(x):
    half = x.shape[0] // 2
    before, after = (shifted(x, "tp", 1), shifted(x, "tp", -1))
    return x, after, shifted(before[:half], "tp", 1), shifted(after[half:], "tp", -1), before


def reduced(after, across_a, across_b, before):
    half = across_a.shape[0]
    from_before = shifted(across_a, "tp", 1)
    from_after = shifted(across_b, "tp", -1)
    add = lambda a, b: (a.astype(F32) + b.astype(F32)).astype(BF16)
    to_after = after.at[:half].set(add(after[:half], from_before))
    to_before = before.at[half:].set(add(before[half:], from_after))
    return shifted(to_after, "tp", 1), shifted(to_before, "tp", -1)


def exchanged(x, axis):
    return lax.all_to_all(x, axis, split_axis=0, concat_axis=0, tiled=True)


def body(
    layer_cot,
    moe_input,
    routes,
    route_weights,
    gate_proj,
    up_proj,
    down_proj,
    out_proj,
    mixer_out,
    queries,
    key_rows,
    values,
    log_decay,
    saved_state,
):
    sp_count = lax.axis_size(SP)
    slots = sp_count * CAP
    tokens, model_width = layer_cot.shape
    quarter = model_width // 4
    hidden_units = gate_proj.shape[2]
    channels = queries.shape[1]
    cols = mixer_out.shape[1]
    rank = lax.axis_index("tp").astype(jnp.int32).reshape(1)
    ranks = jnp.stack([lax.axis_index(axis).astype(jnp.int32) for axis in ("tp", *SP)])
    gate_w, up_w, down_w = (gate_proj[0], up_proj[0], down_proj[0])
    wide = (slots, quarter)
    rows_in, rows_cot, places = routed(
        rank, routes.T, route_weights.T, moe_input, layer_cot, sp_count
    )

    def delivered(x):
        return call(unpack_kernel, [(wide, BF16)], exchanged(x, SP))[0]

    down_part = (hidden_units, quarter)
    s0, s1, s2, s3 = call(parted_kernel, [(down_part, BF16)] * 4, down_w, ranks=ranks)
    d1, d2, d3 = (shifted(s3, "tp", -1), shifted(s2, "tp", 2), shifted(s1, "tp", 1))
    got_in = delivered(rows_in)
    got_in, rows_cot, d1, d2, d3 = lax.optimization_barrier((got_in, rows_cot, d1, d2, d3))
    x = gathered(got_in)
    cot = delivered(rows_cot)
    start, pieces = call(
        start_kernel, [((channels, tokens), BF16), ((channels, 3), BF16)], queries, log_decay
    )
    cot, start, pieces, *x = lax.optimization_barrier((cot, start, pieces, *x))
    rows = (slots, hidden_units)
    half = slots // 2
    piece = (half, hidden_units)
    own, *parts = call(
        cot_kernel,
        [(rows, F32), (rows, BF16), (piece, BF16), (piece, BF16), (rows, BF16)],
        cot, s0, d1, d2, d3,
    )
    totals = pieces.T.reshape(3, sp_count, -1).transpose(1, 0, 2).reshape(sp_count, -1)
    totals = jnp.pad(totals, ((0, 0), (0, 128 - totals.shape[1])))
    left, right = reduced(*parts)
    hidden, to_gate, to_up = call(
        in_kernel, [(rows, BF16), (rows, F32), (rows, F32)], *x, gate_w, up_w, ranks=ranks, flops=2 * 10**9
    )
    left, right, hidden, totals = lax.optimization_barrier((left, right, hidden, totals))
    piece = (half, quarter)
    both, own, *parts = call(
        grads_kernel,
        [((slots, 2 * hidden_units), BF16)]
        + [(shape, BF16) for shape in (wide, wide, piece, piece, wide)],
        own, left, right, to_gate, to_up, gate_w, up_w,
        ranks=ranks,
    )
    left, right = reduced(*parts)
    weight = (model_width, hidden_units)
    grad_gate, grad_up = call(
        weights_kernel, [(weight, BF16)] * 2, *x, both, ranks=ranks, flops=3 * 10**9
    )
    left, right, grad_gate, grad_up = lax.optimization_barrier((left, right, grad_gate, grad_up))
    (packed,) = call(pack_kernel, [(rows_in.shape, BF16)], own, left, right)
    packed, cot = lax.optimization_barrier((packed, cot))
    returned = exchanged(packed, SP)
    c = gathered(cot)
    returned, *c = lax.optimization_barrier((returned, *c))
    mix = gathered(combined(rank, places.T, returned, layer_cot))
    out_grad, term = call(
        out_kernel,
        [((cols, tokens), BF16), ((channels, DV), BF16)],
        *mix, out_proj, start,
        ranks=ranks,
    )
    terms = jnp.concatenate([term.reshape(sp_count, -1), totals], axis=1)
    terms, mix, out_grad = lax.optimization_barrier((terms, mix, out_grad))
    terms = exchanged(terms.reshape(sp_count, 3, -1), SP)
    x_count, z_count = (lax.axis_size(SP[1]), lax.axis_size(SP[0]))
    part = (x_count, z_count, model_width // sp_count, cols)
    mine, other = call(
        part_kernel, [(part, BF16)] * 2, *mix, mixer_out, ranks=ranks, flops=4 * 10**9
    )
    swapped = shifted(other, SP[2], 1)
    line = part[1:]
    pairs = call(pair_kernel, [(line, BF16)] * x_count, mine, swapped)
    lines = [shifted(pairs[k], SP[1], k) for k in range(1, x_count)]
    (laters,) = call(
        scan_kernel,
        [((sp_count, channels * DV // sp_count), BF16)],
        terms.reshape(sp_count, -1),
    )
    laters = exchanged(laters.reshape(sp_count, 2, -1), SP)
    (row,) = call(row_kernel, [(line, BF16)], pairs[0], *lines)
    row = exchanged(row, SP[0])
    grad_outproj = jnp.sum(row.astype(F32), axis=0)
    from_later = laters.reshape(channels, DV).astype(F32)
    (grad_down,) = call(
        down_kernel, [(down_w.shape, BF16)], *c, hidden, ranks=ranks, flops=2 * 10**9
    )
    grad_queries, grad_keys, grad_values, grad_decay = call(
        mixer_kernel,
        [
            (queries.shape, BF16),
            (key_rows.shape, BF16),
            (values.shape, BF16),
            (log_decay.shape, F32),
        ],
        queries,
        key_rows,
        values,
        log_decay,
        out_grad,
        saved_state.reshape(channels, DV),
        from_later,
        scratch=((channels, tokens), (channels, tokens), (values.shape[1], tokens), (channels, 1)),
    )
    return (
        grad_gate[None],
        grad_up[None],
        grad_down[None],
        grad_outproj,
        grad_queries,
        grad_keys,
        grad_values,
        grad_decay,
    )


def solution(mesh):
    torus = Mesh(mesh.devices.reshape(8, 4, 2, mesh.shape["tp"]), ("sp_0", "sp_1", "sp_2", "tp"))

    return jax.shard_map(
        body,
        mesh=torus,
        in_specs=(
            P(SP, None),
            P(SP, None),
            P(SP, None),
            P(SP, None),
            P(SP, None, "tp"),
            P(SP, None, "tp"),
            P(SP, "tp", None),
            P("tp", None),
            P(SP, "tp"),
            P(SP, "tp"),
            P(SP, "tp"),
            P(SP, "tp"),
            P(SP, "tp"),
            P(SP, "tp", None, None),
        ),
        out_specs=(
            P(SP, None, "tp"),
            P(SP, None, "tp"),
            P(SP, "tp", None),
            P(SP, "tp"),
            P(SP, "tp"),
            P(SP, "tp"),
            P(SP, "tp"),
            P(SP, "tp"),
        ),
        check_vma=False,
    )
```

```python
import jax
import jax.numpy as jnp
from jax import lax
from jax.experimental import pallas as pl
from jax.experimental.pallas import tpu as pltpu
from jax.sharding import Mesh
from jax.sharding import PartitionSpec as P


KEY_CHANNELS = 32
DV = 64
BLOCK = 64
CAP = 12
SP = ("sp_0", "sp_1", "sp_2")
GRANT = 24 * 2**20
F32 = jnp.float32
BF16 = jnp.bfloat16


def dot(a, b, contract, dt=jnp.bfloat16):
    return lax.dot_general(
        a.astype(dt), b.astype(dt), (contract, ((), ())), preferred_element_type=jnp.float32
    )


NN = ((1,), (0,))
NT = ((1,), (1,))
TN = ((0,), (0,))


def summed_by(x, mask, pieces):
    total, rest = (None, x)
    for _ in range(pieces):
        part = rest.astype(jnp.bfloat16)
        rest = rest - part.astype(jnp.float32)
        term = dot(part, mask, NN)
        total = term if total is None else total + term
    return total


def triangle(length, keep):
    down = lax.broadcasted_iota(jnp.int32, (length, length), 0)
    across = lax.broadcasted_iota(jnp.int32, (length, length), 1)
    return jnp.where(keep(down, across), 1.0, 0.0).astype(jnp.bfloat16)


def route_kernel(rank_ref, routes_ref, weights_ref, in_ref, cot_ref, in_out, cot_out, places_ref):
    tokens = routes_ref.shape[1]
    experts = in_out.shape[0]
    routes = [routes_ref[k : k + 1, :] for k in range(2)]
    weights = [weights_ref[k : k + 1, :] for k in range(2)]
    expert_ids = lax.broadcasted_iota(jnp.int32, (experts, tokens), 0)
    named = [expert_ids == route for route in routes]
    before = dot(
        jnp.where(named[0] | named[1], 1.0, 0.0), triangle(tokens, lambda u, t: u < t), NN
    )
    low, high = ([], [])
    for k in range(2):
        slot = jnp.sum(jnp.where(named[k], before, 0.0), axis=0, keepdims=True).astype(jnp.int32)
        low.append(jnp.where(slot < 8, routes[k] * 8 + slot, -8))
        high.append(jnp.where(slot < 8, -8, routes[k] * 8 + slot - 8))
        places_ref[k : k + 1, :] = low[k]
        places_ref[k + 2 : k + 3, :] = high[k]
    row = lax.broadcasted_iota(jnp.int32, (experts * 8, tokens), 0)
    upper = (row & 4) == 4
    hits_low = [row == low[k] for k in range(2)]
    hits_high = [(row - jnp.where(upper, 4, 0)) == high[k] for k in range(2)]

    def chosen(hits):
        weight = jnp.where(hits[0], weights[0], 0.0) + jnp.where(hits[1], weights[1], 0.0)
        return (
            jnp.where(hits[0] | hits[1], 1.0, 0.0).astype(BF16),
            jnp.sum(weight, axis=1, keepdims=True),
        )

    picks = (chosen(hits_low), chosen(hits_high))
    first = lax.broadcasted_iota(jnp.int32, (experts * 8, 128), 0) & 4
    for x_ref, out, weighted in ((in_ref, in_out, False), (cot_ref, cot_out, True)):
        x = x_ref[...]
        got = [dot(hot, x, NN) * (weight if weighted else 1.0) for hot, weight in picks]
        blocks = x.shape[1] // 128
        lanes = lambda g, i: g[:, i * 128 : (i + 1) * 128]
        for i in range(blocks):
            out[:, i * 8 : (i + 1) * 8, :] = lanes(got[0], i).astype(BF16).reshape(experts, 8, 128)
        for i in range(0, blocks, 2):
            at = blocks * 8 + i * 4
            pair = jnp.where(first == 0, lanes(got[1], i), lanes(got[1], i + 1))
            out[:, at : at + 8, :] = pair.astype(BF16).reshape(experts, 8, 128)


def unpack_kernel(got_ref, out_ref):
    spans = got_ref.shape[0]
    blocks = out_ref.shape[1] // 128
    low = spans * 8
    lanes = lambda i: slice(i * 128, (i + 1) * 128)
    for i in range(blocks):
        out_ref[:low, lanes(i)] = got_ref[:, i * 8 : (i + 1) * 8, :].reshape(low, 128)
    first = lax.broadcasted_iota(jnp.int32, (spans // 2, 8, 128), 1) < 4
    for i in range(0, blocks, 2):
        at = blocks * 8 + i * 4
        pair = got_ref[:, at : at + 8, :].astype(F32).reshape(spans // 2, 2, 8, 128)
        a, b = (pair[:, 0], pair[:, 1])
        even = jnp.where(first, a, pltpu.roll(b, 4, 1))
        odd = jnp.where(first, pltpu.roll(a, 4, 1), b)
        out_ref[low:, lanes(i)] = even.reshape(low // 2, 128).astype(BF16)
        out_ref[low:, lanes(i + 1)] = odd.reshape(low // 2, 128).astype(BF16)


def pack_kernel(own_ref, left_ref, right_ref, out_ref):
    spans = out_ref.shape[0]
    blocks = own_ref.shape[1] // 128
    low = spans * 8
    total = lambda rows, i: sum(
        ref[rows, i * 128 : (i + 1) * 128].astype(F32) for ref in (own_ref, left_ref, right_ref)
    )
    for i in range(blocks):
        rows = total(slice(0, low), i).astype(BF16)
        out_ref[:, i * 8 : (i + 1) * 8, :] = rows.reshape(spans, 8, 128)
    first = lax.broadcasted_iota(jnp.int32, (spans // 2, 8, 128), 1) < 4
    for i in range(0, blocks, 2):
        at = blocks * 8 + i * 4
        even, odd = (total(slice(low, low + low // 2), j).reshape(spans // 2, 8, 128) for j in (i, i + 1))
        a = jnp.where(first, even, pltpu.roll(odd, 4, 1))
        b = jnp.where(first, pltpu.roll(even, 4, 1), odd)
        pair = jnp.stack([a, b], axis=1).reshape(spans, 8, 128)
        out_ref[:, at : at + 8, :] = pair.astype(BF16)


def combine_kernel(ranks_ref, places_ref, returned_ref, cot_ref, out_ref):
    tokens = cot_ref.shape[0]
    experts = returned_ref.shape[0]
    blocks = cot_ref.shape[1] // 128
    row = lax.broadcasted_iota(jnp.int32, (tokens, experts * 8), 1)
    place = [places_ref[:, k : k + 1] for k in range(4)]
    hot = lambda a, b: jnp.where((row == a) | (row == b), 1.0, 0.0).astype(BF16)
    low = hot(place[0], place[1])
    high = (hot(place[2], place[3]), hot(place[2] + 4, place[3] + 4))
    flat = lambda at: returned_ref[:, at : at + 8, :].reshape(experts * 8, 128)
    for i in range(blocks):
        moe_grad = dot(low, flat(i * 8), NN)
        moe_grad += dot(high[i % 2], flat(blocks * 8 + (i // 2) * 8), NN)
        lanes = slice(i * 128, (i + 1) * 128)
        out_ref[:, lanes] = (cot_ref[:, lanes].astype(F32) + moe_grad).astype(BF16)


def turned(x):
    return x.astype(jnp.float32).T


def start_kernel(q_ref, log_ref, start_ref, total_ref):
    tokens = q_ref.shape[0]
    cum = summed_by(turned(log_ref[...]), triangle(tokens, lambda u, t: u <= t), 3)
    rest = cum[:, tokens - 1 :]
    for k in range(3):
        piece = rest.astype(BF16)
        rest = rest - piece.astype(F32)
        total_ref[:, k : k + 1] = piece
    start_ref[...] = (turned(q_ref[...]) * jnp.exp(cum)).astype(BF16)


def mixer_kernel(
    q_ref, k_ref, v_ref, log_ref, grad_ref, state_ref, later_ref, gq_ref, gk_ref, gv_ref, gd_ref,
    dq_s, dk_s, dv_s, cross_s,
):
    tokens, channels = q_ref.shape
    half = tokens // 2
    cum = summed_by(turned(log_ref[...]), triangle(tokens, lambda u, t: u <= t), 3)
    q, k = (turned(q_ref[...]), turned(k_ref[...]))
    v = turned(v_ref[...]).astype(jnp.bfloat16)
    grad = grad_ref[...]
    lane = lax.broadcasted_iota(jnp.int32, (channels, tokens), 1)
    block = lane // BLOCK
    at = lambda t: cum[:, t : t + 1]
    near = jnp.where(
        block < 2,
        jnp.where(block == 0, at(31), at(95)),
        jnp.where(block == 2, at(159), at(223)),
    )
    wide = jnp.exp(-jnp.abs(cum - at(127)))
    mid = jnp.exp(-jnp.abs(cum - jnp.where(block < 2, at(63), at(191))))
    gap = cum - near
    up, down = (jnp.exp(gap), jnp.exp(-gap))
    start = jnp.exp(cum)
    end = jnp.exp(at(tokens - 1) - cum)
    whole = jnp.exp(at(tokens - 1))
    q_wide = jnp.where(block >= 2, q * wide, 0.0).astype(jnp.bfloat16)
    k_wide = jnp.where(block < 2, k * wide, 0.0).astype(jnp.bfloat16)
    q_mid, k_mid = ((q * mid), (k * mid))
    q_mids = [jnp.where(block == b, q_mid, 0.0).astype(jnp.bfloat16) for b in (1, 3)]
    k_mids = [jnp.where(block == b, k_mid, 0.0).astype(jnp.bfloat16) for b in (0, 2)]
    q_near, k_near = (q * up, k * down)
    q_nears = [jnp.where(block == b, q_near, 0.0).astype(jnp.bfloat16) for b in range(4)]
    k_nears = [jnp.where(block == b, k_near, 0.0).astype(jnp.bfloat16) for b in range(4)]
    q_parts = [q_wide, *q_mids, *q_nears]
    k_parts = [k_wide, *k_mids, *k_nears]
    k_end = (k * end).astype(jnp.bfloat16)
    down_ids = lax.broadcasted_iota(jnp.int32, (tokens, tokens), 0)
    across_ids = lax.broadcasted_iota(jnp.int32, (tokens, tokens), 1)
    causal = down_ids >= across_ids
    first64 = lax.broadcasted_iota(jnp.int32, (KEY_CHANNELS, half), 1) < BLOCK
    lo, hi = (slice(0, half), slice(half, tokens))
    kc = KEY_CHANNELS
    for h in range(channels // kc):
        ks, vs = (slice(h * kc, (h + 1) * kc), slice(h * DV, (h + 1) * DV))
        q_seg = jnp.concatenate([p[ks] for p in q_parts], axis=0)
        k_seg = jnp.concatenate([p[ks] for p in k_parts], axis=0)
        grad_h, v_h = (grad[vs], v[vs])
        scores = jnp.where(causal, dot(q_seg, k_seg, TN), 0.0).astype(jnp.bfloat16)
        coupl = jnp.where(causal, dot(grad_h, v_h, TN), 0.0).astype(jnp.bfloat16)
        to_q = dot(k_seg, coupl, NT)
        to_k = dot(q_seg, coupl, NN)
        seg = lambda x, i, side: x[i * kc : (i + 1) * kc, side]
        state = state_ref[ks, :]
        later = later_ref[ks, :]
        dq = start[ks] * dot(state, grad_h, NN)
        dk = end[ks] * dot(later, v_h, NN)
        dq_lo = up[ks, lo] * jnp.where(first64, seg(to_q, 3, lo), seg(to_q, 4, lo))
        dq_lo += mid[ks, lo] * jnp.where(first64, 0.0, seg(to_q, 1, lo))
        dq_hi = up[ks, hi] * jnp.where(first64, seg(to_q, 5, hi), seg(to_q, 6, hi))
        dq_hi += mid[ks, hi] * jnp.where(first64, 0.0, seg(to_q, 2, hi))
        dq_hi += wide[ks, hi] * seg(to_q, 0, hi)
        dk_lo = down[ks, lo] * jnp.where(first64, seg(to_k, 3, lo), seg(to_k, 4, lo))
        dk_lo += mid[ks, lo] * jnp.where(first64, seg(to_k, 1, lo), 0.0)
        dk_lo += wide[ks, lo] * seg(to_k, 0, lo)
        dk_hi = down[ks, hi] * jnp.where(first64, seg(to_k, 5, hi), seg(to_k, 6, hi))
        dk_hi += mid[ks, hi] * jnp.where(first64, seg(to_k, 2, hi), 0.0)
        dq_s[ks, :] = dq + jnp.concatenate([dq_lo, dq_hi], axis=1)
        dk_s[ks, :] = dk + jnp.concatenate([dk_lo, dk_hi], axis=1)
        dv_s[vs, :] = dot(grad_h, scores, NN) + dot(later, k_end[ks], TN)
        at_end = whole[ks] * state + dot(k_end[ks], v_h, NT)
        cross_s[ks, :] = jnp.sum(at_end * later, axis=1, keepdims=True)
    dq, dk = (dq_s[...], dk_s[...])
    change = q * dq - k * dk
    decay = summed_by(change, triangle(tokens, lambda u, t: u >= t), 2) + cross_s[...]
    gq_ref[...] = dq.T.astype(jnp.bfloat16)
    gk_ref[...] = dk.T.astype(jnp.bfloat16)
    gv_ref[...] = dv_s[...].T.astype(jnp.bfloat16)
    gd_ref[...] = decay.T


def scan_kernel(terms_ref, out_ref):
    spans, width = out_ref.shape
    channels = width // DV
    down_ids = lax.broadcasted_iota(jnp.int32, (spans, spans), 0)
    across_ids = lax.broadcasted_iota(jnp.int32, (spans, spans), 1)
    later = across_ids > down_ids
    up_to = jnp.where(down_ids >= across_ids, 1.0, 0.0)
    before = jnp.where(down_ids < across_ids, 1.0, 0.0)
    exact = lax.Precision.HIGHEST
    terms = terms_ref[...].astype(F32)
    pieces = [terms[:, width + k * channels : width + (k + 1) * channels] for k in range(3)]
    totals = pieces[0] + pieces[1] + pieces[2]
    through = jnp.dot(up_to, totals, precision=exact, preferred_element_type=F32)
    ahead = lax.dot_general(
        totals, before, (TN, ((), ())), precision=exact, preferred_element_type=F32
    )
    for c in range(channels):
        gap = ahead[c : c + 1, :] - through[:, c : c + 1]
        weight = jnp.where(later, jnp.exp(jnp.where(later, gap, 0.0)), 0.0)
        vs = slice(c * DV, (c + 1) * DV)
        out_ref[:, vs] = jnp.dot(
            weight, terms[:, vs], precision=exact, preferred_element_type=F32
        ).astype(out_ref.dtype)


def quarter_of(rank, k, width):
    return pl.ds(pl.multiple_of(lax.rem(rank + k, 4) * width, width), width)


def parted_kernel(ranks_ref, down_ref, *outs):
    width = down_ref.shape[1] // 4
    for k in range(4):
        outs[k][...] = down_ref[:, quarter_of(ranks_ref[0], k, width)]


def cot_kernel(got_ref, d2, cot_ref, a2_ref, a3_ref):
    unpack_kernel(got_ref, cot_ref)
    half = a2_ref.shape[0]
    a2_ref[...] = dot(cot_ref[:half, :], d2[...], NT).astype(BF16)
    a3_ref[...] = dot(cot_ref[half:, :], d2[...], NT).astype(BF16)


def rest_kernel(cot_ref, d0, d1, d3, own_ref, after_ref, before_ref):
    cot = cot_ref[...]
    after_ref[...] = dot(cot, d1[...], NT).astype(BF16)
    before_ref[...] = dot(cot, d3[...], NT).astype(BF16)
    own_ref[...] = dot(cot, d0[...], NT)


def in_kernel(ranks_ref, x0, x1, x2, x3, x4, gate_ref, up_ref, hidden_ref, to_gate_ref, to_up_ref):
    rank = ranks_ref[0]
    width = x0.shape[1]

    def product(w_ref):
        w = [w_ref[quarter_of(rank, k, width), :] for k in range(4)]
        across = jnp.concatenate([dot(x2[...], w[2], NN), dot(x3[...], w[2], NN)], axis=0)
        return dot(x0[...], w[0], NN) + dot(x1[...], w[1], NN) + across + dot(x4[...], w[3], NN)

    gate, up = (product(gate_ref), product(up_ref))
    sigmoid = jax.nn.sigmoid(gate)
    active = gate * sigmoid
    hidden_ref[...] = (active * up).astype(BF16)
    to_up_ref[...] = active
    to_gate_ref[...] = up * sigmoid * (1.0 + gate * (1.0 - sigmoid))


def rows_of(ranks_ref, k, width, gate_ref, up_ref):
    at = quarter_of(ranks_ref[0], k, width)
    return jnp.concatenate([gate_ref[at, :], up_ref[at, :]], axis=1)


def grads_kernel(
    ranks_ref, own_ref, left_ref, right_ref, to_gate_ref, to_up_ref, gate_ref, up_ref,
    both_ref, p2, p3,
):
    half = gate_ref.shape[1]
    grad_hidden = own_ref[...] + left_ref[...].astype(F32) + right_ref[...].astype(F32)
    both_ref[:, :half] = (grad_hidden * to_gate_ref[...]).astype(BF16)
    both_ref[:, half:] = (grad_hidden * to_up_ref[...]).astype(BF16)
    w = rows_of(ranks_ref, 2, p2.shape[1], gate_ref, up_ref)
    rows = p2.shape[0]
    p2[...] = dot(both_ref[:rows, :], w, NT).astype(BF16)
    p3[...] = dot(both_ref[rows:, :], w, NT).astype(BF16)


def parts_kernel(ranks_ref, both_ref, gate_ref, up_ref, p0, p1, p4):
    both = both_ref[...]
    for k, out in ((1, p1), (3, p4), (0, p0)):
        out[...] = dot(both, rows_of(ranks_ref, k, out.shape[1], gate_ref, up_ref), NT).astype(BF16)


def weights_kernel(ranks_ref, x0, x1, x2, x3, x4, both_ref, gate_ref, up_ref):
    rank = ranks_ref[0]
    width = x0.shape[1]
    half, rows = (gate_ref.shape[1], x2.shape[0])

    def put(k, grads):
        at = quarter_of(rank, k, width)
        gate_ref[at, :] = grads[:, :half].astype(BF16)
        up_ref[at, :] = grads[:, half:].astype(BF16)

    for k, x in ((0, x0), (1, x1), (3, x4)):
        put(k, dot(x[...], both_ref[...], TN))
    put(2, dot(x2[...], both_ref[:rows, :], TN) + dot(x3[...], both_ref[rows:, :], TN))


def down_kernel(ranks_ref, c0, c1, c2, c3, c4, hidden_ref, down_ref):
    rank = ranks_ref[0]
    width = c0.shape[1]
    rows = c2.shape[0]
    hidden = hidden_ref[...]
    for k, c in ((0, c0), (1, c1), (3, c4)):
        down_ref[:, quarter_of(rank, k, width)] = dot(hidden, c[...], TN).astype(BF16)
    across = dot(hidden[:rows], c2[...], TN) + dot(hidden[rows:], c3[...], TN)
    down_ref[:, quarter_of(rank, 2, width)] = across.astype(BF16)


def out_kernel(ranks_ref, m0, m1, m2, m3, m4, proj_ref, start_ref, grad_ref, term_ref):
    rank = ranks_ref[0]
    width = m0.shape[1]
    w = [proj_ref[:, quarter_of(rank, k, width)] for k in range(4)]
    across = jnp.concatenate([dot(w[2], m2[...], NT), dot(w[2], m3[...], NT)], axis=1)
    total = dot(w[0], m0[...], NT) + dot(w[1], m1[...], NT) + across + dot(w[3], m4[...], NT)
    grad = total.astype(BF16)
    grad_ref[...] = grad
    for h in range(start_ref.shape[0] // KEY_CHANNELS):
        ks, vs = (slice(h * KEY_CHANNELS, (h + 1) * KEY_CHANNELS), slice(h * DV, (h + 1) * DV))
        term_ref[ks, :] = dot(start_ref[ks, :], grad[vs], NT).astype(BF16)


def part_kernel(ranks_ref, m0, m1, m2, m3, m4, mixer_ref, mine_ref, other_ref):
    rank, x, core = (ranks_ref[k] for k in (0, 2, 3))
    x_count, z_count, lines, _ = mine_ref.shape
    half = m2.shape[0]
    mixer = mixer_ref[...]

    def put(k, part):
        part = part.astype(BF16)
        quarter = lax.rem(rank + k, 4)
        per = z_count // 4
        for i in range(per * x_count):
            first = part[2 * i * lines : (2 * i + 1) * lines]
            second = part[(2 * i + 1) * lines : (2 * i + 2) * lines]
            to_z = quarter * per + i // x_count
            to_x = lax.rem(i % x_count + x_count - x, x_count)
            mine_ref[to_x, to_z, :, :] = jnp.where(core == 0, first, second)
            other_ref[to_x, to_z, :, :] = jnp.where(core == 0, second, first)

    for k, m in ((0, m0), (1, m1), (3, m4)):
        put(k, dot(m[...], mixer, TN))
    put(2, dot(m2[...], mixer[:half], TN) + dot(m3[...], mixer[half:], TN))


def pair_kernel(mine_ref, swapped_ref, *outs):
    for k, out in enumerate(outs):
        out[...] = (mine_ref[k].astype(F32) + swapped_ref[k].astype(F32)).astype(BF16)


def row_kernel(*refs):
    total = refs[0][...].astype(F32)
    for ref in refs[1:-1]:
        total = total + ref[...].astype(F32)
    refs[-1][...] = total.astype(BF16)


def call(kernel, outs, *args, scratch=(), ranks=None, flops=None):
    specs = [pl.BlockSpec(memory_space=pltpu.VMEM) for _ in args]
    if ranks is not None:
        specs, args = ([pl.BlockSpec(memory_space=pltpu.SMEM), *specs], (ranks, *args))
    cost = flops and pl.CostEstimate(flops=flops, bytes_accessed=0, transcendentals=0)
    return pl.pallas_call(
        kernel,
        in_specs=specs,
        out_specs=[pl.BlockSpec(memory_space=pltpu.VMEM) for _ in outs],
        out_shape=[jax.ShapeDtypeStruct(shape, dtype) for shape, dtype in outs],
        scratch_shapes=[pltpu.VMEM(shape, F32) for shape in scratch],
        cost_estimate=cost,
        compiler_params=pltpu.CompilerParams(vmem_limit_bytes=GRANT),
    )(*args)


def routed(rank, routes, weights, moe_input, layer_cot, experts):
    tokens, width = layer_cot.shape
    part = width // 4
    whole = lambda shape: pl.BlockSpec(shape, lambda i, r: (0,) * len(shape))
    own = pl.BlockSpec((tokens, part), lambda i, r: (0, r[0]))
    chunk = (experts, CAP * part // 128, 128)
    places = (4, tokens)
    return pl.pallas_call(
        route_kernel,
        grid_spec=pltpu.PrefetchScalarGridSpec(
            num_scalar_prefetch=1,
            grid=(1,),
            in_specs=[whole(routes.shape), whole(weights.shape), own, own],
            out_specs=[whole(chunk), whole(chunk), whole(places)],
        ),
        out_shape=[
            jax.ShapeDtypeStruct(chunk, BF16),
            jax.ShapeDtypeStruct(chunk, BF16),
            jax.ShapeDtypeStruct(places, jnp.int32),
        ],
    )(rank, routes, weights, moe_input, layer_cot)


def combined(rank, places, returned, layer_cot):
    tokens, width = layer_cot.shape
    part = width // 4
    whole = lambda shape: pl.BlockSpec(shape, lambda i, r: (0,) * len(shape))
    return pl.pallas_call(
        combine_kernel,
        grid_spec=pltpu.PrefetchScalarGridSpec(
            num_scalar_prefetch=1,
            grid=(1,),
            in_specs=[
                whole(places.shape),
                whole(returned.shape),
                pl.BlockSpec((tokens, part), lambda i, r: (0, r[0])),
            ],
            out_specs=whole((tokens, part)),
        ),
        out_shape=jax.ShapeDtypeStruct((tokens, part), BF16),
        compiler_params=pltpu.CompilerParams(vmem_limit_bytes=GRANT),
    )(rank, places, returned, layer_cot)


def shifted(x, axis, by):
    count = lax.axis_size(axis)
    return lax.ppermute(x, axis, [(i, (i + by) % count) for i in range(count)])


def neighbours(x):
    return shifted(x, "tp", 1), shifted(x, "tp", -1)


def across(before, after):
    half = before.shape[0] // 2
    return shifted(before[:half], "tp", 1), shifted(after[half:], "tp", -1)


def gathered(x):
    before, after = neighbours(x)
    return x, after, *across(before, after), before


def reduced(after, before, from_before, from_after):
    half = from_before.shape[0]
    add = lambda a, b: (a.astype(F32) + b.astype(F32)).astype(BF16)
    to_after = after.at[:half].set(add(after[:half], from_before))
    to_before = before.at[half:].set(add(before[half:], from_after))
    return shifted(to_after, "tp", 1), shifted(to_before, "tp", -1)


def exchanged(x, axis):
    return lax.all_to_all(x, axis, split_axis=0, concat_axis=0, tiled=True)


def body(
    layer_cot,
    moe_input,
    routes,
    route_weights,
    gate_proj,
    up_proj,
    down_proj,
    out_proj,
    mixer_out,
    queries,
    key_rows,
    values,
    log_decay,
    saved_state,
):
    sp_count = lax.axis_size(SP)
    slots = sp_count * CAP
    tokens, model_width = layer_cot.shape
    quarter = model_width // 4
    hidden_units = gate_proj.shape[2]
    channels = queries.shape[1]
    cols = mixer_out.shape[1]
    rank = lax.axis_index("tp").astype(jnp.int32).reshape(1)
    ranks = jnp.stack([lax.axis_index(axis).astype(jnp.int32) for axis in ("tp", *SP)])
    gate_w, up_w, down_w = (gate_proj[0], up_proj[0], down_proj[0])
    wide = (slots, quarter)
    rows_in, rows_cot, places = routed(
        rank, routes.T, route_weights.T, moe_input, layer_cot, sp_count
    )

    down_part = (hidden_units, quarter)
    s0, s1, s2, s3 = call(parted_kernel, [(down_part, BF16)] * 4, down_w, ranks=ranks)
    d1, d2, d3 = (shifted(s3, "tp", -1), shifted(s2, "tp", 2), shifted(s1, "tp", 1))
    (got_in,) = call(unpack_kernel, [(wide, BF16)], exchanged(rows_in, SP))
    got_in, rows_cot, d1, d2, d3 = lax.optimization_barrier((got_in, rows_cot, d1, d2, d3))
    x = gathered(got_in)
    got_cot = exchanged(rows_cot, SP)
    rows = (slots, hidden_units)
    start, pieces = call(
        start_kernel, [((channels, tokens), BF16), ((channels, 3), BF16)], queries, log_decay
    )
    got_cot, start, pieces, *x = lax.optimization_barrier((got_cot, start, pieces, *x))
    rows = (slots, hidden_units)
    half = slots // 2
    piece = (half, hidden_units)
    cot, a2, a3 = call(
        cot_kernel, [(wide, BF16), (piece, BF16), (piece, BF16)], got_cot, d2
    )
    hops = (shifted(a2, "tp", 1), shifted(a3, "tp", -1))
    own, after, before = call(
        rest_kernel,
        [(rows, F32), (rows, BF16), (rows, BF16)],
        cot, s0, d1, d3,
        flops=10**9,
    )
    totals = pieces.T.reshape(3, sp_count, -1).transpose(1, 0, 2).reshape(sp_count, -1)
    totals = jnp.pad(totals, ((0, 0), (0, 128 - totals.shape[1])))
    left, right = reduced(after, before, *hops)
    hidden, to_gate, to_up = call(
        in_kernel, [(rows, BF16), (rows, F32), (rows, F32)], *x, gate_w, up_w, ranks=ranks, flops=2 * 10**9
    )
    left, right, hidden, totals = lax.optimization_barrier((left, right, hidden, totals))
    piece = (half, quarter)
    both, a2, a3 = call(
        grads_kernel,
        [((slots, 2 * hidden_units), BF16), (piece, BF16), (piece, BF16)],
        own, left, right, to_gate, to_up, gate_w, up_w,
        ranks=ranks,
    )
    hops = (shifted(a2, "tp", 1), shifted(a3, "tp", -1))
    own, after, before = call(
        parts_kernel, [(wide, BF16)] * 3, both, gate_w, up_w, ranks=ranks, flops=3 * 10**9
    )
    left, right = reduced(after, before, *hops)
    weight = (model_width, hidden_units)
    grad_gate, grad_up = call(
        weights_kernel, [(weight, BF16)] * 2, *x, both, ranks=ranks, flops=3 * 10**9
    )
    left, right, grad_gate, grad_up = lax.optimization_barrier((left, right, grad_gate, grad_up))
    (packed,) = call(pack_kernel, [(rows_in.shape, BF16)], own, left, right)
    packed, cot = lax.optimization_barrier((packed, cot))
    returned = exchanged(packed, SP)
    c_before, c_after = neighbours(cot)
    returned, c_before, c_after = lax.optimization_barrier((returned, c_before, c_after))
    mix = gathered(combined(rank, places.T, returned, layer_cot))
    out_grad, term = call(
        out_kernel,
        [((cols, tokens), BF16), ((channels, DV), BF16)],
        *mix, out_proj, start,
        ranks=ranks,
    )
    terms = jnp.concatenate([term.reshape(sp_count, -1), totals], axis=1)
    terms, mix, out_grad, c_before, c_after = lax.optimization_barrier(
        (terms, mix, out_grad, c_before, c_after)
    )
    c = (cot, c_after, *across(c_before, c_after), c_before)
    terms = exchanged(terms.reshape(sp_count, 3, -1), SP)
    x_count, z_count = (lax.axis_size(SP[1]), lax.axis_size(SP[0]))
    part = (x_count, z_count, model_width // sp_count, cols)
    mine, other = call(
        part_kernel, [(part, BF16)] * 2, *mix, mixer_out, ranks=ranks, flops=4 * 10**9
    )
    swapped = shifted(other, SP[2], 1)
    line = part[1:]
    pairs = call(pair_kernel, [(line, BF16)] * x_count, mine, swapped)
    lines = [shifted(pairs[k], SP[1], k) for k in range(1, x_count)]
    (laters,) = call(
        scan_kernel,
        [((sp_count, channels * DV // sp_count), BF16)],
        terms.reshape(sp_count, -1),
    )
    laters = exchanged(laters.reshape(sp_count, 2, -1), SP)
    (row,) = call(row_kernel, [(line, BF16)], pairs[0], *lines)
    row = exchanged(row, SP[0])
    grad_outproj = jnp.sum(row.astype(F32), axis=0)
    from_later = laters.reshape(channels, DV).astype(F32)
    (grad_down,) = call(
        down_kernel, [(down_w.shape, BF16)], *c, hidden, ranks=ranks, flops=2 * 10**9
    )
    grad_queries, grad_keys, grad_values, grad_decay = call(
        mixer_kernel,
        [
            (queries.shape, BF16),
            (key_rows.shape, BF16),
            (values.shape, BF16),
            (log_decay.shape, F32),
        ],
        queries,
        key_rows,
        values,
        log_decay,
        out_grad,
        saved_state.reshape(channels, DV),
        from_later,
        scratch=((channels, tokens), (channels, tokens), (values.shape[1], tokens), (channels, 1)),
    )
    return (
        grad_gate[None],
        grad_up[None],
        grad_down[None],
        grad_outproj,
        grad_queries,
        grad_keys,
        grad_values,
        grad_decay,
    )


def solution(mesh):
    torus = Mesh(mesh.devices.reshape(8, 4, 2, mesh.shape["tp"]), ("sp_0", "sp_1", "sp_2", "tp"))

    return jax.shard_map(
        body,
        mesh=torus,
        in_specs=(
            P(SP, None),
            P(SP, None),
            P(SP, None),
            P(SP, None),
            P(SP, None, "tp"),
            P(SP, None, "tp"),
            P(SP, "tp", None),
            P("tp", None),
            P(SP, "tp"),
            P(SP, "tp"),
            P(SP, "tp"),
            P(SP, "tp"),
            P(SP, "tp"),
            P(SP, "tp", None, None),
        ),
        out_specs=(
            P(SP, None, "tp"),
            P(SP, None, "tp"),
            P(SP, "tp", None),
            P(SP, "tp"),
            P(SP, "tp"),
            P(SP, "tp"),
            P(SP, "tp"),
            P(SP, "tp"),
        ),
        check_vma=False,
    )
```

```python
import jax
import jax.numpy as jnp
from jax import lax
from jax.experimental import pallas as pl
from jax.experimental.pallas import tpu as pltpu
from jax.sharding import Mesh
from jax.sharding import PartitionSpec as P


KEY_CHANNELS = 32
DV = 64
BLOCK = 64
CAP = 12
SP = ("sp_0", "sp_1", "sp_2")
GRANT = 24 * 2**20
F32 = jnp.float32
BF16 = jnp.bfloat16


def dot(a, b, contract, dt=jnp.bfloat16):
    return lax.dot_general(
        a.astype(dt), b.astype(dt), (contract, ((), ())), preferred_element_type=jnp.float32
    )


NN = ((1,), (0,))
NT = ((1,), (1,))
TN = ((0,), (0,))


def summed_by(x, mask, pieces):
    total, rest = (None, x)
    for _ in range(pieces):
        part = rest.astype(jnp.bfloat16)
        rest = rest - part.astype(jnp.float32)
        term = dot(part, mask, NN)
        total = term if total is None else total + term
    return total


def triangle(length, keep):
    down = lax.broadcasted_iota(jnp.int32, (length, length), 0)
    across = lax.broadcasted_iota(jnp.int32, (length, length), 1)
    return jnp.where(keep(down, across), 1.0, 0.0).astype(jnp.bfloat16)


def route_kernel(rank_ref, routes_ref, weights_ref, in_ref, cot_ref, in_out, cot_out, places_ref):
    tokens = routes_ref.shape[1]
    experts = in_out.shape[0]
    routes = [routes_ref[k : k + 1, :] for k in range(2)]
    weights = [weights_ref[k : k + 1, :] for k in range(2)]
    expert_ids = lax.broadcasted_iota(jnp.int32, (experts, tokens), 0)
    named = [expert_ids == route for route in routes]
    before = dot(
        jnp.where(named[0] | named[1], 1.0, 0.0), triangle(tokens, lambda u, t: u < t), NN
    )
    low, high = ([], [])
    for k in range(2):
        slot = jnp.sum(jnp.where(named[k], before, 0.0), axis=0, keepdims=True).astype(jnp.int32)
        low.append(jnp.where(slot < 8, routes[k] * 8 + slot, -8))
        high.append(jnp.where(slot < 8, -8, routes[k] * 8 + slot - 8))
        places_ref[k : k + 1, :] = low[k]
        places_ref[k + 2 : k + 3, :] = high[k]
    row = lax.broadcasted_iota(jnp.int32, (experts * 8, tokens), 0)
    upper = (row & 4) == 4
    hits_low = [row == low[k] for k in range(2)]
    hits_high = [(row - jnp.where(upper, 4, 0)) == high[k] for k in range(2)]

    def chosen(hits):
        weight = jnp.where(hits[0], weights[0], 0.0) + jnp.where(hits[1], weights[1], 0.0)
        return (
            jnp.where(hits[0] | hits[1], 1.0, 0.0).astype(BF16),
            jnp.sum(weight, axis=1, keepdims=True),
        )

    picks = (chosen(hits_low), chosen(hits_high))
    first = lax.broadcasted_iota(jnp.int32, (experts * 8, 128), 0) & 4
    for x_ref, out, weighted in ((in_ref, in_out, False), (cot_ref, cot_out, True)):
        x = x_ref[...]
        got = [dot(hot, x, NN) * (weight if weighted else 1.0) for hot, weight in picks]
        blocks = x.shape[1] // 128
        lanes = lambda g, i: g[:, i * 128 : (i + 1) * 128]
        for i in range(blocks):
            out[:, i * 8 : (i + 1) * 8, :] = lanes(got[0], i).astype(BF16).reshape(experts, 8, 128)
        for i in range(0, blocks, 2):
            at = blocks * 8 + i * 4
            pair = jnp.where(first == 0, lanes(got[1], i), lanes(got[1], i + 1))
            out[:, at : at + 8, :] = pair.astype(BF16).reshape(experts, 8, 128)


def unpack_kernel(got_ref, first_ref, second_ref):
    spans = got_ref.shape[0]
    blocks = first_ref.shape[1] // 128
    low, half = (spans * 8, first_ref.shape[0])
    first = lax.broadcasted_iota(jnp.int32, (spans // 2, 8, 128), 1) < 4
    for i in range(blocks):
        lanes = slice(i * 128, (i + 1) * 128)
        rows = got_ref[:, i * 8 : (i + 1) * 8, :].reshape(low, 128)
        first_ref[:, lanes] = rows[:half]
        second_ref[: low - half, lanes] = rows[half:]
    for i in range(0, blocks, 2):
        at = blocks * 8 + i * 4
        pair = got_ref[:, at : at + 8, :].astype(F32).reshape(spans // 2, 2, 8, 128)
        a, b = (pair[:, 0], pair[:, 1])
        even = jnp.where(first, a, pltpu.roll(b, 4, 1))
        odd = jnp.where(first, pltpu.roll(a, 4, 1), b)
        for j, x in ((i, even), (i + 1, odd)):
            lanes = slice(j * 128, (j + 1) * 128)
            second_ref[low - half :, lanes] = x.reshape(low // 2, 128).astype(BF16)


def pack_kernel(own_ref, left_a, left_b, right_a, right_b, out_ref):
    spans = out_ref.shape[0]
    blocks = own_ref.shape[1] // 128
    low = spans * 8
    totals = []
    for i in range(blocks):
        lanes = slice(i * 128, (i + 1) * 128)
        totals.append(
            own_ref[:, lanes].astype(F32)
            + joined(left_a, left_b, lanes)
            + joined(right_a, right_b, lanes)
        )
        rows = totals[i][:low].astype(BF16)
        out_ref[:, i * 8 : (i + 1) * 8, :] = rows.reshape(spans, 8, 128)
    first = lax.broadcasted_iota(jnp.int32, (spans // 2, 8, 128), 1) < 4
    for i in range(0, blocks, 2):
        at = blocks * 8 + i * 4
        even, odd = (totals[j][low:].reshape(spans // 2, 8, 128) for j in (i, i + 1))
        a = jnp.where(first, even, pltpu.roll(odd, 4, 1))
        b = jnp.where(first, pltpu.roll(even, 4, 1), odd)
        pair = jnp.stack([a, b], axis=1).reshape(spans, 8, 128)
        out_ref[:, at : at + 8, :] = pair.astype(BF16)


def combine_kernel(ranks_ref, places_ref, returned_ref, cot_ref, first_ref, second_ref):
    tokens = cot_ref.shape[0]
    experts = returned_ref.shape[0]
    blocks = cot_ref.shape[1] // 128
    row = lax.broadcasted_iota(jnp.int32, (tokens, experts * 8), 1)
    place = [places_ref[:, k : k + 1] for k in range(4)]
    hot = lambda a, b: jnp.where((row == a) | (row == b), 1.0, 0.0).astype(BF16)
    low = hot(place[0], place[1])
    high = (hot(place[2], place[3]), hot(place[2] + 4, place[3] + 4))
    flat = lambda at: returned_ref[:, at : at + 8, :].reshape(experts * 8, 128)
    for i in range(blocks):
        moe_grad = dot(low, flat(i * 8), NN)
        moe_grad += dot(high[i % 2], flat(blocks * 8 + (i // 2) * 8), NN)
        lanes = slice(i * 128, (i + 1) * 128)
        mix = (cot_ref[:, lanes].astype(F32) + moe_grad).astype(BF16)
        first_ref[:, lanes] = mix[: tokens // 2]
        second_ref[:, lanes] = mix[tokens // 2 :]


def turned(x):
    return x.astype(jnp.float32).T


def start_kernel(q_ref, log_ref, start_ref, total_ref):
    tokens = q_ref.shape[0]
    cum = summed_by(turned(log_ref[...]), triangle(tokens, lambda u, t: u <= t), 3)
    rest = cum[:, tokens - 1 :]
    for k in range(3):
        piece = rest.astype(BF16)
        rest = rest - piece.astype(F32)
        total_ref[:, k : k + 1] = piece
    start_ref[...] = (turned(q_ref[...]) * jnp.exp(cum)).astype(BF16)


def mixer_kernel(
    q_ref, k_ref, v_ref, log_ref, grad_ref, state_ref, later_ref, gq_ref, gk_ref, gv_ref, gd_ref,
    dq_s, dk_s, dv_s, cross_s,
):
    tokens, channels = q_ref.shape
    half = tokens // 2
    cum = summed_by(turned(log_ref[...]), triangle(tokens, lambda u, t: u <= t), 3)
    q, k = (turned(q_ref[...]), turned(k_ref[...]))
    v = turned(v_ref[...]).astype(jnp.bfloat16)
    grad = grad_ref[...]
    lane = lax.broadcasted_iota(jnp.int32, (channels, tokens), 1)
    block = lane // BLOCK
    at = lambda t: cum[:, t : t + 1]
    near = jnp.where(
        block < 2,
        jnp.where(block == 0, at(31), at(95)),
        jnp.where(block == 2, at(159), at(223)),
    )
    wide = jnp.exp(-jnp.abs(cum - at(127)))
    mid = jnp.exp(-jnp.abs(cum - jnp.where(block < 2, at(63), at(191))))
    gap = cum - near
    up, down = (jnp.exp(gap), jnp.exp(-gap))
    start = jnp.exp(cum)
    end = jnp.exp(at(tokens - 1) - cum)
    whole = jnp.exp(at(tokens - 1))
    q_wide = jnp.where(block >= 2, q * wide, 0.0).astype(jnp.bfloat16)
    k_wide = jnp.where(block < 2, k * wide, 0.0).astype(jnp.bfloat16)
    q_mid, k_mid = ((q * mid), (k * mid))
    q_mids = [jnp.where(block == b, q_mid, 0.0).astype(jnp.bfloat16) for b in (1, 3)]
    k_mids = [jnp.where(block == b, k_mid, 0.0).astype(jnp.bfloat16) for b in (0, 2)]
    q_near, k_near = (q * up, k * down)
    q_nears = [jnp.where(block == b, q_near, 0.0).astype(jnp.bfloat16) for b in range(4)]
    k_nears = [jnp.where(block == b, k_near, 0.0).astype(jnp.bfloat16) for b in range(4)]
    q_parts = [q_wide, *q_mids, *q_nears]
    k_parts = [k_wide, *k_mids, *k_nears]
    k_end = (k * end).astype(jnp.bfloat16)
    down_ids = lax.broadcasted_iota(jnp.int32, (tokens, tokens), 0)
    across_ids = lax.broadcasted_iota(jnp.int32, (tokens, tokens), 1)
    causal = down_ids >= across_ids
    first64 = lax.broadcasted_iota(jnp.int32, (KEY_CHANNELS, half), 1) < BLOCK
    lo, hi = (slice(0, half), slice(half, tokens))
    kc = KEY_CHANNELS
    for h in range(channels // kc):
        ks, vs = (slice(h * kc, (h + 1) * kc), slice(h * DV, (h + 1) * DV))
        q_seg = jnp.concatenate([p[ks] for p in q_parts], axis=0)
        k_seg = jnp.concatenate([p[ks] for p in k_parts], axis=0)
        grad_h, v_h = (grad[vs], v[vs])
        scores = jnp.where(causal, dot(q_seg, k_seg, TN), 0.0).astype(jnp.bfloat16)
        coupl = jnp.where(causal, dot(grad_h, v_h, TN), 0.0).astype(jnp.bfloat16)
        to_q = dot(k_seg, coupl, NT)
        to_k = dot(q_seg, coupl, NN)
        seg = lambda x, i, side: x[i * kc : (i + 1) * kc, side]
        state = state_ref[ks, :]
        later = later_ref[ks, :]
        dq = start[ks] * dot(state, grad_h, NN)
        dk = end[ks] * dot(later, v_h, NN)
        dq_lo = up[ks, lo] * jnp.where(first64, seg(to_q, 3, lo), seg(to_q, 4, lo))
        dq_lo += mid[ks, lo] * jnp.where(first64, 0.0, seg(to_q, 1, lo))
        dq_hi = up[ks, hi] * jnp.where(first64, seg(to_q, 5, hi), seg(to_q, 6, hi))
        dq_hi += mid[ks, hi] * jnp.where(first64, 0.0, seg(to_q, 2, hi))
        dq_hi += wide[ks, hi] * seg(to_q, 0, hi)
        dk_lo = down[ks, lo] * jnp.where(first64, seg(to_k, 3, lo), seg(to_k, 4, lo))
        dk_lo += mid[ks, lo] * jnp.where(first64, seg(to_k, 1, lo), 0.0)
        dk_lo += wide[ks, lo] * seg(to_k, 0, lo)
        dk_hi = down[ks, hi] * jnp.where(first64, seg(to_k, 5, hi), seg(to_k, 6, hi))
        dk_hi += mid[ks, hi] * jnp.where(first64, seg(to_k, 2, hi), 0.0)
        dq_s[ks, :] = dq + jnp.concatenate([dq_lo, dq_hi], axis=1)
        dk_s[ks, :] = dk + jnp.concatenate([dk_lo, dk_hi], axis=1)
        dv_s[vs, :] = dot(grad_h, scores, NN) + dot(later, k_end[ks], TN)
        at_end = whole[ks] * state + dot(k_end[ks], v_h, NT)
        cross_s[ks, :] = jnp.sum(at_end * later, axis=1, keepdims=True)
    dq, dk = (dq_s[...], dk_s[...])
    change = q * dq - k * dk
    decay = summed_by(change, triangle(tokens, lambda u, t: u >= t), 2) + cross_s[...]
    gq_ref[...] = dq.T.astype(jnp.bfloat16)
    gk_ref[...] = dk.T.astype(jnp.bfloat16)
    gv_ref[...] = dv_s[...].T.astype(jnp.bfloat16)
    gd_ref[...] = decay.T


def scan_kernel(terms_ref, out_ref):
    spans, width = out_ref.shape
    channels = width // DV
    down_ids = lax.broadcasted_iota(jnp.int32, (spans, spans), 0)
    across_ids = lax.broadcasted_iota(jnp.int32, (spans, spans), 1)
    later = across_ids > down_ids
    up_to = jnp.where(down_ids >= across_ids, 1.0, 0.0)
    before = jnp.where(down_ids < across_ids, 1.0, 0.0)
    exact = lax.Precision.HIGHEST
    terms = terms_ref[...].astype(F32)
    pieces = [terms[:, width + k * channels : width + (k + 1) * channels] for k in range(3)]
    totals = pieces[0] + pieces[1] + pieces[2]
    through = jnp.dot(up_to, totals, precision=exact, preferred_element_type=F32)
    ahead = lax.dot_general(
        totals, before, (TN, ((), ())), precision=exact, preferred_element_type=F32
    )
    for c in range(channels):
        gap = ahead[c : c + 1, :] - through[:, c : c + 1]
        weight = jnp.where(later, jnp.exp(jnp.where(later, gap, 0.0)), 0.0)
        vs = slice(c * DV, (c + 1) * DV)
        out_ref[:, vs] = jnp.dot(
            weight, terms[:, vs], precision=exact, preferred_element_type=F32
        ).astype(out_ref.dtype)


def quarter_of(rank, k, width):
    return pl.ds(pl.multiple_of(lax.rem(rank + k, 4) * width, width), width)


def parted_kernel(ranks_ref, down_ref, *outs):
    width = down_ref.shape[1] // 4
    for k in range(4):
        outs[k][...] = down_ref[:, quarter_of(ranks_ref[0], k, width)]


def cot_kernel(got_ref, d2, cot_a, cot_b, a2_ref, a3_ref):
    unpack_kernel(got_ref, cot_a, cot_b)
    a2_ref[...] = dot(cot_a[...], d2[...], NT).astype(BF16)
    a3_ref[...] = dot(cot_b[...], d2[...], NT).astype(BF16)


def halves(part, first_ref, second_ref):
    part = part.astype(BF16)
    rows = first_ref.shape[0]
    first_ref[...] = part[:rows]
    second_ref[...] = part[rows:]


def rest_kernel(cot_a, cot_b, d0, d1, d3, own_ref, after_a, after_b, before_a, before_b):
    half = cot_a.shape[0]
    own_ref[:half, :] = dot(cot_a[...], d0[...], NT)
    own_ref[half:, :] = dot(cot_b[...], d0[...], NT)
    for cot, after, before in ((cot_a, after_a, before_a), (cot_b, after_b, before_b)):
        after[...] = dot(cot[...], d1[...], NT).astype(BF16)
        before[...] = dot(cot[...], d3[...], NT).astype(BF16)


def joined(a_ref, b_ref, lanes=slice(None)):
    return jnp.concatenate([a_ref[:, lanes], b_ref[:, lanes]], axis=0).astype(F32)


def in_kernel(ranks_ref, x0, x1, x2, x3, x4, x5, x6, x7, gate_ref, up_ref, hidden_ref, to_gate_ref, to_up_ref):
    rank = ranks_ref[0]
    width = x0.shape[1]
    half = x0.shape[0]
    for rows, pieces in ((slice(0, half), (x0, x2, x4, x6)), (slice(half, 2 * half), (x1, x3, x5, x7))):
        x = [piece[...] for piece in pieces]
        gate, up = (
            sum(dot(x[k], w_ref[quarter_of(rank, k, width), :], NN) for k in range(4))
            for w_ref in (gate_ref, up_ref)
        )
        sigmoid = jax.nn.sigmoid(gate)
        active = gate * sigmoid
        hidden_ref[rows, :] = (active * up).astype(BF16)
        to_up_ref[rows, :] = active
        to_gate_ref[rows, :] = up * sigmoid * (1.0 + gate * (1.0 - sigmoid))


def rows_of(ranks_ref, k, width, gate_ref, up_ref):
    at = quarter_of(ranks_ref[0], k, width)
    return jnp.concatenate([gate_ref[at, :], up_ref[at, :]], axis=1)


def grads_kernel(
    ranks_ref, own_ref, left_a, left_b, right_a, right_b, to_gate_ref, to_up_ref, gate_ref, up_ref,
    both_ref, p2, p3,
):
    half = gate_ref.shape[1]
    grad_hidden = own_ref[...] + joined(left_a, left_b) + joined(right_a, right_b)
    both_ref[:, :half] = (grad_hidden * to_gate_ref[...]).astype(BF16)
    both_ref[:, half:] = (grad_hidden * to_up_ref[...]).astype(BF16)
    w = rows_of(ranks_ref, 2, p2.shape[1], gate_ref, up_ref)
    rows = p2.shape[0]
    p2[...] = dot(both_ref[:rows, :], w, NT).astype(BF16)
    p3[...] = dot(both_ref[rows:, :], w, NT).astype(BF16)


def parts_kernel(ranks_ref, both_ref, gate_ref, up_ref, own_ref, after_a, after_b, before_a, before_b):
    both = both_ref[...]
    part = lambda k: dot(both, rows_of(ranks_ref, k, own_ref.shape[1], gate_ref, up_ref), NT)
    halves(part(1), after_a, after_b)
    halves(part(3), before_a, before_b)
    own_ref[...] = part(0).astype(BF16)


def weights_kernel(ranks_ref, x0, x1, x2, x3, x4, x5, x6, x7, both_ref, gate_ref, up_ref):
    rank = ranks_ref[0]
    width = x0.shape[1]
    half, rows = (gate_ref.shape[1], x0.shape[0])
    for k, (a, b) in enumerate(((x0, x1), (x2, x3), (x4, x5), (x6, x7))):
        grads = dot(a[...], both_ref[:rows, :], TN) + dot(b[...], both_ref[rows:, :], TN)
        at = quarter_of(rank, k, width)
        gate_ref[at, :] = grads[:, :half].astype(BF16)
        up_ref[at, :] = grads[:, half:].astype(BF16)


def down_kernel(ranks_ref, c0, c1, c2, c3, c4, c5, c6, c7, hidden_ref, down_ref):
    rank = ranks_ref[0]
    width = c0.shape[1]
    rows = c0.shape[0]
    hidden = hidden_ref[...]
    for k, (a, b) in enumerate(((c0, c1), (c2, c3), (c4, c5), (c6, c7))):
        grads = dot(hidden[:rows], a[...], TN) + dot(hidden[rows:], b[...], TN)
        down_ref[:, quarter_of(rank, k, width)] = grads.astype(BF16)


def out_kernel(
    ranks_ref, m0, m1, m2, m3, m4, m5, m6, m7, proj_ref, start_ref, grad_ref, term_ref
):
    rank = ranks_ref[0]
    width = m0.shape[1]
    w = [proj_ref[:, quarter_of(rank, k, width)] for k in range(4)]
    total = jnp.concatenate(
        [
            sum(dot(w[k], m[...], NT) for k, m in enumerate(side))
            for side in ((m0, m2, m4, m6), (m1, m3, m5, m7))
        ],
        axis=1,
    )
    grad = total.astype(BF16)
    grad_ref[...] = grad
    for h in range(start_ref.shape[0] // KEY_CHANNELS):
        ks, vs = (slice(h * KEY_CHANNELS, (h + 1) * KEY_CHANNELS), slice(h * DV, (h + 1) * DV))
        term_ref[ks, :] = dot(start_ref[ks, :], grad[vs], NT).astype(BF16)


def part_kernel(
    ranks_ref, m0, m1, m2, m3, m4, m5, m6, m7, mixer_ref, mine_ref, other_ref
):
    rank, x, core = (ranks_ref[k] for k in (0, 2, 3))
    x_count, z_count, lines, _ = mine_ref.shape
    half = m0.shape[0]
    mixer = mixer_ref[...]

    def put(k, part):
        part = part.astype(BF16)
        quarter = lax.rem(rank + k, 4)
        per = z_count // 4
        for i in range(per * x_count):
            first = part[2 * i * lines : (2 * i + 1) * lines]
            second = part[(2 * i + 1) * lines : (2 * i + 2) * lines]
            to_z = quarter * per + i // x_count
            to_x = lax.rem(i % x_count + x_count - x, x_count)
            mine_ref[to_x, to_z, :, :] = jnp.where(core == 0, first, second)
            other_ref[to_x, to_z, :, :] = jnp.where(core == 0, second, first)

    for k, (a, b) in enumerate(((m0, m1), (m2, m3), (m4, m5), (m6, m7))):
        put(k, dot(a[...], mixer[:half], TN) + dot(b[...], mixer[half:], TN))


def add_kernel(a_ref, b_ref, out_ref):
    out_ref[...] = (a_ref[...].astype(F32) + b_ref[...].astype(F32)).astype(BF16)


def pair_kernel(mine_ref, swapped_ref, *outs):
    for k, out in enumerate(outs):
        out[...] = (mine_ref[k].astype(F32) + swapped_ref[k].astype(F32)).astype(BF16)


def row_kernel(*refs):
    total = refs[0][...].astype(F32)
    for ref in refs[1:-1]:
        total = total + ref[...].astype(F32)
    refs[-1][...] = total.astype(BF16)


def call(kernel, outs, *args, scratch=(), ranks=None, flops=None):
    specs = [pl.BlockSpec(memory_space=pltpu.VMEM) for _ in args]
    if ranks is not None:
        specs, args = ([pl.BlockSpec(memory_space=pltpu.SMEM), *specs], (ranks, *args))
    cost = flops and pl.CostEstimate(flops=flops, bytes_accessed=0, transcendentals=0)
    return pl.pallas_call(
        kernel,
        in_specs=specs,
        out_specs=[pl.BlockSpec(memory_space=pltpu.VMEM) for _ in outs],
        out_shape=[jax.ShapeDtypeStruct(shape, dtype) for shape, dtype in outs],
        scratch_shapes=[pltpu.VMEM(shape, F32) for shape in scratch],
        cost_estimate=cost,
        compiler_params=pltpu.CompilerParams(vmem_limit_bytes=GRANT),
    )(*args)


def routed(rank, routes, weights, moe_input, layer_cot, experts):
    tokens, width = layer_cot.shape
    part = width // 4
    whole = lambda shape: pl.BlockSpec(shape, lambda i, r: (0,) * len(shape))
    own = pl.BlockSpec((tokens, part), lambda i, r: (0, r[0]))
    chunk = (experts, CAP * part // 128, 128)
    places = (4, tokens)
    return pl.pallas_call(
        route_kernel,
        grid_spec=pltpu.PrefetchScalarGridSpec(
            num_scalar_prefetch=1,
            grid=(1,),
            in_specs=[whole(routes.shape), whole(weights.shape), own, own],
            out_specs=[whole(chunk), whole(chunk), whole(places)],
        ),
        out_shape=[
            jax.ShapeDtypeStruct(chunk, BF16),
            jax.ShapeDtypeStruct(chunk, BF16),
            jax.ShapeDtypeStruct(places, jnp.int32),
        ],
    )(rank, routes, weights, moe_input, layer_cot)


def combined(rank, places, returned, layer_cot):
    tokens, width = layer_cot.shape
    part = width // 4
    whole = lambda shape: pl.BlockSpec(shape, lambda i, r: (0,) * len(shape))
    return pl.pallas_call(
        combine_kernel,
        grid_spec=pltpu.PrefetchScalarGridSpec(
            num_scalar_prefetch=1,
            grid=(1,),
            in_specs=[
                whole(places.shape),
                whole(returned.shape),
                pl.BlockSpec((tokens, part), lambda i, r: (0, r[0])),
            ],
            out_specs=[whole((tokens // 2, part))] * 2,
        ),
        out_shape=[jax.ShapeDtypeStruct((tokens // 2, part), BF16)] * 2,
        compiler_params=pltpu.CompilerParams(vmem_limit_bytes=GRANT),
    )(rank, places, returned, layer_cot)


def shifted(x, axis, by):
    count = lax.axis_size(axis)
    return lax.ppermute(x, axis, [(i, (i + by) % count) for i in range(count)])


def neighbours(a, b):
    from_before = (shifted(a, "tp", 1), shifted(b, "tp", 1))
    from_after = (shifted(b, "tp", -1), shifted(a, "tp", -1))
    return from_before, from_after[::-1]


def across(before, after):
    return shifted(before[0], "tp", 1), shifted(after[1], "tp", -1)


def gathered(pair):
    before, after = neighbours(*pair)
    return *pair, *after, *across(before, after), *before


def added(a, b):
    return call(add_kernel, [(a.shape, BF16)], a, b)[0]


def reduced(after_a, after_b, before_a, before_b, from_before, from_after):
    left_b, right_a = (shifted(after_b, "tp", 1), shifted(before_a, "tp", -1))
    left_a = shifted(added(after_a, from_before), "tp", 1)
    right_b = shifted(added(before_b, from_after), "tp", -1)
    return left_a, left_b, right_a, right_b


def exchanged(x, axis):
    return lax.all_to_all(x, axis, split_axis=0, concat_axis=0, tiled=True)


def body(
    layer_cot,
    moe_input,
    routes,
    route_weights,
    gate_proj,
    up_proj,
    down_proj,
    out_proj,
    mixer_out,
    queries,
    key_rows,
    values,
    log_decay,
    saved_state,
):
    sp_count = lax.axis_size(SP)
    slots = sp_count * CAP
    tokens, model_width = layer_cot.shape
    quarter = model_width // 4
    hidden_units = gate_proj.shape[2]
    channels = queries.shape[1]
    cols = mixer_out.shape[1]
    rank = lax.axis_index("tp").astype(jnp.int32).reshape(1)
    ranks = jnp.stack([lax.axis_index(axis).astype(jnp.int32) for axis in ("tp", *SP)])
    gate_w, up_w, down_w = (gate_proj[0], up_proj[0], down_proj[0])
    wide = (slots, quarter)
    rows_in, rows_cot, places = routed(
        rank, routes.T, route_weights.T, moe_input, layer_cot, sp_count
    )

    down_part = (hidden_units, quarter)
    s0, s1, s2, s3 = call(parted_kernel, [(down_part, BF16)] * 4, down_w, ranks=ranks)
    d1, d2, d3 = (shifted(s3, "tp", -1), shifted(s2, "tp", 2), shifted(s1, "tp", 1))
    arrived = exchanged(rows_in, SP)
    half = slots // 2
    piece = (half, hidden_units)
    block = (half, quarter)
    got_in = call(unpack_kernel, [(block, BF16)] * 2, arrived)
    got_in, rows_cot = lax.optimization_barrier((got_in, rows_cot))
    x = gathered(got_in)
    got_cot = exchanged(rows_cot, SP)
    rows = (slots, hidden_units)
    start, pieces = call(
        start_kernel, [((channels, tokens), BF16), ((channels, 3), BF16)], queries, log_decay
    )
    got_cot, start, pieces, d1, d2, d3, *x = lax.optimization_barrier(
        (got_cot, start, pieces, d1, d2, d3, *x)
    )
    rows = (slots, hidden_units)
    *cot, a2, a3 = call(
        cot_kernel, [(block, BF16)] * 2 + [(piece, BF16)] * 2, got_cot, d2
    )
    hops = (shifted(a2, "tp", 1), shifted(a3, "tp", -1))
    own, *rest = call(
        rest_kernel,
        [(rows, F32)] + [(piece, BF16)] * 4,
        *cot, s0, d1, d3,
        flops=10**9,
    )
    totals = pieces.T.reshape(3, sp_count, -1).transpose(1, 0, 2).reshape(sp_count, -1)
    totals = jnp.pad(totals, ((0, 0), (0, 128 - totals.shape[1])))
    sides = reduced(*rest, *hops)
    hidden, to_gate, to_up = call(
        in_kernel, [(rows, BF16), (rows, F32), (rows, F32)], *x, gate_w, up_w, ranks=ranks, flops=2 * 10**9
    )
    hidden, totals, *sides = lax.optimization_barrier((hidden, totals, *sides))
    piece = (half, quarter)
    both, a2, a3 = call(
        grads_kernel,
        [((slots, 2 * hidden_units), BF16), (piece, BF16), (piece, BF16)],
        own, *sides, to_gate, to_up, gate_w, up_w,
        ranks=ranks,
    )
    hops = (shifted(a2, "tp", 1), shifted(a3, "tp", -1))
    own, *rest = call(
        parts_kernel, [(wide, BF16)] + [(piece, BF16)] * 4, both, gate_w, up_w, ranks=ranks, flops=3 * 10**9
    )
    sides = reduced(*rest, *hops)
    weight = (model_width, hidden_units)
    grad_gate, grad_up = call(
        weights_kernel, [(weight, BF16)] * 2, *x, both, ranks=ranks, flops=3 * 10**9
    )
    grad_gate, grad_up, *sides = lax.optimization_barrier((grad_gate, grad_up, *sides))
    (packed,) = call(pack_kernel, [(rows_in.shape, BF16)], own, *sides)
    packed, cot = lax.optimization_barrier((packed, cot))
    returned = exchanged(packed, SP)
    c_before, c_after = neighbours(*cot)
    returned, c_before, c_after = lax.optimization_barrier((returned, c_before, c_after))
    mix = gathered(combined(rank, places.T, returned, layer_cot))
    out_grad, term = call(
        out_kernel,
        [((cols, tokens), BF16), ((channels, DV), BF16)],
        *mix, out_proj, start,
        ranks=ranks,
    )
    terms = jnp.concatenate([term.reshape(sp_count, -1), totals], axis=1)
    terms, mix, out_grad, c_before, c_after = lax.optimization_barrier(
        (terms, mix, out_grad, c_before, c_after)
    )
    c = (*cot, *c_after, *across(c_before, c_after), *c_before)
    terms = exchanged(terms.reshape(sp_count, 3, -1), SP)
    x_count, z_count = (lax.axis_size(SP[1]), lax.axis_size(SP[0]))
    part = (x_count, z_count, model_width // sp_count, cols)
    mine, other = call(
        part_kernel, [(part, BF16)] * 2, *mix, mixer_out, ranks=ranks, flops=4 * 10**9
    )
    swapped = shifted(other, SP[2], 1)
    line = part[1:]
    pairs = call(pair_kernel, [(line, BF16)] * x_count, mine, swapped)
    lines = [shifted(pairs[k], SP[1], k) for k in range(1, x_count)]
    (laters,) = call(
        scan_kernel,
        [((sp_count, channels * DV // sp_count), BF16)],
        terms.reshape(sp_count, -1),
    )
    laters = exchanged(laters.reshape(sp_count, 2, -1), SP)
    (row,) = call(row_kernel, [(line, BF16)], pairs[0], *lines)
    row = exchanged(row, SP[0])
    grad_outproj = jnp.sum(row.astype(F32), axis=0)
    from_later = laters.reshape(channels, DV).astype(F32)
    (grad_down,) = call(
        down_kernel, [(down_w.shape, BF16)], *c, hidden, ranks=ranks, flops=2 * 10**9
    )
    grad_queries, grad_keys, grad_values, grad_decay = call(
        mixer_kernel,
        [
            (queries.shape, BF16),
            (key_rows.shape, BF16),
            (values.shape, BF16),
            (log_decay.shape, F32),
        ],
        queries,
        key_rows,
        values,
        log_decay,
        out_grad,
        saved_state.reshape(channels, DV),
        from_later,
        scratch=((channels, tokens), (channels, tokens), (values.shape[1], tokens), (channels, 1)),
    )
    return (
        grad_gate[None],
        grad_up[None],
        grad_down[None],
        grad_outproj,
        grad_queries,
        grad_keys,
        grad_values,
        grad_decay,
    )


def solution(mesh):
    torus = Mesh(mesh.devices.reshape(8, 4, 2, mesh.shape["tp"]), ("sp_0", "sp_1", "sp_2", "tp"))

    return jax.shard_map(
        body,
        mesh=torus,
        in_specs=(
            P(SP, None),
            P(SP, None),
            P(SP, None),
            P(SP, None),
            P(SP, None, "tp"),
            P(SP, None, "tp"),
            P(SP, "tp", None),
            P("tp", None),
            P(SP, "tp"),
            P(SP, "tp"),
            P(SP, "tp"),
            P(SP, "tp"),
            P(SP, "tp"),
            P(SP, "tp", None, None),
        ),
        out_specs=(
            P(SP, None, "tp"),
            P(SP, None, "tp"),
            P(SP, "tp", None),
            P(SP, "tp"),
            P(SP, "tp"),
            P(SP, "tp"),
            P(SP, "tp"),
            P(SP, "tp"),
        ),
        check_vma=False,
    )
```

```python
import jax
import jax.numpy as jnp
from jax import lax
from jax.experimental import pallas as pl
from jax.experimental.pallas import tpu as pltpu
from jax.sharding import Mesh
from jax.sharding import PartitionSpec as P


KEY_CHANNELS = 32
DV = 64
BLOCK = 64
CAP = 12
SP = ("sp_0", "sp_1", "sp_2")
GRANT = 24 * 2**20
F32 = jnp.float32
BF16 = jnp.bfloat16


def dot(a, b, contract, dt=jnp.bfloat16):
    return lax.dot_general(
        a.astype(dt), b.astype(dt), (contract, ((), ())), preferred_element_type=jnp.float32
    )


NN = ((1,), (0,))
NT = ((1,), (1,))
TN = ((0,), (0,))


def summed_by(x, mask, pieces):
    total, rest = (None, x)
    for _ in range(pieces):
        part = rest.astype(jnp.bfloat16)
        rest = rest - part.astype(jnp.float32)
        term = dot(part, mask, NN)
        total = term if total is None else total + term
    return total


def triangle(length, keep):
    down = lax.broadcasted_iota(jnp.int32, (length, length), 0)
    across = lax.broadcasted_iota(jnp.int32, (length, length), 1)
    return jnp.where(keep(down, across), 1.0, 0.0).astype(jnp.bfloat16)


def route_kernel(rank_ref, routes_ref, weights_ref, in_ref, cot_ref, in_out, cot_out, places_ref):
    tokens = routes_ref.shape[1]
    experts = in_out.shape[0]
    routes = [routes_ref[k : k + 1, :] for k in range(2)]
    weights = [weights_ref[k : k + 1, :] for k in range(2)]
    expert_ids = lax.broadcasted_iota(jnp.int32, (experts, tokens), 0)
    named = [expert_ids == route for route in routes]
    before = dot(
        jnp.where(named[0] | named[1], 1.0, 0.0), triangle(tokens, lambda u, t: u < t), NN
    )
    low, high = ([], [])
    for k in range(2):
        slot = jnp.sum(jnp.where(named[k], before, 0.0), axis=0, keepdims=True).astype(jnp.int32)
        low.append(jnp.where(slot < 8, routes[k] * 8 + slot, -8))
        high.append(jnp.where(slot < 8, -8, routes[k] * 8 + slot - 8))
        places_ref[k : k + 1, :] = low[k]
        places_ref[k + 2 : k + 3, :] = high[k]
    row = lax.broadcasted_iota(jnp.int32, (experts * 8, tokens), 0)
    upper = (row & 4) == 4
    hits_low = [row == low[k] for k in range(2)]
    hits_high = [(row - jnp.where(upper, 4, 0)) == high[k] for k in range(2)]

    def chosen(hits):
        weight = jnp.where(hits[0], weights[0], 0.0) + jnp.where(hits[1], weights[1], 0.0)
        return (
            jnp.where(hits[0] | hits[1], 1.0, 0.0).astype(BF16),
            jnp.sum(weight, axis=1, keepdims=True),
        )

    picks = (chosen(hits_low), chosen(hits_high))
    first = lax.broadcasted_iota(jnp.int32, (experts * 8, 128), 0) & 4
    for x_ref, out, weighted in ((in_ref, in_out, False), (cot_ref, cot_out, True)):
        x = x_ref[...]
        got = [dot(hot, x, NN) * (weight if weighted else 1.0) for hot, weight in picks]
        blocks = x.shape[1] // 128
        lanes = lambda g, i: g[:, i * 128 : (i + 1) * 128]
        for i in range(blocks):
            out[:, i * 8 : (i + 1) * 8, :] = lanes(got[0], i).astype(BF16).reshape(experts, 8, 128)
        for i in range(0, blocks, 2):
            at = blocks * 8 + i * 4
            pair = jnp.where(first == 0, lanes(got[1], i), lanes(got[1], i + 1))
            out[:, at : at + 8, :] = pair.astype(BF16).reshape(experts, 8, 128)


def unpack_kernel(got_ref, first_ref, second_ref):
    spans = got_ref.shape[0]
    blocks = first_ref.shape[1] // 128
    low, half = (spans * 8, first_ref.shape[0])
    first = lax.broadcasted_iota(jnp.int32, (spans // 2, 8, 128), 1) < 4
    for i in range(blocks):
        lanes = slice(i * 128, (i + 1) * 128)
        rows = got_ref[:, i * 8 : (i + 1) * 8, :].reshape(low, 128)
        first_ref[:, lanes] = rows[:half]
        second_ref[: low - half, lanes] = rows[half:]
    for i in range(0, blocks, 2):
        at = blocks * 8 + i * 4
        pair = got_ref[:, at : at + 8, :].astype(F32).reshape(spans // 2, 2, 8, 128)
        a, b = (pair[:, 0], pair[:, 1])
        even = jnp.where(first, a, pltpu.roll(b, 4, 1))
        odd = jnp.where(first, pltpu.roll(a, 4, 1), b)
        for j, x in ((i, even), (i + 1, odd)):
            lanes = slice(j * 128, (j + 1) * 128)
            second_ref[low - half :, lanes] = x.reshape(low // 2, 128).astype(BF16)


def pack_kernel(own_ref, left_a, left_b, right_a, right_b, out_ref):
    spans = out_ref.shape[0]
    blocks = own_ref.shape[1] // 128
    low = spans * 8
    totals = []
    for i in range(blocks):
        lanes = slice(i * 128, (i + 1) * 128)
        totals.append(
            own_ref[:, lanes].astype(F32)
            + joined(left_a, left_b, lanes)
            + joined(right_a, right_b, lanes)
        )
        rows = totals[i][:low].astype(BF16)
        out_ref[:, i * 8 : (i + 1) * 8, :] = rows.reshape(spans, 8, 128)
    first = lax.broadcasted_iota(jnp.int32, (spans // 2, 8, 128), 1) < 4
    for i in range(0, blocks, 2):
        at = blocks * 8 + i * 4
        even, odd = (totals[j][low:].reshape(spans // 2, 8, 128) for j in (i, i + 1))
        a = jnp.where(first, even, pltpu.roll(odd, 4, 1))
        b = jnp.where(first, pltpu.roll(even, 4, 1), odd)
        pair = jnp.stack([a, b], axis=1).reshape(spans, 8, 128)
        out_ref[:, at : at + 8, :] = pair.astype(BF16)


def combine_kernel(ranks_ref, places_ref, returned_ref, cot_ref, first_ref, second_ref):
    tokens = cot_ref.shape[0]
    experts = returned_ref.shape[0]
    blocks = cot_ref.shape[1] // 128
    row = lax.broadcasted_iota(jnp.int32, (tokens, experts * 8), 1)
    place = [places_ref[:, k : k + 1] for k in range(4)]
    hot = lambda a, b: jnp.where((row == a) | (row == b), 1.0, 0.0).astype(BF16)
    low = hot(place[0], place[1])
    high = (hot(place[2], place[3]), hot(place[2] + 4, place[3] + 4))
    flat = lambda at: returned_ref[:, at : at + 8, :].reshape(experts * 8, 128)
    for i in range(blocks):
        moe_grad = dot(low, flat(i * 8), NN)
        moe_grad += dot(high[i % 2], flat(blocks * 8 + (i // 2) * 8), NN)
        lanes = slice(i * 128, (i + 1) * 128)
        mix = (cot_ref[:, lanes].astype(F32) + moe_grad).astype(BF16)
        first_ref[:, lanes] = mix[: tokens // 2]
        second_ref[:, lanes] = mix[tokens // 2 :]


def turned(x):
    return x.astype(jnp.float32).T


def start_kernel(q_ref, log_ref, start_ref, total_ref):
    tokens = q_ref.shape[0]
    cum = summed_by(turned(log_ref[...]), triangle(tokens, lambda u, t: u <= t), 3)
    rest = cum[:, tokens - 1 :]
    for k in range(3):
        piece = rest.astype(BF16)
        rest = rest - piece.astype(F32)
        total_ref[:, k : k + 1] = piece
    start_ref[...] = (turned(q_ref[...]) * jnp.exp(cum)).astype(BF16)


def mixer_kernel(
    q_ref, k_ref, v_ref, log_ref, grad_ref, state_ref, later_ref, gq_ref, gk_ref, gv_ref, gd_ref,
    dq_s, dk_s, dv_s, cross_s,
):
    tokens, channels = q_ref.shape
    half = tokens // 2
    cum = summed_by(turned(log_ref[...]), triangle(tokens, lambda u, t: u <= t), 3)
    q, k = (turned(q_ref[...]), turned(k_ref[...]))
    v = turned(v_ref[...]).astype(jnp.bfloat16)
    grad = grad_ref[...]
    lane = lax.broadcasted_iota(jnp.int32, (channels, tokens), 1)
    block = lane // BLOCK
    at = lambda t: cum[:, t : t + 1]
    near = jnp.where(
        block < 2,
        jnp.where(block == 0, at(31), at(95)),
        jnp.where(block == 2, at(159), at(223)),
    )
    wide = jnp.exp(-jnp.abs(cum - at(127)))
    mid = jnp.exp(-jnp.abs(cum - jnp.where(block < 2, at(63), at(191))))
    gap = cum - near
    up, down = (jnp.exp(gap), jnp.exp(-gap))
    start = jnp.exp(cum)
    end = jnp.exp(at(tokens - 1) - cum)
    whole = jnp.exp(at(tokens - 1))
    q_wide = jnp.where(block >= 2, q * wide, 0.0).astype(jnp.bfloat16)
    k_wide = jnp.where(block < 2, k * wide, 0.0).astype(jnp.bfloat16)
    q_mid, k_mid = ((q * mid), (k * mid))
    q_mids = [jnp.where(block == b, q_mid, 0.0).astype(jnp.bfloat16) for b in (1, 3)]
    k_mids = [jnp.where(block == b, k_mid, 0.0).astype(jnp.bfloat16) for b in (0, 2)]
    q_near, k_near = (q * up, k * down)
    q_nears = [jnp.where(block == b, q_near, 0.0).astype(jnp.bfloat16) for b in range(4)]
    k_nears = [jnp.where(block == b, k_near, 0.0).astype(jnp.bfloat16) for b in range(4)]
    q_parts = [q_wide, *q_mids, *q_nears]
    k_parts = [k_wide, *k_mids, *k_nears]
    k_end = (k * end).astype(jnp.bfloat16)
    down_ids = lax.broadcasted_iota(jnp.int32, (tokens, tokens), 0)
    across_ids = lax.broadcasted_iota(jnp.int32, (tokens, tokens), 1)
    causal = down_ids >= across_ids
    first64 = lax.broadcasted_iota(jnp.int32, (KEY_CHANNELS, half), 1) < BLOCK
    lo, hi = (slice(0, half), slice(half, tokens))
    kc = KEY_CHANNELS
    for h in range(channels // kc):
        ks, vs = (slice(h * kc, (h + 1) * kc), slice(h * DV, (h + 1) * DV))
        q_seg = jnp.concatenate([p[ks] for p in q_parts], axis=0)
        k_seg = jnp.concatenate([p[ks] for p in k_parts], axis=0)
        grad_h, v_h = (grad[vs], v[vs])
        scores = jnp.where(causal, dot(q_seg, k_seg, TN), 0.0).astype(jnp.bfloat16)
        coupl = jnp.where(causal, dot(grad_h, v_h, TN), 0.0).astype(jnp.bfloat16)
        to_q = dot(k_seg, coupl, NT)
        to_k = dot(q_seg, coupl, NN)
        seg = lambda x, i, side: x[i * kc : (i + 1) * kc, side]
        state = state_ref[ks, :]
        later = later_ref[ks, :]
        dq = start[ks] * dot(state, grad_h, NN)
        dk = end[ks] * dot(later, v_h, NN)
        dq_lo = up[ks, lo] * jnp.where(first64, seg(to_q, 3, lo), seg(to_q, 4, lo))
        dq_lo += mid[ks, lo] * jnp.where(first64, 0.0, seg(to_q, 1, lo))
        dq_hi = up[ks, hi] * jnp.where(first64, seg(to_q, 5, hi), seg(to_q, 6, hi))
        dq_hi += mid[ks, hi] * jnp.where(first64, 0.0, seg(to_q, 2, hi))
        dq_hi += wide[ks, hi] * seg(to_q, 0, hi)
        dk_lo = down[ks, lo] * jnp.where(first64, seg(to_k, 3, lo), seg(to_k, 4, lo))
        dk_lo += mid[ks, lo] * jnp.where(first64, seg(to_k, 1, lo), 0.0)
        dk_lo += wide[ks, lo] * seg(to_k, 0, lo)
        dk_hi = down[ks, hi] * jnp.where(first64, seg(to_k, 5, hi), seg(to_k, 6, hi))
        dk_hi += mid[ks, hi] * jnp.where(first64, seg(to_k, 2, hi), 0.0)
        dq_s[ks, :] = dq + jnp.concatenate([dq_lo, dq_hi], axis=1)
        dk_s[ks, :] = dk + jnp.concatenate([dk_lo, dk_hi], axis=1)
        dv_s[vs, :] = dot(grad_h, scores, NN) + dot(later, k_end[ks], TN)
        at_end = whole[ks] * state + dot(k_end[ks], v_h, NT)
        cross_s[ks, :] = jnp.sum(at_end * later, axis=1, keepdims=True)
    dq, dk = (dq_s[...], dk_s[...])
    change = q * dq - k * dk
    decay = summed_by(change, triangle(tokens, lambda u, t: u >= t), 2) + cross_s[...]
    gq_ref[...] = dq.T.astype(jnp.bfloat16)
    gk_ref[...] = dk.T.astype(jnp.bfloat16)
    gv_ref[...] = dv_s[...].T.astype(jnp.bfloat16)
    gd_ref[...] = decay.T


def scan_kernel(terms_ref, out_ref):
    spans, width = out_ref.shape
    channels = width // DV
    down_ids = lax.broadcasted_iota(jnp.int32, (spans, spans), 0)
    across_ids = lax.broadcasted_iota(jnp.int32, (spans, spans), 1)
    later = across_ids > down_ids
    up_to = jnp.where(down_ids >= across_ids, 1.0, 0.0)
    before = jnp.where(down_ids < across_ids, 1.0, 0.0)
    exact = lax.Precision.HIGHEST
    terms = terms_ref[...].astype(F32)
    pieces = [terms[:, width + k * channels : width + (k + 1) * channels] for k in range(3)]
    totals = pieces[0] + pieces[1] + pieces[2]
    through = jnp.dot(up_to, totals, precision=exact, preferred_element_type=F32)
    ahead = lax.dot_general(
        totals, before, (TN, ((), ())), precision=exact, preferred_element_type=F32
    )
    for c in range(channels):
        gap = ahead[c : c + 1, :] - through[:, c : c + 1]
        weight = jnp.where(later, jnp.exp(jnp.where(later, gap, 0.0)), 0.0)
        vs = slice(c * DV, (c + 1) * DV)
        out_ref[:, vs] = jnp.dot(
            weight, terms[:, vs], precision=exact, preferred_element_type=F32
        ).astype(out_ref.dtype)


def quarter_of(rank, k, width):
    return pl.ds(pl.multiple_of(lax.rem(rank + k, 4) * width, width), width)


def parted_kernel(ranks_ref, down_ref, *outs):
    width = down_ref.shape[1] // 4
    for k in range(4):
        outs[k][...] = down_ref[:, quarter_of(ranks_ref[0], k, width)]


def cot_kernel(got_ref, d2, cot_a, cot_b, a2_ref, a3_ref):
    unpack_kernel(got_ref, cot_a, cot_b)
    a2_ref[...] = dot(cot_a[...], d2[...], NT).astype(BF16)
    a3_ref[...] = dot(cot_b[...], d2[...], NT).astype(BF16)


def halves(part, first_ref, second_ref):
    part = part.astype(BF16)
    rows = first_ref.shape[0]
    first_ref[...] = part[:rows]
    second_ref[...] = part[rows:]


def rest_kernel(cot_a, cot_b, d0, d1, d3, own_ref, after_a, after_b, before_a, before_b):
    half = cot_a.shape[0]
    own_ref[:half, :] = dot(cot_a[...], d0[...], NT)
    own_ref[half:, :] = dot(cot_b[...], d0[...], NT)
    for cot, after, before in ((cot_a, after_a, before_a), (cot_b, after_b, before_b)):
        after[...] = dot(cot[...], d1[...], NT).astype(BF16)
        before[...] = dot(cot[...], d3[...], NT).astype(BF16)


def joined(a_ref, b_ref, lanes=slice(None)):
    return jnp.concatenate([a_ref[:, lanes], b_ref[:, lanes]], axis=0).astype(F32)


def in_kernel(ranks_ref, x0, x1, x2, x3, x4, x5, x6, x7, gate_ref, up_ref, hidden_ref, to_gate_ref, to_up_ref, held, sems):
    rank = ranks_ref[0]
    moves = [
        pltpu.make_async_copy(ref, held.at[k], sems.at[k])
        for k, ref in enumerate((x0, x1, x2, x3, x4, x5, x6, x7))
    ]
    for move in moves:
        move.start()
    for move in moves:
        move.wait()
    width = x0.shape[1]
    half = x0.shape[0]
    for side in range(2):
        rows = slice(side * half, (side + 1) * half)
        x = [held[2 * k + side] for k in range(4)]
        gate, up = (
            sum(dot(x[k], w_ref[quarter_of(rank, k, width), :], NN) for k in range(4))
            for w_ref in (gate_ref, up_ref)
        )
        sigmoid = jax.nn.sigmoid(gate)
        active = gate * sigmoid
        hidden_ref[rows, :] = (active * up).astype(BF16)
        to_up_ref[rows, :] = active
        to_gate_ref[rows, :] = up * sigmoid * (1.0 + gate * (1.0 - sigmoid))


def rows_of(ranks_ref, k, width, gate_ref, up_ref):
    at = quarter_of(ranks_ref[0], k, width)
    return jnp.concatenate([gate_ref[at, :], up_ref[at, :]], axis=1)


def grads_kernel(
    ranks_ref, own_ref, left_a, left_b, right_a, right_b, to_gate_ref, to_up_ref, gate_ref, up_ref,
    both_ref, p2, p3,
):
    half = gate_ref.shape[1]
    grad_hidden = own_ref[...] + joined(left_a, left_b) + joined(right_a, right_b)
    both_ref[:, :half] = (grad_hidden * to_gate_ref[...]).astype(BF16)
    both_ref[:, half:] = (grad_hidden * to_up_ref[...]).astype(BF16)
    w = rows_of(ranks_ref, 2, p2.shape[1], gate_ref, up_ref)
    rows = p2.shape[0]
    p2[...] = dot(both_ref[:rows, :], w, NT).astype(BF16)
    p3[...] = dot(both_ref[rows:, :], w, NT).astype(BF16)


def parts_kernel(ranks_ref, both_ref, gate_ref, up_ref, own_ref, after_a, after_b, before_a, before_b):
    both = both_ref[...]
    part = lambda k: dot(both, rows_of(ranks_ref, k, own_ref.shape[1], gate_ref, up_ref), NT)
    halves(part(1), after_a, after_b)
    halves(part(3), before_a, before_b)
    own_ref[...] = part(0).astype(BF16)


def weights_kernel(ranks_ref, x0, x1, x2, x3, x4, x5, x6, x7, both_ref, gate_ref, up_ref):
    rank = ranks_ref[0]
    width = x0.shape[1]
    half, rows = (gate_ref.shape[1], x0.shape[0])
    for k, (a, b) in enumerate(((x0, x1), (x2, x3), (x4, x5), (x6, x7))):
        grads = dot(a[...], both_ref[:rows, :], TN) + dot(b[...], both_ref[rows:, :], TN)
        at = quarter_of(rank, k, width)
        gate_ref[at, :] = grads[:, :half].astype(BF16)
        up_ref[at, :] = grads[:, half:].astype(BF16)


def down_kernel(ranks_ref, c0, c1, c2, c3, c4, c5, c6, c7, hidden_ref, down_ref):
    rank = ranks_ref[0]
    width = c0.shape[1]
    rows = c0.shape[0]
    hidden = hidden_ref[...]
    for k, (a, b) in enumerate(((c0, c1), (c2, c3), (c4, c5), (c6, c7))):
        grads = dot(hidden[:rows], a[...], TN) + dot(hidden[rows:], b[...], TN)
        down_ref[:, quarter_of(rank, k, width)] = grads.astype(BF16)


def out_kernel(
    ranks_ref, m0, m1, m2, m3, m4, m5, m6, m7, proj_ref, start_ref, grad_ref, term_ref
):
    rank = ranks_ref[0]
    width = m0.shape[1]
    w = [proj_ref[:, quarter_of(rank, k, width)] for k in range(4)]
    total = jnp.concatenate(
        [
            sum(dot(w[k], m[...], NT) for k, m in enumerate(side))
            for side in ((m0, m2, m4, m6), (m1, m3, m5, m7))
        ],
        axis=1,
    )
    grad = total.astype(BF16)
    grad_ref[...] = grad
    for h in range(start_ref.shape[0] // KEY_CHANNELS):
        ks, vs = (slice(h * KEY_CHANNELS, (h + 1) * KEY_CHANNELS), slice(h * DV, (h + 1) * DV))
        term_ref[ks, :] = dot(start_ref[ks, :], grad[vs], NT).astype(BF16)


def part_kernel(
    ranks_ref, m0, m1, m2, m3, m4, m5, m6, m7, mixer_ref, mine_ref, other_ref
):
    rank, x, core = (ranks_ref[k] for k in (0, 2, 3))
    x_count, z_count, lines, _ = mine_ref.shape
    half = m0.shape[0]
    mixer = mixer_ref[...]

    def put(k, part):
        part = part.astype(BF16)
        quarter = lax.rem(rank + k, 4)
        per = z_count // 4
        for i in range(per * x_count):
            first = part[2 * i * lines : (2 * i + 1) * lines]
            second = part[(2 * i + 1) * lines : (2 * i + 2) * lines]
            to_z = quarter * per + i // x_count
            to_x = lax.rem(i % x_count + x_count - x, x_count)
            mine_ref[to_x, to_z, :, :] = jnp.where(core == 0, first, second)
            other_ref[to_x, to_z, :, :] = jnp.where(core == 0, second, first)

    for k, (a, b) in enumerate(((m0, m1), (m2, m3), (m4, m5), (m6, m7))):
        put(k, dot(a[...], mixer[:half], TN) + dot(b[...], mixer[half:], TN))


def add_kernel(a_ref, b_ref, out_ref):
    out_ref[...] = (a_ref[...].astype(F32) + b_ref[...].astype(F32)).astype(BF16)


def pair_kernel(mine_ref, swapped_ref, *outs):
    for k, out in enumerate(outs):
        out[...] = (mine_ref[k].astype(F32) + swapped_ref[k].astype(F32)).astype(BF16)


def row_kernel(*refs):
    total = refs[0][...].astype(F32)
    for ref in refs[1:-1]:
        total = total + ref[...].astype(F32)
    refs[-1][...] = total.astype(BF16)


def call(kernel, outs, *args, scratch=(), ranks=None, flops=None, far=0, scratches=()):
    specs = [
        pl.BlockSpec(memory_space=pltpu.HBM if k < far else pltpu.VMEM) for k in range(len(args))
    ]
    if ranks is not None:
        specs, args = ([pl.BlockSpec(memory_space=pltpu.SMEM), *specs], (ranks, *args))
    cost = flops and pl.CostEstimate(flops=flops, bytes_accessed=0, transcendentals=0)
    return pl.pallas_call(
        kernel,
        in_specs=specs,
        out_specs=[pl.BlockSpec(memory_space=pltpu.VMEM) for _ in outs],
        out_shape=[jax.ShapeDtypeStruct(shape, dtype) for shape, dtype in outs],
        scratch_shapes=[*(pltpu.VMEM(shape, F32) for shape in scratch), *scratches],
        cost_estimate=cost,
        compiler_params=pltpu.CompilerParams(vmem_limit_bytes=GRANT),
    )(*args)


def routed(rank, routes, weights, moe_input, layer_cot, experts):
    tokens, width = layer_cot.shape
    part = width // 4
    whole = lambda shape: pl.BlockSpec(shape, lambda i, r: (0,) * len(shape))
    own = pl.BlockSpec((tokens, part), lambda i, r: (0, r[0]))
    chunk = (experts, CAP * part // 128, 128)
    places = (4, tokens)
    return pl.pallas_call(
        route_kernel,
        grid_spec=pltpu.PrefetchScalarGridSpec(
            num_scalar_prefetch=1,
            grid=(1,),
            in_specs=[whole(routes.shape), whole(weights.shape), own, own],
            out_specs=[whole(chunk), whole(chunk), whole(places)],
        ),
        out_shape=[
            jax.ShapeDtypeStruct(chunk, BF16),
            jax.ShapeDtypeStruct(chunk, BF16),
            jax.ShapeDtypeStruct(places, jnp.int32),
        ],
    )(rank, routes, weights, moe_input, layer_cot)


def combined(rank, places, returned, layer_cot):
    tokens, width = layer_cot.shape
    part = width // 4
    whole = lambda shape: pl.BlockSpec(shape, lambda i, r: (0,) * len(shape))
    return pl.pallas_call(
        combine_kernel,
        grid_spec=pltpu.PrefetchScalarGridSpec(
            num_scalar_prefetch=1,
            grid=(1,),
            in_specs=[
                whole(places.shape),
                whole(returned.shape),
                pl.BlockSpec((tokens, part), lambda i, r: (0, r[0])),
            ],
            out_specs=[whole((tokens // 2, part))] * 2,
        ),
        out_shape=[jax.ShapeDtypeStruct((tokens // 2, part), BF16)] * 2,
        compiler_params=pltpu.CompilerParams(vmem_limit_bytes=GRANT),
    )(rank, places, returned, layer_cot)


def shifted(x, axis, by):
    count = lax.axis_size(axis)
    return lax.ppermute(x, axis, [(i, (i + by) % count) for i in range(count)])


def neighbours(a, b):
    from_before = (shifted(a, "tp", 1), shifted(b, "tp", 1))
    from_after = (shifted(b, "tp", -1), shifted(a, "tp", -1))
    return from_before, from_after[::-1]


def across(before, after):
    return shifted(before[0], "tp", 1), shifted(after[1], "tp", -1)


def gathered(pair):
    before, after = neighbours(*pair)
    return *pair, *after, *across(before, after), *before


def added(a, b):
    return call(add_kernel, [(a.shape, BF16)], a, b)[0]


def reduced(after_a, after_b, before_a, before_b, from_before, from_after):
    left_b, right_a = (shifted(after_b, "tp", 1), shifted(before_a, "tp", -1))
    left_a = shifted(added(after_a, from_before), "tp", 1)
    right_b = shifted(added(before_b, from_after), "tp", -1)
    return left_a, left_b, right_a, right_b


def exchanged(x, axis):
    return lax.all_to_all(x, axis, split_axis=0, concat_axis=0, tiled=True)


def body(
    layer_cot,
    moe_input,
    routes,
    route_weights,
    gate_proj,
    up_proj,
    down_proj,
    out_proj,
    mixer_out,
    queries,
    key_rows,
    values,
    log_decay,
    saved_state,
):
    sp_count = lax.axis_size(SP)
    slots = sp_count * CAP
    tokens, model_width = layer_cot.shape
    quarter = model_width // 4
    hidden_units = gate_proj.shape[2]
    channels = queries.shape[1]
    cols = mixer_out.shape[1]
    rank = lax.axis_index("tp").astype(jnp.int32).reshape(1)
    ranks = jnp.stack([lax.axis_index(axis).astype(jnp.int32) for axis in ("tp", *SP)])
    gate_w, up_w, down_w = (gate_proj[0], up_proj[0], down_proj[0])
    wide = (slots, quarter)
    rows_in, rows_cot, places = routed(
        rank, routes.T, route_weights.T, moe_input, layer_cot, sp_count
    )

    down_part = (hidden_units, quarter)
    s0, s1, s2, s3 = call(parted_kernel, [(down_part, BF16)] * 4, down_w, ranks=ranks)
    d1, d2, d3 = (shifted(s3, "tp", -1), shifted(s2, "tp", 2), shifted(s1, "tp", 1))
    arrived = exchanged(rows_in, SP)
    half = slots // 2
    piece = (half, hidden_units)
    block = (half, quarter)
    got_in = call(unpack_kernel, [(block, BF16)] * 2, arrived)
    got_in, rows_cot = lax.optimization_barrier((got_in, rows_cot))
    x = gathered(got_in)
    got_cot = exchanged(rows_cot, SP)
    rows = (slots, hidden_units)
    start, pieces = call(
        start_kernel, [((channels, tokens), BF16), ((channels, 3), BF16)], queries, log_decay
    )
    got_cot, start, pieces, d1, d2, d3, *x = lax.optimization_barrier(
        (got_cot, start, pieces, d1, d2, d3, *x)
    )
    rows = (slots, hidden_units)
    *cot, a2, a3 = call(
        cot_kernel, [(block, BF16)] * 2 + [(piece, BF16)] * 2, got_cot, d2
    )
    hops = (shifted(a2, "tp", 1), shifted(a3, "tp", -1))
    own, *rest = call(
        rest_kernel,
        [(rows, F32)] + [(piece, BF16)] * 4,
        *cot, s0, d1, d3,
        flops=10**9,
    )
    totals = pieces.T.reshape(3, sp_count, -1).transpose(1, 0, 2).reshape(sp_count, -1)
    totals = jnp.pad(totals, ((0, 0), (0, 128 - totals.shape[1])))
    sides = reduced(*rest, *hops)
    hidden, to_gate, to_up = call(
        in_kernel, [(rows, BF16), (rows, F32), (rows, F32)], *x, gate_w, up_w, ranks=ranks, flops=2 * 10**9, far=8,
        scratches=(pltpu.VMEM((8, *block), BF16), pltpu.SemaphoreType.DMA((8,))),
    )
    hidden, totals, *sides = lax.optimization_barrier((hidden, totals, *sides))
    piece = (half, quarter)
    both, a2, a3 = call(
        grads_kernel,
        [((slots, 2 * hidden_units), BF16), (piece, BF16), (piece, BF16)],
        own, *sides, to_gate, to_up, gate_w, up_w,
        ranks=ranks,
    )
    hops = (shifted(a2, "tp", 1), shifted(a3, "tp", -1))
    own, *rest = call(
        parts_kernel, [(wide, BF16)] + [(piece, BF16)] * 4, both, gate_w, up_w, ranks=ranks, flops=3 * 10**9
    )
    sides = reduced(*rest, *hops)
    weight = (model_width, hidden_units)
    grad_gate, grad_up = call(
        weights_kernel, [(weight, BF16)] * 2, *x, both, ranks=ranks, flops=3 * 10**9
    )
    grad_gate, grad_up, *sides = lax.optimization_barrier((grad_gate, grad_up, *sides))
    (packed,) = call(pack_kernel, [(rows_in.shape, BF16)], own, *sides)
    packed, cot = lax.optimization_barrier((packed, cot))
    returned = exchanged(packed, SP)
    c_before, c_after = neighbours(*cot)
    returned, c_before, c_after = lax.optimization_barrier((returned, c_before, c_after))
    mix = gathered(combined(rank, places.T, returned, layer_cot))
    out_grad, term = call(
        out_kernel,
        [((cols, tokens), BF16), ((channels, DV), BF16)],
        *mix, out_proj, start,
        ranks=ranks,
    )
    terms = jnp.concatenate([term.reshape(sp_count, -1), totals], axis=1)
    terms, mix, out_grad, c_before, c_after = lax.optimization_barrier(
        (terms, mix, out_grad, c_before, c_after)
    )
    c = (*cot, *c_after, *across(c_before, c_after), *c_before)
    terms = exchanged(terms.reshape(sp_count, 3, -1), SP)
    x_count, z_count = (lax.axis_size(SP[1]), lax.axis_size(SP[0]))
    part = (x_count, z_count, model_width // sp_count, cols)
    mine, other = call(
        part_kernel, [(part, BF16)] * 2, *mix, mixer_out, ranks=ranks, flops=4 * 10**9
    )
    swapped = shifted(other, SP[2], 1)
    line = part[1:]
    pairs = call(pair_kernel, [(line, BF16)] * x_count, mine, swapped)
    lines = [shifted(pairs[k], SP[1], k) for k in range(1, x_count)]
    (laters,) = call(
        scan_kernel,
        [((sp_count, channels * DV // sp_count), BF16)],
        terms.reshape(sp_count, -1),
    )
    laters = exchanged(laters.reshape(sp_count, 2, -1), SP)
    (row,) = call(row_kernel, [(line, BF16)], pairs[0], *lines)
    row = exchanged(row, SP[0])
    grad_outproj = jnp.sum(row.astype(F32), axis=0)
    from_later = laters.reshape(channels, DV).astype(F32)
    (grad_down,) = call(
        down_kernel, [(down_w.shape, BF16)], *c, hidden, ranks=ranks, flops=2 * 10**9
    )
    grad_queries, grad_keys, grad_values, grad_decay = call(
        mixer_kernel,
        [
            (queries.shape, BF16),
            (key_rows.shape, BF16),
            (values.shape, BF16),
            (log_decay.shape, F32),
        ],
        queries,
        key_rows,
        values,
        log_decay,
        out_grad,
        saved_state.reshape(channels, DV),
        from_later,
        scratch=((channels, tokens), (channels, tokens), (values.shape[1], tokens), (channels, 1)),
    )
    return (
        grad_gate[None],
        grad_up[None],
        grad_down[None],
        grad_outproj,
        grad_queries,
        grad_keys,
        grad_values,
        grad_decay,
    )


def solution(mesh):
    torus = Mesh(mesh.devices.reshape(8, 4, 2, mesh.shape["tp"]), ("sp_0", "sp_1", "sp_2", "tp"))

    return jax.shard_map(
        body,
        mesh=torus,
        in_specs=(
            P(SP, None),
            P(SP, None),
            P(SP, None),
            P(SP, None),
            P(SP, None, "tp"),
            P(SP, None, "tp"),
            P(SP, "tp", None),
            P("tp", None),
            P(SP, "tp"),
            P(SP, "tp"),
            P(SP, "tp"),
            P(SP, "tp"),
            P(SP, "tp"),
            P(SP, "tp", None, None),
        ),
        out_specs=(
            P(SP, None, "tp"),
            P(SP, None, "tp"),
            P(SP, "tp", None),
            P(SP, "tp"),
            P(SP, "tp"),
            P(SP, "tp"),
            P(SP, "tp"),
            P(SP, "tp"),
        ),
        check_vma=False,
    )
```
